256 devices in a mesh: grp: 2 (over y), sp: 32 (over z, core), tp: 4 (over x).
Axes of the slice: x: 4, y: 2, z: 16, core: 2. Of those that a mesh axis runs over, the one named last changes fastest.
The devices are a block of a 4x16x16 slice.
Arguments:
- queries_small: bfloat16 [16384, 1024], P(('grp', 'sp'), 'tp'), parts along dimension 0, may hold values from -6 to 6
- keys_small: bfloat16 [16384, 512], P(('grp', 'sp'), 'tp'), parts along dimension 0, may hold values from -6 to 6
- values_small: bfloat16 [16384, 512], P(('grp', 'sp'), 'tp'), parts along dimension 0, may hold values from -6 to 6
- queries_large: bfloat16 [16384, 1024], P(('grp', 'sp'), 'tp'), parts along dimension 0, may hold values from -6 to 6
- keys_large: bfloat16 [16384, 512], P(('grp', 'sp'), 'tp'), parts along dimension 0, may hold values from -6 to 6
- values_large: bfloat16 [16384, 512], P(('grp', 'sp'), 'tp'), parts along dimension 0, may hold values from -6 to 6
- query_gain_small: float32 [128], P('grp'), parts along dimension 0, may hold values from 1.2 to 12
- key_gain_small: float32 [128], P('grp'), parts along dimension 0, may hold values from 1.2 to 12
- query_gain_large: float32 [256], P('grp'), parts along dimension 0, may hold values from 1.2 to 12
- key_gain_large: float32 [256], P('grp'), parts along dimension 0, may hold values from 1.2 to 12
- residual_in: bfloat16 [16384, 2048], P(('grp', 'sp', 'tp')), parts along dimension 0, may hold values from -1.5 to 1.5
- out_weight_small: bfloat16 [1024, 2048], P('tp'), may hold values from -0.125 to 0.125
- out_weight_large: bfloat16 [1024, 2048], P('tp'), may hold values from -0.125 to 0.125
- norm_gain: float32 [2048], replicated, may hold values from 0.1 to 1.9
- routes: int32 [16384, 2], P(('grp', 'sp', 'tp')), parts along dimension 0, may hold values from 0 to 63, all different within a row; in each aligned block of 64 rows (0 to 63, 64 to 127, ...) at most 4 rows name the same one
- route_scores: float32 [16384, 2], P(('grp', 'sp', 'tp')), parts along dimension 0, may hold values from 0.05 to 1
- expert_gate: bfloat16 [64, 2048, 1024], P('sp', None, 'tp'), may hold values from -0.125 to 0.125
- expert_up: bfloat16 [64, 2048, 1024], P('sp', None, 'tp'), may hold values from -0.125 to 0.125
- expert_down: bfloat16 [64, 1024, 2048], P('sp', 'tp'), may hold values from -0.1875 to 0.1875
Outputs:
- result: bfloat16 [16384, 2048], P(('grp', 'sp', 'tp')), parts along dimension 0
The draws below stay inside these ranges and needn't reach their ends.
There are 2 independent parts, one for each index of `grp`. The reference program is written for one: setup_inputs(seed, part) draws one part's arguments, and reference() takes and returns one part's arrays. A program takes and returns all parts, laid end to end along the dimension named above; an argument that names none is the same for every part. Nothing has to cross between parts.
Inputs may be any that keep to these rules, and one draw needn't show every extreme that they name: `routes`: each token names 2 different experts; within the rows of one device (aligned blocks of 64 tokens) no expert is named more than 4 times, a bound that some block reaches.
All inputs are finite; a program needn't handle non-finite values.
Results may differ from the reference program's by a relative error of at most 0.02.
The reference program's roundings to bfloat16 on the way count: a program that leaves them out, or rounds other values in their place, can miss the bound.
Values may be sent and summed in bfloat16 or wider, within the bound.
A program may use at most 128 MiB of HBM per device.

```python
import math
import jax
import jax.numpy as jnp
import numpy as np
from jax import lax

D = 2048
FFE = 1024
HS_SMALL = 64
HS_LARGE = 128
Q_SMALL = 16
KV_SMALL = 8
Q_LARGE = 8
KV_LARGE = 4
GRID_W = 64
TOP = 2
TOK_DEV = 256
SEQ = 8192
ROWS_DEV = 64
EXPERTS = 64
CAP = 4
N_TP = 4


def group_draw(key, query_heads, key_heads, head_size):
    draw_keys = jax.random.split(jax.random.fold_in(key, 7919 + head_size), 4)
    key_rows = jnp.clip(jax.random.normal(draw_keys[0], (SEQ, key_heads * head_size), jnp.float32), -6.0, 6.0)
    query_rows = jnp.clip(jax.random.normal(draw_keys[1], (SEQ, query_heads * head_size), jnp.float32), -6.0, 6.0)
    query_gain = jax.random.uniform(draw_keys[2], (head_size,), jnp.float32, 1.2, 2.0)
    key_gain = jax.random.uniform(draw_keys[3], (head_size,), jnp.float32, 1.2, 2.0)
    return (query_rows, key_rows, query_gain, key_gain)


def draw_queries_small(key, part):
    return group_draw(key, Q_SMALL, KV_SMALL, HS_SMALL)[0].astype(jnp.bfloat16)


def draw_keys_small(key, part):
    return group_draw(key, Q_SMALL, KV_SMALL, HS_SMALL)[1].astype(jnp.bfloat16)


def draw_query_gain_small(key, part):
    return group_draw(key, Q_SMALL, KV_SMALL, HS_SMALL)[2].astype(jnp.float32)


def draw_key_gain_small(key, part):
    return group_draw(key, Q_SMALL, KV_SMALL, HS_SMALL)[3].astype(jnp.float32)


def draw_queries_large(key, part):
    return group_draw(key, Q_LARGE, KV_LARGE, HS_LARGE)[0].astype(jnp.bfloat16)


def draw_keys_large(key, part):
    return group_draw(key, Q_LARGE, KV_LARGE, HS_LARGE)[1].astype(jnp.bfloat16)


def draw_query_gain_large(key, part):
    return group_draw(key, Q_LARGE, KV_LARGE, HS_LARGE)[2].astype(jnp.float32)


def draw_key_gain_large(key, part):
    return group_draw(key, Q_LARGE, KV_LARGE, HS_LARGE)[3].astype(jnp.float32)


def shard_levels(key, shape, pieces, low, largest):
    def one(axis_at, blocks):
        steps = jax.random.uniform(jax.random.fold_in(jax.random.fold_in(key, 6), axis_at), (blocks,), jnp.float32, low / len(pieces), largest / len(pieces))
        return jnp.repeat(jnp.exp(steps), shape[axis_at] // blocks).reshape((-1,) + (1,) * (len(shape) - axis_at - 1))

    loudness = one(*pieces[0])
    for cut in pieces[1:]:
        loudness = loudness * one(*cut)
    return loudness


def deal_out(own_key, own, number, rows, count, top, reach, slope):
    ranking = jax.random.permutation(own_key, count)
    crowded, usual = portions_of(count, rows * top, reach, slope, True), portions_of(count, rows * top, reach, slope, False)
    places = jnp.arange(count)

    def named(lengths, offset_by):
        used = int((lengths > 0).sum())
        fixed = max(1, used // 4)
        passed = fixed + (places - fixed + offset_by * (used - fixed)) % max(1, count - fixed)
        return jnp.zeros((count,), jnp.int32).at[ranking[jnp.where(places < fixed, places, passed)]].set(jnp.asarray(lengths, jnp.int32))

    lengths = jnp.where(number % 4 == 0, named(crowded, number // 4), named(usual, number - number // 4 - 1))
    mixed = jax.random.permutation(jax.random.fold_in(own, 3), count)
    giver, sink = mixed[0:count // 2 * 2:2], mixed[1:count // 2 * 2:2]
    slack = jnp.minimum(lengths[giver] - 1, reach - lengths[sink]) // 2
    slack = jnp.where((giver == ranking[0]) | (sink == ranking[0]) | (lengths[sink] == 0), 0, jnp.maximum(slack, 0))
    passed = jax.random.randint(jax.random.fold_in(own, 4), (count // 2,), 0, 1 << 20) % (slack + 1)
    lengths = lengths.at[giver].add(-passed).at[sink].add(passed)
    members = jnp.searchsorted(jnp.cumsum(lengths), jnp.arange(rows * top), side="right").astype(jnp.int32)
    listing = members.reshape(top, rows).T
    listing = listing[jax.random.permutation(jax.random.fold_in(own, 1), rows)]
    offset_by = jax.random.randint(jax.random.fold_in(own, 2), (rows, 1), 0, top)
    return jnp.take_along_axis(listing, (jnp.arange(top)[None, :] + offset_by) % top, axis=1)


def portions_of(amount, total, reach, skew, full):
    weights = [(1 << 20) // math.isqrt(standing ** skew) + 1 for standing in range(1, amount + 1)]
    largest = reach if full else min(reach, max(-(-total // amount), total * weights[0] // sum(weights)))
    least = 1 if total - largest >= amount - 1 else 0
    given, surplus = [largest] + [least] * (amount - 1), total - largest - least * (amount - 1)
    while surplus > 0:
        movable = [i for i in range(1, amount) if given[i] < largest] or [i for i in range(1, amount) if given[i] < reach]
        mass, remaining = sum([weights[i] for i in movable]), surplus
        for i in movable:
            addition = min(reach - given[i], max(1, remaining * weights[i] // mass), surplus)
            given[i] = given[i] + addition
            surplus = surplus - addition
    return np.array(given)


def normal_values(key, extent, scale, most, cuts=(), held_as=jnp.bfloat16):
    factor_of = shard_levels(key, extent, cuts, -0.22, 0.18) if cuts else 1.0
    array = jax.random.normal(key, extent, jnp.float32) * scale * factor_of
    return jnp.minimum(jnp.maximum(array, -most), most).astype(held_as)


def setup_inputs(seed: int = 0, part: int = 0) -> dict:
    keys = jax.random.split(jax.random.key(seed), 20)
    part_keys = jax.random.split(jax.random.fold_in(keys[19], part), 20)
    queries_small = draw_queries_small(jax.random.fold_in(jax.random.fold_in(keys[19], part), 71), part)
    keys_small = draw_keys_small(jax.random.fold_in(jax.random.fold_in(keys[19], part), 71), part)
    values_small = normal_values(part_keys[2], (SEQ, KV_SMALL * HS_SMALL), 1.0, 6.0, ((0, 32), (1, 4)))
    queries_large = draw_queries_large(jax.random.fold_in(jax.random.fold_in(keys[19], part), 71), part)
    keys_large = draw_keys_large(jax.random.fold_in(jax.random.fold_in(keys[19], part), 71), part)
    values_large = normal_values(part_keys[5], (SEQ, KV_LARGE * HS_LARGE), 1.0, 6.0, ((0, 32), (1, 4)))
    query_gain_small = draw_query_gain_small(jax.random.fold_in(jax.random.fold_in(keys[19], part), 71), part)
    key_gain_small = draw_key_gain_small(jax.random.fold_in(jax.random.fold_in(keys[19], part), 71), part)
    query_gain_large = draw_query_gain_large(jax.random.fold_in(jax.random.fold_in(keys[19], part), 71), part)
    key_gain_large = draw_key_gain_large(jax.random.fold_in(jax.random.fold_in(keys[19], part), 71), part)
    residual_in = normal_values(part_keys[10], (SEQ, D), 0.25, 1.5, ((0, 128),))
    out_weight_small = normal_values(keys[11], (Q_SMALL * HS_SMALL, D), (Q_SMALL * HS_SMALL + Q_LARGE * HS_LARGE) ** -0.5, 0.125, ((0, 4),))
    out_weight_large = normal_values(keys[12], (Q_LARGE * HS_LARGE, D), (Q_SMALL * HS_SMALL + Q_LARGE * HS_LARGE) ** -0.5, 0.125, ((0, 4),))
    norm_gain = jnp.clip(1.0 + 0.18 * jax.random.normal(keys[13], (D,), jnp.float32), 0.1, 1.9)
    routes_keys = jax.random.split(jax.random.fold_in(part_keys[14], 1), SEQ // ROWS_DEV)
    routes_turns = jax.random.permutation(jax.random.fold_in(part_keys[14], 3), SEQ // ROWS_DEV)
    routes = jax.vmap(lambda own, number: deal_out(jax.random.fold_in(part_keys[14], 2), own, number, ROWS_DEV, EXPERTS, TOP, CAP, 1))(routes_keys, routes_turns).reshape((SEQ, TOP))
    route_scores = jnp.clip(0.05 + 0.95 * jax.random.uniform(part_keys[15], (SEQ, TOP), jnp.float32) ** shard_levels(part_keys[15], (SEQ, TOP), ((0, 128),), -0.2, 0.2), 0.05, 1.0)
    expert_gate = normal_values(keys[16], (EXPERTS, D, FFE), D ** -0.5, 0.125, ((0, 32), (2, 4)))
    expert_up = normal_values(keys[17], (EXPERTS, D, FFE), D ** -0.5, 0.125, ((0, 32), (2, 4)))
    expert_down = normal_values(keys[18], (EXPERTS, FFE, D), FFE ** -0.5, 0.1875, ((0, 32), (1, 4)))
    return dict(queries_small=queries_small, keys_small=keys_small, values_small=values_small, queries_large=queries_large, keys_large=keys_large, values_large=values_large, query_gain_small=query_gain_small, key_gain_small=key_gain_small, query_gain_large=query_gain_large, key_gain_large=key_gain_large, residual_in=residual_in, out_weight_small=out_weight_small, out_weight_large=out_weight_large, norm_gain=norm_gain, routes=routes, route_scores=route_scores, expert_gate=expert_gate, expert_up=expert_up, expert_down=expert_down)


theta_base = 10000.0
norm_eps = 1e-06

def grid_tables(offset, length, head_size):
    places = offset + jnp.arange(length, dtype=jnp.int32)
    grid_rows = (places // GRID_W).astype(jnp.float32)
    grid_cols = (places % GRID_W).astype(jnp.float32)
    rates = jnp.power(theta_base, -2.0 * jnp.arange(head_size // 4, dtype=jnp.float32) / (head_size // 2))
    row_angles = grid_rows[:, None, None] * rates
    col_angles = grid_cols[:, None, None] * rates
    return (jnp.cos(row_angles), jnp.sin(row_angles), jnp.cos(col_angles), jnp.sin(col_angles))

def half_turn(segment, cosine, sine_part):
    half_size = segment.shape[-1] // 2
    leading = segment[..., :half_size]
    trailing = segment[..., half_size:]
    return jnp.concatenate([leading * cosine - trailing * sine_part, trailing * cosine + leading * sine_part], axis=-1)

def grid_turn(vectors, tables):
    row_cos, row_sin, col_cos, col_sin = tables
    half_size = vectors.shape[-1] // 2
    return jnp.concatenate([half_turn(vectors[..., :half_size], row_cos, row_sin), half_turn(vectors[..., half_size:], col_cos, col_sin)], axis=-1)

def normed_turn(raw_rows, gain, tables):
    widened = raw_rows.astype(jnp.float32)
    scaled = widened * lax.rsqrt(lax.optimization_barrier(jnp.mean(widened * widened, axis=-1, keepdims=True)) + norm_eps) * gain
    return grid_turn(scaled, tables).astype(jnp.bfloat16)

def attend_group(queries, key_rows, value_rows, query_gain, key_gain, head_size):
    seq_len = queries.shape[0]
    query_heads = queries.shape[1] // head_size
    key_heads = key_rows.shape[1] // head_size
    group_ratio = query_heads // key_heads
    tables = grid_tables(0, seq_len, head_size)
    asked = normed_turn(queries.reshape(seq_len, query_heads, head_size), query_gain, tables)
    keyed = normed_turn(key_rows.reshape(seq_len, key_heads, head_size), key_gain, tables)
    valued = value_rows.reshape(seq_len, key_heads, head_size)

    def one_head(head_index):
        asked_head = lax.dynamic_index_in_dim(asked, head_index, 1, keepdims=False)
        keyed_head = lax.dynamic_index_in_dim(keyed, head_index // group_ratio, 1, keepdims=False)
        valued_head = lax.dynamic_index_in_dim(valued, head_index // group_ratio, 1, keepdims=False)

        def one_block(query_block):
            scores = jnp.dot(query_block, keyed_head.T, preferred_element_type=jnp.float32) * head_size ** (-0.5)
            peak_score = lax.optimization_barrier(jnp.max(scores, axis=1, keepdims=True))
            weights = jnp.exp(scores - peak_score)
            summed = jnp.dot(weights.astype(jnp.bfloat16), valued_head, preferred_element_type=jnp.float32)
            return (summed / lax.optimization_barrier(jnp.sum(weights, axis=1, keepdims=True))).astype(jnp.bfloat16)
        blocks = asked_head.reshape(seq_len // TOK_DEV, TOK_DEV, head_size)
        return lax.map(one_block, blocks).reshape(seq_len, head_size)
    heard = lax.map(one_head, jnp.arange(query_heads, dtype=jnp.int32))
    return jnp.transpose(heard, (1, 0, 2)).reshape(seq_len, query_heads * head_size)

def expert_chain(rows_in, gate_weight, up_weight, down_weight):
    gate_out = jnp.dot(rows_in, gate_weight, preferred_element_type=jnp.float32)
    up_out = jnp.dot(rows_in, up_weight, preferred_element_type=jnp.float32)
    active = (jax.nn.silu(gate_out) * up_out).astype(jnp.bfloat16)
    width_part = FFE // N_TP
    total_terms = jnp.zeros((rows_in.shape[0], D), jnp.float32)
    for part_index in range(N_TP):
        lower = part_index * width_part
        term = jnp.dot(active[:, lower:lower + width_part], down_weight[lower:lower + width_part], preferred_element_type=jnp.float32).astype(jnp.bfloat16)
        total_terms = total_terms + lax.optimization_barrier(term).astype(jnp.float32)
    return total_terms.astype(jnp.bfloat16)

def reference(queries_small, keys_small, values_small, queries_large, keys_large, values_large, query_gain_small, key_gain_small, query_gain_large, key_gain_large, residual_in, out_weight_small, out_weight_large, norm_gain, routes, route_scores, expert_gate, expert_up, expert_down):
    heard_small = attend_group(queries_small, keys_small, values_small, query_gain_small, key_gain_small, HS_SMALL)
    heard_large = attend_group(queries_large, keys_large, values_large, query_gain_large, key_gain_large, HS_LARGE)
    small_cols = Q_SMALL * HS_SMALL // N_TP
    large_cols = Q_LARGE * HS_LARGE // N_TP
    projected = jnp.zeros((SEQ, D), jnp.float32)
    for part_index in range(N_TP):
        lower_small = part_index * small_cols
        lower_large = part_index * large_cols
        term = jnp.dot(heard_small[:, lower_small:lower_small + small_cols], out_weight_small[lower_small:lower_small + small_cols], preferred_element_type=jnp.float32) + jnp.dot(heard_large[:, lower_large:lower_large + large_cols], out_weight_large[lower_large:lower_large + large_cols], preferred_element_type=jnp.float32)
        term = term.astype(jnp.bfloat16)
        projected = projected + lax.optimization_barrier(term).astype(jnp.float32)
    attended = (residual_in.astype(jnp.float32) + projected).astype(jnp.bfloat16)
    widened = attended.astype(jnp.float32)
    normed = (widened * lax.rsqrt(lax.optimization_barrier(jnp.mean(widened * widened, axis=-1, keepdims=True)) + norm_eps) * norm_gain).astype(jnp.bfloat16)
    shares = route_scores / lax.optimization_barrier(jnp.sum(route_scores, axis=1, keepdims=True))
    block_count = SEQ // ROWS_DEV
    flat_routes = routes.reshape(block_count, ROWS_DEV * TOP)
    member = (flat_routes[:, :, None] == jnp.arange(EXPERTS, dtype=jnp.int32)[None, None, :]).astype(jnp.int32)
    ranks = lax.optimization_barrier(jnp.sum((jnp.cumsum(member, axis=1) - member) * member, axis=2))
    slot_within = jnp.arange(block_count, dtype=jnp.int32)[:, None] * CAP + ranks
    token_ids = jnp.arange(SEQ, dtype=jnp.int32).reshape(block_count, ROWS_DEV)
    token_of = jnp.broadcast_to(token_ids[:, :, None], (block_count, ROWS_DEV, TOP)).reshape(-1)
    slot_tokens = jnp.zeros((EXPERTS, block_count * CAP), jnp.int32).at[flat_routes.reshape(-1), slot_within.reshape(-1)].set(token_of)
    slot_shares = jnp.zeros((EXPERTS, block_count * CAP), jnp.float32).at[flat_routes.reshape(-1), slot_within.reshape(-1)].set(shares.reshape(-1))

    def add_expert(mixed, inputs):
        tokens_here, shares_here, gate_weight, up_weight, down_weight = inputs
        outputs = expert_chain(normed[tokens_here], gate_weight, up_weight, down_weight)
        return (mixed.at[tokens_here].add(outputs.astype(jnp.float32) * shares_here[:, None]), None)
    mixed = lax.scan(add_expert, jnp.zeros((SEQ, D), jnp.float32), (slot_tokens, slot_shares, expert_gate, expert_up, expert_down))[0]
    return (attended.astype(jnp.float32) + mixed).astype(jnp.bfloat16)
```

```python
import functools
import jax
import jax.numpy as jnp
from jax import lax
from jax.experimental import pallas as pl
from jax.experimental.pallas import tpu as pltpu
from jax.sharding import PartitionSpec as P

HS_SMALL = 64
HS_LARGE = 128
GRID_W = 64
LOG2E = 1.4426950408889634
theta_base = 10000.0
norm_eps = 1e-06


def _send(src, dst, ssem, rsem, axis, dev):
    return pltpu.make_async_remote_copy(
        src_ref=src,
        dst_ref=dst,
        send_sem=ssem,
        recv_sem=rsem,
        device_id={axis: dev},
        device_id_type=pl.DeviceIdType.MESH,
    )


def attend_kernel(
    heads,
    kv_hbm,
    qt_ref,
    ws_hbm,
    wl_hbm,
    res_ref,
    gain_ref,
    att_ref,
    nrm_ref,
    rts_ref,
    kvbuf,
    wbuf,
    acc,
    mbuf,
    lbuf,
    hbuf,
    pbuf,
    xbuf,
    lsem,
    rsem,
    ssem,
    psem,
    xr,
    xs,
):
    n_sp = lax.axis_size("sp")
    n_z = n_sp // 2
    last = n_z // 2
    tok = kvbuf.shape[3]
    kv_rows = kvbuf.shape[2]
    sp = lax.axis_index("sp")
    tp = lax.axis_index("tp")
    right = lax.rem(sp + 2, n_sp)
    left = lax.rem(sp + n_sp - 2, n_sp)
    partner = sp + 1 - 2 * lax.rem(sp, 2)
    x_right = lax.rem(tp + 1, 4)
    x_left = lax.rem(tp + 3, 4)
    x_far = lax.rem(tp + 2, 4)

    own = pltpu.make_async_copy(kv_hbm, kvbuf.at[0, 0], lsem.at[0])
    own.start()
    w_copies = [
        pltpu.make_async_copy(ws_hbm, wbuf.at[pl.ds(0, 256)], lsem.at[1]),
        pltpu.make_async_copy(wl_hbm, wbuf.at[pl.ds(256, 256)], lsem.at[2]),
    ]
    for w in w_copies:
        w.start()

    barrier = pltpu.get_barrier_semaphore()
    for dev in (right, left, partner):
        pl.semaphore_signal(
            barrier, inc=1, device_id={"sp": dev}, device_id_type=pl.DeviceIdType.MESH
        )
    for dev in (x_right, x_left):
        pl.semaphore_signal(
            barrier, inc=1, device_id={"tp": dev}, device_id_type=pl.DeviceIdType.MESH
        )
    pl.semaphore_wait(barrier, 5)

    parts = (pl.ds(0, tok), pl.ds(tok, kv_rows - tok))

    def at(pair, side, part):
        return kvbuf.at[pair, side, parts[part]]

    def to_right(step, pair, part, dst_pair):
        return _send(
            at(pair, 0, part),
            at(dst_pair, 0, part),
            ssem.at[step, 0, part],
            rsem.at[dst_pair, 0, part],
            "sp",
            right,
        )

    def to_left(step, pair, part, dst_pair, src_side=1, dst_side=1):
        return _send(
            at(pair, src_side, part),
            at(dst_pair, dst_side, part),
            ssem.at[step, 1, part],
            rsem.at[dst_pair, dst_side, part],
            "sp",
            left,
        )

    def to_partner(pair, side, part, dst_pair, dst_side):
        return _send(
            at(pair, side, part),
            at(dst_pair, dst_side, part),
            psem.at[dst_pair, dst_side, part],
            rsem.at[dst_pair, dst_side, part],
            "sp",
            partner,
        )

    def arrived(pair, side, part):
        to_partner(pair, side, part, pair, side).wait_recv()

    own.wait()
    for part in range(2):
        to_right(1, 0, part, 1).start()
        to_left(1, 0, part, 1, src_side=0).start()
        to_partner(0, 0, part, 0, 1).start()

    acc[...] = jnp.zeros_like(acc)
    lbuf[...] = jnp.zeros_like(lbuf)
    mbuf[...] = jnp.full(mbuf.shape, -1e30, jnp.float32)

    def compute(pair):
        keys = kvbuf[pair, :, pl.ds(0, tok), :].reshape(2 * tok, tok)
        for h, (a0, rows, v0, scale) in enumerate(heads):
            s = jnp.dot(keys, qt_ref[h], preferred_element_type=jnp.float32)
            m_old = mbuf[h]
            m_new = jnp.maximum(m_old, jnp.max(s, axis=0, keepdims=True))
            p = jnp.exp2((s - m_new) * (scale * LOG2E))
            shrink = jnp.exp2((m_old - m_new) * (scale * LOG2E))
            mbuf[h] = m_new
            lbuf[h] = lbuf[h] * shrink + jnp.sum(p, axis=0, keepdims=True)
            pb = p.astype(jnp.bfloat16)
            pv = jnp.dot(
                kvbuf[pair, 0, pl.ds(tok + v0, rows), :],
                pb[:tok],
                preferred_element_type=jnp.float32,
            ) + jnp.dot(
                kvbuf[pair, 1, pl.ds(tok + v0, rows), :],
                pb[tok:],
                preferred_element_type=jnp.float32,
            )
            acc[pl.ds(a0, rows), :] = acc[pl.ds(a0, rows), :] * shrink + pv

    def turn(t, carry):
        step = t // 2 + 1
        phase = lax.rem(t, 2)
        pair = 2 * step - 1
        for part in range(2):

            @pl.when((phase == part) & (step < last))
            def _():
                for side in range(2):
                    arrived(pair, side, part)

                @pl.when(step < last - 1)
                def _():
                    to_right(step + 1, pair, part, pair + 2).start()
                    to_left(step + 1, pair, part, pair + 2).start()

                @pl.when(step == last - 1)
                def _():
                    if part == 0:
                        to_right(step + 1, pair, 0, 2 * last - 1).start()
                    else:
                        to_left(step + 1, pair, 1, 2 * last - 1, dst_side=0).start()

                for side in range(2):
                    to_partner(pair, side, part, pair + 1, side).start()

        @pl.when(t == 0)
        def _():
            for part in range(2):
                arrived(0, 1, part)

        @pl.when((phase == 0) & (t > 0))
        def _():
            for side in range(2):
                for part in range(2):
                    arrived(t, side, part)

        @pl.when(t == 2 * last - 1)
        def _():
            for part in range(2):
                arrived(2 * last - 1, 0, part)
                to_partner(2 * last - 1, 0, part, 2 * last - 1, 1).start()
            for part in range(2):
                arrived(2 * last - 1, 1, part)

        compute(t)
        return carry

    lax.fori_loop(0, 2 * last, turn, 0)

    for w in w_copies:
        w.wait()
    for h, (a0, rows, v0, scale) in enumerate(heads):
        heard = acc[pl.ds(a0, rows), :] / lbuf[h]
        acc[pl.ds(a0, rows), :] = heard
    heard = jnp.transpose(acc[...]).astype(jnp.bfloat16)
    block = tok // 4
    hbuf[...] = heard.reshape(4, block, heard.shape[1])

    def project(where, owner):
        pbuf[where] = jnp.dot(
            hbuf[owner], wbuf[...], preferred_element_type=jnp.float32
        ).astype(jnp.bfloat16)

    half = block // 2
    lo, hi = pl.ds(0, half), pl.ds(half, half)
    project(0, x_far)
    first_r = _send(pbuf.at[0, lo], xbuf.at[3, lo], xs.at[0], xr.at[0], "tp", x_right)
    first_l = _send(pbuf.at[0, hi], xbuf.at[3, hi], xs.at[1], xr.at[1], "tp", x_left)
    first_r.start()
    first_l.start()
    project(1, x_right)
    near_r = _send(pbuf.at[1], xbuf.at[0], xs.at[2], xr.at[2], "tp", x_right)
    near_r.start()
    project(2, x_left)
    near_l = _send(pbuf.at[2], xbuf.at[1], xs.at[3], xr.at[3], "tp", x_left)
    near_l.start()
    project(3, tp)
    first_r.wait_recv()
    pass_r = _send(xbuf.at[3, lo], xbuf.at[2, lo], xs.at[4], xr.at[4], "tp", x_right)
    pass_r.start()
    first_l.wait_recv()
    pass_l = _send(xbuf.at[3, hi], xbuf.at[2, hi], xs.at[5], xr.at[5], "tp", x_left)
    pass_l.start()

    for pair in range(2 * last):
        for side in range(2):
            rts_ref[pair, side] = kvbuf[pair, side, pl.ds(kv_rows - 16, 16), pl.ds(0, 128)]

    near_r.wait_recv()
    near_l.wait_recv()
    pass_r.wait_recv()
    pass_l.wait_recv()
    total = (
        pbuf[3].astype(jnp.float32)
        + xbuf[0].astype(jnp.float32)
        + xbuf[1].astype(jnp.float32)
        + xbuf[2].astype(jnp.float32)
    )
    attended = (res_ref[...].astype(jnp.float32) + total).astype(jnp.bfloat16)
    att_ref[...] = attended
    wide = attended.astype(jnp.float32)
    nrm_ref[...] = (
        wide
        * lax.rsqrt(jnp.mean(wide * wide, axis=-1, keepdims=True) + norm_eps)
        * gain_ref[...]
    ).astype(jnp.bfloat16)

    for c in (first_r, first_l, near_r, near_l, pass_r, pass_l):
        c.wait_send()
    for part in range(2):
        to_right(1, 0, part, 1).wait_send()
        to_left(1, 0, part, 1, src_side=0).wait_send()
        to_partner(0, 0, part, 0, 1).wait_send()

    def sent(step, carry):
        pair = 2 * step - 1
        for part in range(2):

            @pl.when(step < last - 1)
            def _():
                to_right(step + 1, pair, part, pair + 2).wait_send()
                to_left(step + 1, pair, part, pair + 2).wait_send()

            for side in range(2):
                to_partner(pair, side, part, pair + 1, side).wait_send()
        return carry

    lax.fori_loop(1, last, sent, 0)
    to_right(last, 2 * last - 3, 0, 2 * last - 1).wait_send()
    to_left(last, 2 * last - 3, 1, 2 * last - 1, dst_side=0).wait_send()
    for part in range(2):
        to_partner(2 * last - 1, 0, part, 2 * last - 1, 1).wait_send()


def attend(kv_block, queries_t, w_small, w_large, residual, gain, heads, n_sp):
    pairs = n_sp // 2
    kv_rows, tok = kv_block.shape
    width = residual.shape[1]
    rows = residual.shape[0]
    n_heads = queries_t.shape[0]
    vmem = pl.BlockSpec(memory_space=pltpu.VMEM)
    hbm = pl.BlockSpec(memory_space=pl.ANY)
    depth = w_small.shape[0] + w_large.shape[0]
    return pl.pallas_call(
        functools.partial(attend_kernel, heads),
        out_shape=(
            jax.ShapeDtypeStruct((rows, width), jnp.bfloat16),
            jax.ShapeDtypeStruct((rows, width), jnp.bfloat16),
            jax.ShapeDtypeStruct((pairs, 2, 16, 128), jnp.bfloat16),
        ),
        in_specs=[hbm, vmem, hbm, hbm, vmem, vmem],
        out_specs=(vmem, vmem, vmem),
        scratch_shapes=[
            pltpu.VMEM((pairs, 2, kv_rows, tok), jnp.bfloat16),
            pltpu.VMEM((depth, width), jnp.bfloat16),
            pltpu.VMEM((depth, tok), jnp.float32),
            pltpu.VMEM((n_heads, 1, tok), jnp.float32),
            pltpu.VMEM((n_heads, 1, tok), jnp.float32),
            pltpu.VMEM((4, tok // 4, depth), jnp.bfloat16),
            pltpu.VMEM((4, rows, width), jnp.bfloat16),
            pltpu.VMEM((4, rows, width), jnp.bfloat16),
            pltpu.SemaphoreType.DMA((3,)),
            pltpu.SemaphoreType.DMA((pairs, 2, 2)),
            pltpu.SemaphoreType.DMA((pairs // 2 + 1, 2, 2)),
            pltpu.SemaphoreType.DMA((pairs, 2, 2)),
            pltpu.SemaphoreType.DMA((6,)),
            pltpu.SemaphoreType.DMA((6,)),
        ],
        compiler_params=pltpu.CompilerParams(
            collective_id=0, has_side_effects=True, vmem_limit_bytes=48 * 1024 * 1024
        ),
        name="attend",
    )(kv_block, queries_t, w_small, w_large, residual, gain)


def grid_tables(offset, length, head_size):
    places = offset + jnp.arange(length, dtype=jnp.int32)
    grid_rows = (places // GRID_W).astype(jnp.float32)
    grid_cols = (places % GRID_W).astype(jnp.float32)
    rates = jnp.power(
        theta_base, -2.0 * jnp.arange(head_size // 4, dtype=jnp.float32) / (head_size // 2)
    )
    row_angles = grid_rows[:, None, None] * rates
    col_angles = grid_cols[:, None, None] * rates
    return (jnp.cos(row_angles), jnp.sin(row_angles), jnp.cos(col_angles), jnp.sin(col_angles))


def half_turn(segment, cosine, sine_part):
    half_size = segment.shape[-1] // 2
    leading = segment[..., :half_size]
    trailing = segment[..., half_size:]
    return jnp.concatenate(
        [leading * cosine - trailing * sine_part, trailing * cosine + leading * sine_part], axis=-1
    )


def grid_turn(vectors, tables):
    row_cos, row_sin, col_cos, col_sin = tables
    half_size = vectors.shape[-1] // 2
    return jnp.concatenate(
        [
            half_turn(vectors[..., :half_size], row_cos, row_sin),
            half_turn(vectors[..., half_size:], col_cos, col_sin),
        ],
        axis=-1,
    )


def normed_turn(raw_rows, gain, tables):
    widened = raw_rows.astype(jnp.float32)
    scaled = (
        widened * lax.rsqrt(jnp.mean(widened * widened, axis=-1, keepdims=True) + norm_eps) * gain
    )
    return grid_turn(scaled, tables).astype(jnp.bfloat16)


def on_device(
    queries_small,
    keys_small,
    values_small,
    queries_large,
    keys_large,
    values_large,
    query_gain_small,
    key_gain_small,
    query_gain_large,
    key_gain_large,
    residual_in,
    out_weight_small,
    out_weight_large,
    norm_gain,
    routes,
    route_scores,
    expert_gate,
    expert_up,
    expert_down,
):
    token_rows = queries_small.shape[0]
    offset = lax.axis_index("sp") * token_rows
    tables_small = grid_tables(offset, token_rows, HS_SMALL)
    tables_large = grid_tables(offset, token_rows, HS_LARGE)
    kv_small = keys_small.shape[1] // HS_SMALL
    kv_large = keys_large.shape[1] // HS_LARGE
    asked_small = normed_turn(
        queries_small.reshape(token_rows, -1, HS_SMALL), query_gain_small, tables_small
    )
    asked_large = normed_turn(
        queries_large.reshape(token_rows, -1, HS_LARGE), query_gain_large, tables_large
    )
    turned_small = normed_turn(
        keys_small.reshape(token_rows, kv_small, HS_SMALL), key_gain_small, tables_small
    ).reshape(token_rows, -1)
    turned_large = normed_turn(
        keys_large.reshape(token_rows, kv_large, HS_LARGE), key_gain_large, tables_large
    ).reshape(token_rows, -1)
    wide_small = turned_small.shape[1]
    width = wide_small + turned_large.shape[1]
    key_block = jnp.concatenate([turned_small, turned_large], axis=1)
    value_block = jnp.concatenate([values_small, values_large], axis=1).T
    names = routes.T.reshape(1, -1).astype(jnp.bfloat16)
    names = jnp.pad(names, ((0, 15), (0, token_rows - names.shape[1])))
    kv_block = jnp.concatenate([key_block, value_block, names], axis=0)
    heads, query_parts = [], []
    for asked, count, size, base in (
        (asked_small, kv_small, HS_SMALL, 0),
        (asked_large, kv_large, HS_LARGE, wide_small),
    ):
        by_head = jnp.transpose(asked, (1, 2, 0))
        ratio = asked.shape[1] // count
        for h in range(asked.shape[1]):
            at = base + (h // ratio) * size
            heads.append((base * 2 + h * size, size, at, size ** (-0.5)))
            query_parts.append(jnp.pad(by_head[h], ((at, width - at - size), (0, 0))))
    attended, normed, names_all = attend(
        kv_block,
        jnp.stack(query_parts),
        out_weight_small,
        out_weight_large,
        residual_in,
        norm_gain.reshape(1, -1),
        tuple(heads),
        lax.axis_size("sp"),
    )
    local_rows = routes.shape[0]
    top_count = routes.shape[1]
    sp_count = lax.axis_size("sp")
    local_experts = expert_gate.shape[0]
    expert_count = local_experts * sp_count
    capacity = max(2, (2 * top_count * local_rows + expert_count - 1) // expert_count)
    flat_routes = routes.reshape(-1)
    member = (flat_routes[:, None] == jnp.arange(expert_count, dtype=jnp.int32)[None, :]).astype(
        jnp.int32
    )
    ranks = jnp.sum((jnp.cumsum(member, axis=0) - member) * member, axis=1)
    slots = flat_routes * capacity + ranks
    picker = (
        slots[:, None] == jnp.arange(expert_count * capacity, dtype=jnp.int32)[None, :]
    ).astype(jnp.bfloat16)
    placer = jnp.sum(picker.reshape(local_rows, top_count, -1), axis=1)
    outgoing = jnp.einsum("ts,td->sd", placer, normed, preferred_element_type=jnp.float32).astype(
        jnp.bfloat16
    )
    outgoing = outgoing.reshape(sp_count, local_experts, capacity, -1)
    everyone = lax.all_gather(
        lax.all_to_all(outgoing, "sp", split_axis=0, concat_axis=0, tiled=True),
        "tp",
        axis=0,
        tiled=True,
    )
    gate_out = jnp.einsum(
        "secd,edf->secf", everyone, expert_gate, preferred_element_type=jnp.float32
    )
    up_out = jnp.einsum("secd,edf->secf", everyone, expert_up, preferred_element_type=jnp.float32)
    active = (jax.nn.silu(gate_out) * up_out).astype(jnp.bfloat16)
    summed = lax.psum_scatter(
        jnp.einsum(
            "secf,efd->secd", active, expert_down, preferred_element_type=jnp.float32
        ).astype(jnp.bfloat16),
        "tp",
        scatter_dimension=0,
        tiled=True,
    )
    returned = lax.all_to_all(summed, "sp", split_axis=0, concat_axis=0, tiled=True)
    back_rows = returned.reshape(expert_count * capacity, -1)
    chosen_rows = jnp.dot(picker, back_rows, preferred_element_type=jnp.float32).reshape(
        local_rows, top_count, -1
    )
    shares = route_scores / jnp.sum(route_scores, axis=1, keepdims=True)
    mixed = jnp.sum(chosen_rows * shares[:, :, None], axis=1)
    return (attended.astype(jnp.float32) + mixed).astype(jnp.bfloat16)


def solution(mesh):
    in_specs = (
        P(("grp", "sp"), "tp"),
        P(("grp", "sp"), "tp"),
        P(("grp", "sp"), "tp"),
        P(("grp", "sp"), "tp"),
        P(("grp", "sp"), "tp"),
        P(("grp", "sp"), "tp"),
        P("grp"),
        P("grp"),
        P("grp"),
        P("grp"),
        P(("grp", "sp", "tp"), None),
        P("tp", None),
        P("tp", None),
        P(),
        P(("grp", "sp", "tp"), None),
        P(("grp", "sp", "tp"), None),
        P("sp", None, "tp"),
        P("sp", None, "tp"),
        P("sp", "tp", None),
    )
    out_specs = P(("grp", "sp", "tp"), None)
    return jax.shard_map(
        on_device, mesh=mesh, in_specs=in_specs, out_specs=out_specs, check_vma=False
    )
```

```python
import functools
import jax
import jax.numpy as jnp
from jax import lax
from jax.experimental import pallas as pl
from jax.experimental.pallas import tpu as pltpu
from jax.sharding import PartitionSpec as P

HS_SMALL = 64
HS_LARGE = 128
GRID_W = 64
LOG2E = 1.4426950408889634
theta_base = 10000.0
norm_eps = 1e-06


def _send(src, dst, ssem, rsem, axis, dev):
    return pltpu.make_async_remote_copy(
        src_ref=src,
        dst_ref=dst,
        send_sem=ssem,
        recv_sem=rsem,
        device_id={axis: dev},
        device_id_type=pl.DeviceIdType.MESH,
    )


def attend_kernel(
    heads,
    kv_hbm,
    qt_ref,
    ws_hbm,
    wl_hbm,
    res_ref,
    gain_ref,
    att_ref,
    nrm_ref,
    rts_ref,
    kvbuf,
    wbuf,
    acc,
    mbuf,
    lbuf,
    hbuf,
    pbuf,
    xbuf,
    lsem,
    rsem,
    ssem,
    psem,
    xr,
    xs,
):
    n_sp = lax.axis_size("sp")
    n_z = n_sp // 2
    last = n_z // 2
    tok = kvbuf.shape[3]
    kv_rows = kvbuf.shape[2]
    sp = lax.axis_index("sp")
    tp = lax.axis_index("tp")
    right = lax.rem(sp + 2, n_sp)
    left = lax.rem(sp + n_sp - 2, n_sp)
    partner = sp + 1 - 2 * lax.rem(sp, 2)
    x_right = lax.rem(tp + 1, 4)
    x_left = lax.rem(tp + 3, 4)
    x_far = lax.rem(tp + 2, 4)

    own = pltpu.make_async_copy(kv_hbm, kvbuf.at[0, 0], lsem.at[0])
    own.start()
    w_copies = [
        pltpu.make_async_copy(ws_hbm, wbuf.at[pl.ds(0, 256)], lsem.at[1]),
        pltpu.make_async_copy(wl_hbm, wbuf.at[pl.ds(256, 256)], lsem.at[2]),
    ]
    for w in w_copies:
        w.start()

    barrier = pltpu.get_barrier_semaphore()
    for dev in (right, left, partner):
        pl.semaphore_signal(
            barrier, inc=1, device_id={"sp": dev}, device_id_type=pl.DeviceIdType.MESH
        )
    for dev in (x_right, x_left):
        pl.semaphore_signal(
            barrier, inc=1, device_id={"tp": dev}, device_id_type=pl.DeviceIdType.MESH
        )
    pl.semaphore_wait(barrier, 5)

    parts = (pl.ds(0, tok), pl.ds(tok, kv_rows - tok))

    def at(pair, side, part):
        return kvbuf.at[pair, side, parts[part]]

    def to_right(step, pair, part, dst_pair):
        return _send(
            at(pair, 0, part),
            at(dst_pair, 0, part),
            ssem.at[step, 0, part],
            rsem.at[dst_pair, 0, part],
            "sp",
            right,
        )

    def to_left(step, pair, part, dst_pair, src_side=1, dst_side=1):
        return _send(
            at(pair, src_side, part),
            at(dst_pair, dst_side, part),
            ssem.at[step, 1, part],
            rsem.at[dst_pair, dst_side, part],
            "sp",
            left,
        )

    def to_partner(pair, side, part, dst_pair, dst_side):
        return _send(
            at(pair, side, part),
            at(dst_pair, dst_side, part),
            psem.at[dst_pair, dst_side, part],
            rsem.at[dst_pair, dst_side, part],
            "sp",
            partner,
        )

    def arrived(pair, side, part):
        to_partner(pair, side, part, pair, side).wait_recv()

    own.wait()
    for part in range(2):
        to_right(1, 0, part, 1).start()
        to_left(1, 0, part, 1, src_side=0).start()
        to_partner(0, 0, part, 0, 1).start()

    acc[...] = jnp.zeros_like(acc)
    lbuf[...] = jnp.zeros_like(lbuf)
    mbuf[...] = jnp.full(mbuf.shape, -1e30, jnp.float32)

    def compute(pair):
        keys = kvbuf[pair, :, pl.ds(0, tok), :].reshape(2 * tok, tok)
        for h, (a0, rows, v0, scale) in enumerate(heads):
            s = jnp.dot(keys, qt_ref[h], preferred_element_type=jnp.float32)
            m_old = mbuf[h]
            m_new = jnp.maximum(m_old, jnp.max(s, axis=0, keepdims=True))
            p = jnp.exp2((s - m_new) * (scale * LOG2E))
            shrink = jnp.exp2((m_old - m_new) * (scale * LOG2E))
            mbuf[h] = m_new
            lbuf[h] = lbuf[h] * shrink + jnp.sum(p, axis=0, keepdims=True)
            pb = p.astype(jnp.bfloat16)
            pv = jnp.dot(
                kvbuf[pair, 0, pl.ds(tok + v0, rows), :],
                pb[:tok],
                preferred_element_type=jnp.float32,
            ) + jnp.dot(
                kvbuf[pair, 1, pl.ds(tok + v0, rows), :],
                pb[tok:],
                preferred_element_type=jnp.float32,
            )
            acc[pl.ds(a0, rows), :] = acc[pl.ds(a0, rows), :] * shrink + pv

    def turn(t, carry):
        step = t // 2 + 1
        phase = lax.rem(t, 2)
        pair = 2 * step - 1
        for part in range(2):

            @pl.when((phase == part) & (step < last))
            def _():
                for side in range(2):
                    arrived(pair, side, part)

                @pl.when(step < last - 1)
                def _():
                    to_right(step + 1, pair, part, pair + 2).start()
                    to_left(step + 1, pair, part, pair + 2).start()

                @pl.when(step == last - 1)
                def _():
                    if part == 0:
                        to_right(step + 1, pair, 0, 2 * last - 1).start()
                    else:
                        to_left(step + 1, pair, 1, 2 * last - 1, dst_side=0).start()

                for side in range(2):
                    to_partner(pair, side, part, pair + 1, side).start()

        @pl.when(t == 0)
        def _():
            for part in range(2):
                arrived(0, 1, part)

        @pl.when((phase == 0) & (t > 0))
        def _():
            for side in range(2):
                for part in range(2):
                    arrived(t, side, part)

        @pl.when(t == 2 * last - 1)
        def _():
            for part in range(2):
                arrived(2 * last - 1, 0, part)
                to_partner(2 * last - 1, 0, part, 2 * last - 1, 1).start()
            for part in range(2):
                arrived(2 * last - 1, 1, part)

        compute(t)
        return carry

    lax.fori_loop(0, 2 * last, turn, 0)

    for w in w_copies:
        w.wait()
    for h, (a0, rows, v0, scale) in enumerate(heads):
        heard = acc[pl.ds(a0, rows), :] / lbuf[h]
        acc[pl.ds(a0, rows), :] = heard
    heard = jnp.transpose(acc[...]).astype(jnp.bfloat16)
    block = tok // 4
    hbuf[...] = heard.reshape(4, block, heard.shape[1])

    def project(where, owner):
        pbuf[where] = jnp.dot(
            hbuf[owner], wbuf[...], preferred_element_type=jnp.float32
        ).astype(jnp.bfloat16)

    half = block // 2
    lo, hi = pl.ds(0, half), pl.ds(half, half)
    project(0, x_far)
    first_r = _send(pbuf.at[0, lo], xbuf.at[3, lo], xs.at[0], xr.at[0], "tp", x_right)
    first_l = _send(pbuf.at[0, hi], xbuf.at[3, hi], xs.at[1], xr.at[1], "tp", x_left)
    first_r.start()
    first_l.start()
    project(1, x_right)
    near_r = _send(pbuf.at[1], xbuf.at[0], xs.at[2], xr.at[2], "tp", x_right)
    near_r.start()
    project(2, x_left)
    near_l = _send(pbuf.at[2], xbuf.at[1], xs.at[3], xr.at[3], "tp", x_left)
    near_l.start()
    project(3, tp)
    first_r.wait_recv()
    pass_r = _send(xbuf.at[3, lo], xbuf.at[2, lo], xs.at[4], xr.at[4], "tp", x_right)
    pass_r.start()
    first_l.wait_recv()
    pass_l = _send(xbuf.at[3, hi], xbuf.at[2, hi], xs.at[5], xr.at[5], "tp", x_left)
    pass_l.start()

    for pair in range(2 * last):
        for side in range(2):
            rts_ref[pair, side] = kvbuf[pair, side, pl.ds(kv_rows - 16, 16), pl.ds(0, 128)]

    near_r.wait_recv()
    near_l.wait_recv()
    pass_r.wait_recv()
    pass_l.wait_recv()
    total = (
        pbuf[3].astype(jnp.float32)
        + xbuf[0].astype(jnp.float32)
        + xbuf[1].astype(jnp.float32)
        + xbuf[2].astype(jnp.float32)
    )
    attended = (res_ref[...].astype(jnp.float32) + total).astype(jnp.bfloat16)
    att_ref[...] = attended
    wide = attended.astype(jnp.float32)
    nrm_ref[...] = (
        wide
        * lax.rsqrt(jnp.mean(wide * wide, axis=-1, keepdims=True) + norm_eps)
        * gain_ref[...]
    ).astype(jnp.bfloat16)

    for c in (first_r, first_l, near_r, near_l, pass_r, pass_l):
        c.wait_send()
    for part in range(2):
        to_right(1, 0, part, 1).wait_send()
        to_left(1, 0, part, 1, src_side=0).wait_send()
        to_partner(0, 0, part, 0, 1).wait_send()

    def sent(step, carry):
        pair = 2 * step - 1
        for part in range(2):

            @pl.when(step < last - 1)
            def _():
                to_right(step + 1, pair, part, pair + 2).wait_send()
                to_left(step + 1, pair, part, pair + 2).wait_send()

            for side in range(2):
                to_partner(pair, side, part, pair + 1, side).wait_send()
        return carry

    lax.fori_loop(1, last, sent, 0)
    to_right(last, 2 * last - 3, 0, 2 * last - 1).wait_send()
    to_left(last, 2 * last - 3, 1, 2 * last - 1, dst_side=0).wait_send()
    for part in range(2):
        to_partner(2 * last - 1, 0, part, 2 * last - 1, 1).wait_send()


def attend(kv_block, queries_t, w_small, w_large, residual, gain, heads, n_sp):
    pairs = n_sp // 2
    kv_rows, tok = kv_block.shape
    width = residual.shape[1]
    rows = residual.shape[0]
    n_heads = queries_t.shape[0]
    vmem = pl.BlockSpec(memory_space=pltpu.VMEM)
    hbm = pl.BlockSpec(memory_space=pl.ANY)
    depth = w_small.shape[0] + w_large.shape[0]
    return pl.pallas_call(
        functools.partial(attend_kernel, heads),
        out_shape=(
            jax.ShapeDtypeStruct((rows, width), jnp.bfloat16),
            jax.ShapeDtypeStruct((rows, width), jnp.bfloat16),
            jax.ShapeDtypeStruct((pairs, 2, 16, 128), jnp.bfloat16),
        ),
        in_specs=[hbm, vmem, hbm, hbm, vmem, vmem],
        out_specs=(vmem, vmem, vmem),
        scratch_shapes=[
            pltpu.VMEM((pairs, 2, kv_rows, tok), jnp.bfloat16),
            pltpu.VMEM((depth, width), jnp.bfloat16),
            pltpu.VMEM((depth, tok), jnp.float32),
            pltpu.VMEM((n_heads, 1, tok), jnp.float32),
            pltpu.VMEM((n_heads, 1, tok), jnp.float32),
            pltpu.VMEM((4, tok // 4, depth), jnp.bfloat16),
            pltpu.VMEM((4, rows, width), jnp.bfloat16),
            pltpu.VMEM((4, rows, width), jnp.bfloat16),
            pltpu.SemaphoreType.DMA((3,)),
            pltpu.SemaphoreType.DMA((pairs, 2, 2)),
            pltpu.SemaphoreType.DMA((pairs // 2 + 1, 2, 2)),
            pltpu.SemaphoreType.DMA((pairs, 2, 2)),
            pltpu.SemaphoreType.DMA((6,)),
            pltpu.SemaphoreType.DMA((6,)),
        ],
        compiler_params=pltpu.CompilerParams(
            collective_id=0, has_side_effects=True, vmem_limit_bytes=48 * 1024 * 1024
        ),
        name="attend",
    )(kv_block, queries_t, w_small, w_large, residual, gain)


def experts_kernel(
    x_hbm,
    att_ref,
    sel_ref,
    perm_ref,
    pick_ref,
    share_ref,
    wg_hbm,
    wu_hbm,
    wd_hbm,
    out_ref,
    xbuf,
    wg,
    wu,
    wd,
    gbuf,
    pbuf,
    rbuf,
    fbuf,
    obuf,
    ret,
    lsem,
    rsem,
    ssem,
    psem,
    gr,
    gs,
    rr,
    rs,
    tr,
    ts,
):
    n_sp = lax.axis_size("sp")
    n_z = n_sp // 2
    last = n_z // 2
    sp = lax.axis_index("sp")
    tp = lax.axis_index("tp")
    z = sp // 2
    core = lax.rem(sp, 2)
    right = lax.rem(sp + 2, n_sp)
    left = lax.rem(sp + n_sp - 2, n_sp)
    partner = sp + 1 - 2 * core
    x_right = lax.rem(tp + 1, 4)
    x_left = lax.rem(tp + 3, 4)
    rows = xbuf.shape[2]

    own = pltpu.make_async_copy(x_hbm, xbuf.at[0, 0], lsem.at[0])
    own.start()
    w_copies = [
        pltpu.make_async_copy(a, b, lsem.at[1 + i])
        for i, (a, b) in enumerate(((wg_hbm, wg), (wu_hbm, wu), (wd_hbm, wd)))
    ]
    for w in w_copies:
        w.start()

    barrier = pltpu.get_barrier_semaphore()

    def greet(i, carry):
        pl.semaphore_signal(
            barrier,
            inc=1,
            device_id={"sp": lax.rem(sp + i, n_sp)},
            device_id_type=pl.DeviceIdType.MESH,
        )
        return carry

    lax.fori_loop(1, n_sp, greet, 0)
    for dev in (x_right, x_left):
        pl.semaphore_signal(
            barrier, inc=1, device_id={"tp": dev}, device_id_type=pl.DeviceIdType.MESH
        )
    pl.semaphore_wait(barrier, n_sp + 1)

    half = rows // 2
    parts = (pl.ds(0, half), pl.ds(half, half))

    def at(pair, side, part):
        return xbuf.at[pair, side, parts[part]]

    def to_right(step, pair, part, dst_pair):
        return _send(
            at(pair, 0, part),
            at(dst_pair, 0, part),
            ssem.at[step, 0, part],
            rsem.at[dst_pair, 0, part],
            "sp",
            right,
        )

    def to_left(step, pair, part, dst_pair, src_side=1, dst_side=1):
        return _send(
            at(pair, src_side, part),
            at(dst_pair, dst_side, part),
            ssem.at[step, 1, part],
            rsem.at[dst_pair, dst_side, part],
            "sp",
            left,
        )

    def to_partner(pair, side, part, dst_pair, dst_side):
        return _send(
            at(pair, side, part),
            at(dst_pair, dst_side, part),
            psem.at[dst_pair, dst_side, part],
            rsem.at[dst_pair, dst_side, part],
            "sp",
            partner,
        )

    def arrived(pair, side, part):
        to_partner(pair, side, part, pair, side).wait_recv()

    def share_right(c):
        return _send(gbuf.at[c, 0], gbuf.at[c, 1], gs.at[c, 0], gr.at[c, 0], "tp", x_right)

    def share_left(c):
        return _send(gbuf.at[c, 0], gbuf.at[c, 2], gs.at[c, 1], gr.at[c, 1], "tp", x_left)

    def pass_right(c):
        return _send(
            gbuf.at[c, 1, 0], gbuf.at[c, 3, 0], gs.at[c, 2], gr.at[c, 2], "tp", x_right
        )

    def pass_left(c):
        return _send(gbuf.at[c, 2, 1], gbuf.at[c, 3, 1], gs.at[c, 3], gr.at[c, 3], "tp", x_left)

    def far_right(c):
        return _send(pbuf.at[c, 3, 0], rbuf.at[c, 0], rs.at[c, 0], rr.at[c, 0], "tp", x_right)

    def far_left(c):
        return _send(pbuf.at[c, 3, 1], rbuf.at[c, 1], rs.at[c, 1], rr.at[c, 1], "tp", x_left)

    def near_right(c):
        return _send(pbuf.at[c, 2], fbuf.at[c, 0], rs.at[c, 2], rr.at[c, 2], "tp", x_right)

    def near_left(c):
        return _send(pbuf.at[c, 1], fbuf.at[c, 1], rs.at[c, 3], rr.at[c, 3], "tp", x_left)

    own.wait()
    for part in range(2):
        to_right(1, 0, part, 1).start()
        to_left(1, 0, part, 1, src_side=0).start()
        to_partner(0, 0, part, 0, 1).start()

    def run_experts(c):
        for e in range(2):
            x = gbuf[c, :, e].reshape(64, gbuf.shape[4])
            gate = jnp.dot(x, wg[e], preferred_element_type=jnp.float32)
            up = jnp.dot(x, wu[e], preferred_element_type=jnp.float32)
            active = (gate / (1.0 + jnp.exp(-gate)) * up).astype(jnp.bfloat16)
            term = jnp.dot(active, wd[e], preferred_element_type=jnp.float32)
            pbuf[c, :, e] = term.astype(jnp.bfloat16).reshape(4, 16, gbuf.shape[4])

    def gather_turn(c, carry):
        step = c + 1
        pair = 2 * step - 1

        @pl.when(step < last)
        def _():
            for part in range(2):
                for side in range(2):
                    arrived(pair, side, part)

                @pl.when(step < last - 1)
                def _():
                    to_right(step + 1, pair, part, pair + 2).start()
                    to_left(step + 1, pair, part, pair + 2).start()

                @pl.when(step == last - 1)
                def _():
                    if part == 0:
                        to_right(step + 1, pair, 0, 2 * last - 1).start()
                    else:
                        to_left(step + 1, pair, 1, 2 * last - 1, dst_side=0).start()

                for side in range(2):
                    to_partner(pair, side, part, pair + 1, side).start()

        @pl.when(step == last)
        def _():
            for part in range(2):
                arrived(2 * last - 1, 0, part)
                to_partner(2 * last - 1, 0, part, 2 * last - 1, 1).start()

        @pl.when(c == 0)
        def _():
            for part in range(2):
                arrived(0, 1, part)

        @pl.when((c > 0) & (c < last))
        def _():
            for side in range(2):
                for part in range(2):
                    arrived(2 * c, side, part)

        @pl.when(step == last)
        def _():
            for part in range(2):
                arrived(2 * last - 1, 1, part)

        @pl.when(c < last)
        def _():
            tokens = xbuf[pl.ds(2 * c, 2)].reshape(4 * rows, xbuf.shape[3])
            chosen = jnp.dot(sel_ref[c], tokens, preferred_element_type=jnp.float32)
            gbuf[c, 0] = chosen.astype(jnp.bfloat16).reshape(2, 16, xbuf.shape[3])
            share_right(c).start()
            share_left(c).start()

        @pl.when((c >= 1) & (c < last + 1))
        def _():
            share_right(c - 1).wait_recv()
            pass_right(c - 1).start()
            share_left(c - 1).wait_recv()
            pass_left(c - 1).start()

        @pl.when(c == 2)
        def _():
            for w in w_copies:
                w.wait()

        @pl.when(c >= 2)
        def _():
            pass_right(c - 2).wait_recv()
            pass_left(c - 2).wait_recv()
            run_experts(c - 2)

        return carry

    lax.fori_loop(0, last + 2, gather_turn, 0)

    def home(c, q):
        if q == 0:
            return lax.rem(z - c + n_z, n_z) * 2 + 1 - core, 2 * c, 0
        if q == 1:
            return lax.rem(z + c, n_z) * 2 + 1 - core, 2 * c, 1
        if q == 2:
            return lax.rem(z - c - 1 + n_z, n_z) * 2 + core, 2 * c + 1, 0
        return lax.rem(z + c + 1, n_z) * 2 + core, 2 * c + 1, 1

    def give(c, q):
        dev, pair, side = home(c, q)
        return _send(
            obuf.at[c, q], ret.at[pair, side], ts.at[c, q], tr.at[pair, side], "sp", dev
        )

    def give_last():
        dev = lax.rem(z + last, n_z) * 2 + 1 - core
        return _send(
            obuf.at[last - 1, 3],
            ret.at[2 * last - 1, 1],
            ts.at[last - 1, 3],
            tr.at[2 * last - 1, 1],
            "sp",
            dev,
        )

    width = fbuf.shape[4]

    def return_turn(i, carry):
        @pl.when(i < last)
        def _():
            c = last - 1 - i
            far_right(c).start()
            far_left(c).start()

        @pl.when((i >= 1) & (i < last + 1))
        def _():
            c = last - i
            far_right(c).wait_recv()
            pbuf[c, 2, 0] = (
                pbuf[c, 2, 0].astype(jnp.float32) + rbuf[c, 0].astype(jnp.float32)
            ).astype(jnp.bfloat16)
            near_right(c).start()
            far_left(c).wait_recv()
            pbuf[c, 1, 1] = (
                pbuf[c, 1, 1].astype(jnp.float32) + rbuf[c, 1].astype(jnp.float32)
            ).astype(jnp.bfloat16)
            near_left(c).start()

        @pl.when(i >= 2)
        def _():
            c = last + 1 - i
            near_right(c).wait_recv()
            near_left(c).wait_recv()
            total = (
                pbuf[c, 0].astype(jnp.float32)
                + fbuf[c, 0].astype(jnp.float32)
                + fbuf[c, 1].astype(jnp.float32)
            )
            total = total.astype(jnp.bfloat16).reshape(32, width)
            split = jnp.concatenate([total[:, : width // 2], total[:, width // 2 :]], axis=0)
            ordered = jnp.dot(perm_ref[...], split, preferred_element_type=jnp.float32)
            obuf[c] = ordered.astype(jnp.bfloat16).reshape(4, 16, width // 2)

            @pl.when(c > 0)
            def _():
                give(c, 0).start()

            @pl.when(c == 0)
            def _():
                ret[0, 0] = obuf[0, 0]

            give(c, 1).start()
            give(c, 2).start()

            @pl.when(c < last - 1)
            def _():
                give(c, 3).start()

            @pl.when(c == last - 1)
            def _():
                give_last().start()

        return carry

    lax.fori_loop(0, last + 2, return_turn, 0)

    for part in range(2):
        to_right(1, 0, part, 1).wait_send()
        to_left(1, 0, part, 1, src_side=0).wait_send()
        to_partner(0, 0, part, 0, 1).wait_send()

    def sent(step, carry):
        pair = 2 * step - 1
        for part in range(2):

            @pl.when(step < last - 1)
            def _():
                to_right(step + 1, pair, part, pair + 2).wait_send()
                to_left(step + 1, pair, part, pair + 2).wait_send()

            for side in range(2):
                to_partner(pair, side, part, pair + 1, side).wait_send()
        return carry

    lax.fori_loop(1, last, sent, 0)
    to_right(last, 2 * last - 3, 0, 2 * last - 1).wait_send()
    to_left(last, 2 * last - 3, 1, 2 * last - 1, dst_side=0).wait_send()
    for part in range(2):
        to_partner(2 * last - 1, 0, part, 2 * last - 1, 1).wait_send()

    def left_all(c, carry):
        for copy in (share_right, share_left, pass_right, pass_left):
            copy(c).wait_send()
        for copy in (far_right, far_left, near_right, near_left):
            copy(c).wait_send()
        return carry

    lax.fori_loop(0, last, left_all, 0)

    def came(i, carry):
        c = last - 1 - i

        @pl.when(c > 0)
        def _():
            give(c, 0).wait_recv()

        for q in (1, 2, 3):
            give(c, q).wait_recv()
        return carry

    lax.fori_loop(0, last, came, 0)

    back = ret[...].reshape(ret.shape[0] * 32, width // 2)
    picked = jnp.dot(pick_ref[...], back, preferred_element_type=jnp.float32)
    out = att_ref[...].astype(jnp.float32)
    lo = picked[:rows] * share_ref[:, 0:1] + picked[rows : 2 * rows] * share_ref[:, 1:2]
    hi = (
        picked[2 * rows : 3 * rows] * share_ref[:, 0:1]
        + picked[3 * rows :] * share_ref[:, 1:2]
    )
    out_ref[:, : width // 2] = (out[:, : width // 2] + lo).astype(jnp.bfloat16)
    out_ref[:, width // 2 :] = (out[:, width // 2 :] + hi).astype(jnp.bfloat16)

    def gone(c, carry):
        @pl.when(c > 0)
        def _():
            give(c, 0).wait_send()

        for q in (1, 2, 3):
            give(c, q).wait_send()
        return carry

    lax.fori_loop(0, last, gone, 0)


def run_layer_experts(normed, attended, sel, perm, pick, shares, gate, up, down, n_sp):
    pairs = n_sp // 2
    chunks = pairs // 2
    rows, width = normed.shape
    vmem = pl.BlockSpec(memory_space=pltpu.VMEM)
    hbm = pl.BlockSpec(memory_space=pl.ANY)
    bf16 = jnp.bfloat16
    dma = pltpu.SemaphoreType.DMA
    return pl.pallas_call(
        experts_kernel,
        out_shape=jax.ShapeDtypeStruct((rows, width), bf16),
        in_specs=[hbm, vmem, vmem, vmem, vmem, vmem, hbm, hbm, hbm],
        out_specs=vmem,
        scratch_shapes=[
            pltpu.VMEM((pairs, 2, rows, width), bf16),
            pltpu.VMEM(gate.shape, bf16),
            pltpu.VMEM(up.shape, bf16),
            pltpu.VMEM(down.shape, bf16),
            pltpu.VMEM((chunks, 4, 2, 16, width), bf16),
            pltpu.VMEM((chunks, 4, 2, 16, width), bf16),
            pltpu.VMEM((chunks, 2, 16, width), bf16),
            pltpu.VMEM((chunks, 2, 2, 16, width), bf16),
            pltpu.VMEM((chunks, 4, 16, width // 2), bf16),
            pltpu.VMEM((pairs, 2, 16, width // 2), bf16),
            dma((4,)),
            dma((pairs, 2, 2)),
            dma((chunks + 1, 2, 2)),
            dma((pairs, 2, 2)),
            dma((chunks, 4)),
            dma((chunks, 4)),
            dma((chunks, 4)),
            dma((chunks, 4)),
            dma((pairs, 2)),
            dma((chunks, 4)),
        ],
        compiler_params=pltpu.CompilerParams(
            collective_id=1, has_side_effects=True, vmem_limit_bytes=56 * 1024 * 1024
        ),
        name="experts",
    )(normed, attended, sel, perm, pick, shares, gate, up, down)


def experts_of(normed, attended, names_all, routes, route_scores, gate, up, down):
    n_sp = lax.axis_size("sp")
    n_z = n_sp // 2
    last = n_z // 2
    pairs = n_sp // 2
    chunks = pairs // 2
    rows = routes.shape[0]
    sp = lax.axis_index("sp")
    bf16 = jnp.bfloat16
    names = names_all[:, :, 0, :].reshape(n_sp, 2, rows)
    mine = (2 * sp + jnp.arange(2)).astype(bf16)
    member = jnp.any(names[:, None] == mine[None, :, None, None], axis=2)
    before = (jnp.arange(rows)[:, None] < jnp.arange(rows)[None, :]).astype(bf16)
    rank = jnp.einsum(
        "bet,tu->beu", member.astype(bf16), before, preferred_element_type=jnp.float32
    )
    seats = jnp.arange(4, dtype=jnp.float32)
    seated = member[:, :, None] & (rank[:, :, None] == seats[None, None, :, None])
    seated = seated.reshape(chunks, 4, 2, 4, rows).transpose(0, 2, 1, 3, 4)
    same_block = jnp.arange(4)[:, None, None, None] == jnp.arange(4)[None, None, :, None]
    sel = (seated[:, :, :, :, None] & same_block[None, None]).astype(bf16)
    sel = sel.reshape(chunks, 32, 4 * rows)
    out_row = jnp.arange(64)
    block, piece, slot = out_row // 16, (out_row // 8) % 2, out_row % 8
    in_row = piece * 32 + (slot // 4) * 16 + block * 4 + slot % 4
    perm = (in_row[:, None] == jnp.arange(64)[None, :]).astype(bf16)
    same = routes[:, :, None, None] == routes[None, None, :, :]
    earlier = jnp.arange(rows)[:, None, None, None] > jnp.arange(rows)[None, None, :, None]
    own_rank = jnp.sum((same & earlier).astype(jnp.int32), axis=(2, 3))
    host = routes // 2
    away = (sp // 2 - host // 2 + n_z) % n_z
    other = (host % 2 != sp % 2).astype(jnp.int32)
    step = jnp.minimum(away, n_z - away)
    edge = (away == 0) | (away == last)
    pair = jnp.where(away == 0, 0, jnp.where(away == last, 2 * last - 1, 2 * step - 1 + other))
    side = jnp.where(edge, other, (away < last).astype(jnp.int32))
    base = (pair * 2 + side) * 16 + (routes % 2) * 4 + own_rank
    seats_back = jnp.concatenate([base[:, 0], base[:, 1], base[:, 0] + 8, base[:, 1] + 8])
    pick = (seats_back[:, None] == jnp.arange(pairs * 32)[None, :]).astype(bf16)
    shares = route_scores / jnp.sum(route_scores, axis=1, keepdims=True)
    return run_layer_experts(
        normed, attended, sel, perm, pick, shares, gate, up, down, n_sp
    )


def grid_tables(offset, length, head_size):
    places = offset + jnp.arange(length, dtype=jnp.int32)
    grid_rows = (places // GRID_W).astype(jnp.float32)
    grid_cols = (places % GRID_W).astype(jnp.float32)
    rates = jnp.power(
        theta_base, -2.0 * jnp.arange(head_size // 4, dtype=jnp.float32) / (head_size // 2)
    )
    row_angles = grid_rows[:, None, None] * rates
    col_angles = grid_cols[:, None, None] * rates
    return (jnp.cos(row_angles), jnp.sin(row_angles), jnp.cos(col_angles), jnp.sin(col_angles))


def half_turn(segment, cosine, sine_part):
    half_size = segment.shape[-1] // 2
    leading = segment[..., :half_size]
    trailing = segment[..., half_size:]
    return jnp.concatenate(
        [leading * cosine - trailing * sine_part, trailing * cosine + leading * sine_part], axis=-1
    )


def grid_turn(vectors, tables):
    row_cos, row_sin, col_cos, col_sin = tables
    half_size = vectors.shape[-1] // 2
    return jnp.concatenate(
        [
            half_turn(vectors[..., :half_size], row_cos, row_sin),
            half_turn(vectors[..., half_size:], col_cos, col_sin),
        ],
        axis=-1,
    )


def normed_turn(raw_rows, gain, tables):
    widened = raw_rows.astype(jnp.float32)
    scaled = (
        widened * lax.rsqrt(jnp.mean(widened * widened, axis=-1, keepdims=True) + norm_eps) * gain
    )
    return grid_turn(scaled, tables).astype(jnp.bfloat16)


def on_device(
    queries_small,
    keys_small,
    values_small,
    queries_large,
    keys_large,
    values_large,
    query_gain_small,
    key_gain_small,
    query_gain_large,
    key_gain_large,
    residual_in,
    out_weight_small,
    out_weight_large,
    norm_gain,
    routes,
    route_scores,
    expert_gate,
    expert_up,
    expert_down,
):
    token_rows = queries_small.shape[0]
    offset = lax.axis_index("sp") * token_rows
    tables_small = grid_tables(offset, token_rows, HS_SMALL)
    tables_large = grid_tables(offset, token_rows, HS_LARGE)
    kv_small = keys_small.shape[1] // HS_SMALL
    kv_large = keys_large.shape[1] // HS_LARGE
    asked_small = normed_turn(
        queries_small.reshape(token_rows, -1, HS_SMALL), query_gain_small, tables_small
    )
    asked_large = normed_turn(
        queries_large.reshape(token_rows, -1, HS_LARGE), query_gain_large, tables_large
    )
    turned_small = normed_turn(
        keys_small.reshape(token_rows, kv_small, HS_SMALL), key_gain_small, tables_small
    ).reshape(token_rows, -1)
    turned_large = normed_turn(
        keys_large.reshape(token_rows, kv_large, HS_LARGE), key_gain_large, tables_large
    ).reshape(token_rows, -1)
    wide_small = turned_small.shape[1]
    width = wide_small + turned_large.shape[1]
    key_block = jnp.concatenate([turned_small, turned_large], axis=1)
    value_block = jnp.concatenate([values_small, values_large], axis=1).T
    names = routes.T.reshape(1, -1).astype(jnp.bfloat16)
    names = jnp.pad(names, ((0, 15), (0, token_rows - names.shape[1])))
    kv_block = jnp.concatenate([key_block, value_block, names], axis=0)
    heads, query_parts = [], []
    for asked, count, size, base in (
        (asked_small, kv_small, HS_SMALL, 0),
        (asked_large, kv_large, HS_LARGE, wide_small),
    ):
        by_head = jnp.transpose(asked, (1, 2, 0))
        ratio = asked.shape[1] // count
        for h in range(asked.shape[1]):
            at = base + (h // ratio) * size
            heads.append((base * 2 + h * size, size, at, size ** (-0.5)))
            query_parts.append(jnp.pad(by_head[h], ((at, width - at - size), (0, 0))))
    attended, normed, names_all = attend(
        kv_block,
        jnp.stack(query_parts),
        out_weight_small,
        out_weight_large,
        residual_in,
        norm_gain.reshape(1, -1),
        tuple(heads),
        lax.axis_size("sp"),
    )
    return experts_of(
        normed,
        attended,
        names_all,
        routes,
        route_scores,
        expert_gate,
        expert_up,
        expert_down,
    )


def solution(mesh):
    in_specs = (
        P(("grp", "sp"), "tp"),
        P(("grp", "sp"), "tp"),
        P(("grp", "sp"), "tp"),
        P(("grp", "sp"), "tp"),
        P(("grp", "sp"), "tp"),
        P(("grp", "sp"), "tp"),
        P("grp"),
        P("grp"),
        P("grp"),
        P("grp"),
        P(("grp", "sp", "tp"), None),
        P("tp", None),
        P("tp", None),
        P(),
        P(("grp", "sp", "tp"), None),
        P(("grp", "sp", "tp"), None),
        P("sp", None, "tp"),
        P("sp", None, "tp"),
        P("sp", "tp", None),
    )
    out_specs = P(("grp", "sp", "tp"), None)
    return jax.shard_map(
        on_device, mesh=mesh, in_specs=in_specs, out_specs=out_specs, check_vma=False
    )
```

```python
import functools
import jax
import jax.numpy as jnp
from jax import lax
from jax.experimental import pallas as pl
from jax.experimental.pallas import tpu as pltpu
from jax.sharding import PartitionSpec as P

HS_SMALL = 64
HS_LARGE = 128
GRID_W = 64
LOG2E = 1.4426950408889634
theta_base = 10000.0
norm_eps = 1e-06
return_lag = 5


def _send(src, dst, ssem, rsem, axis, dev):
    return pltpu.make_async_remote_copy(
        src_ref=src,
        dst_ref=dst,
        send_sem=ssem,
        recv_sem=rsem,
        device_id={axis: dev},
        device_id_type=pl.DeviceIdType.MESH,
    )


def attend_kernel(
    heads,
    kv_hbm,
    qt_ref,
    ws_hbm,
    wl_hbm,
    res_ref,
    gain_ref,
    att_ref,
    nrm_ref,
    rts_ref,
    kvbuf,
    wbuf,
    acc,
    mbuf,
    lbuf,
    hbuf,
    pbuf,
    xbuf,
    lsem,
    rsem,
    ssem,
    psem,
    xr,
    xs,
):
    n_sp = lax.axis_size("sp")
    n_z = n_sp // 2
    last = n_z // 2
    tok = kvbuf.shape[3]
    kv_rows = kvbuf.shape[2]
    sp = lax.axis_index("sp")
    tp = lax.axis_index("tp")
    right = lax.rem(sp + 2, n_sp)
    left = lax.rem(sp + n_sp - 2, n_sp)
    partner = sp + 1 - 2 * lax.rem(sp, 2)
    x_right = lax.rem(tp + 1, 4)
    x_left = lax.rem(tp + 3, 4)
    x_far = lax.rem(tp + 2, 4)

    own = pltpu.make_async_copy(kv_hbm, kvbuf.at[0, 0], lsem.at[0])
    own.start()
    w_copies = [
        pltpu.make_async_copy(ws_hbm, wbuf.at[pl.ds(0, 256)], lsem.at[1]),
        pltpu.make_async_copy(wl_hbm, wbuf.at[pl.ds(256, 256)], lsem.at[2]),
    ]
    for w in w_copies:
        w.start()

    barrier = pltpu.get_barrier_semaphore()
    for dev in (right, left, partner):
        pl.semaphore_signal(
            barrier, inc=1, device_id={"sp": dev}, device_id_type=pl.DeviceIdType.MESH
        )
    for dev in (x_right, x_left):
        pl.semaphore_signal(
            barrier, inc=1, device_id={"tp": dev}, device_id_type=pl.DeviceIdType.MESH
        )
    pl.semaphore_wait(barrier, 5)

    parts = (pl.ds(0, tok), pl.ds(tok, kv_rows - tok))

    def at(pair, side, part):
        return kvbuf.at[pair, side, parts[part]]

    def to_right(step, pair, part, dst_pair):
        return _send(
            at(pair, 0, part),
            at(dst_pair, 0, part),
            ssem.at[step, 0, part],
            rsem.at[dst_pair, 0, part],
            "sp",
            right,
        )

    def to_left(step, pair, part, dst_pair, src_side=1, dst_side=1):
        return _send(
            at(pair, src_side, part),
            at(dst_pair, dst_side, part),
            ssem.at[step, 1, part],
            rsem.at[dst_pair, dst_side, part],
            "sp",
            left,
        )

    def to_partner(pair, side, part, dst_pair, dst_side):
        return _send(
            at(pair, side, part),
            at(dst_pair, dst_side, part),
            psem.at[dst_pair, dst_side, part],
            rsem.at[dst_pair, dst_side, part],
            "sp",
            partner,
        )

    def arrived(pair, side, part):
        to_partner(pair, side, part, pair, side).wait_recv()

    own.wait()
    for part in range(2):
        to_right(1, 0, part, 1).start()
        to_left(1, 0, part, 1, src_side=0).start()
        to_partner(0, 0, part, 0, 1).start()

    acc[...] = jnp.zeros_like(acc)
    lbuf[...] = jnp.zeros_like(lbuf)
    mbuf[...] = jnp.full(mbuf.shape, -1e30, jnp.float32)

    def compute(pair):
        keys = kvbuf[pair, :, pl.ds(0, tok), :].reshape(2 * tok, tok)
        for h, (a0, rows, v0, scale) in enumerate(heads):
            s = jnp.dot(keys, qt_ref[h], preferred_element_type=jnp.float32)
            m_old = mbuf[h]
            m_new = jnp.maximum(m_old, jnp.max(s, axis=0, keepdims=True))
            p = jnp.exp2((s - m_new) * (scale * LOG2E))
            shrink = jnp.exp2((m_old - m_new) * (scale * LOG2E))
            mbuf[h] = m_new
            lbuf[h] = lbuf[h] * shrink + jnp.sum(p, axis=0, keepdims=True)
            pb = p.astype(jnp.bfloat16)
            pv = jnp.dot(
                kvbuf[pair, 0, pl.ds(tok + v0, rows), :],
                pb[:tok],
                preferred_element_type=jnp.float32,
            ) + jnp.dot(
                kvbuf[pair, 1, pl.ds(tok + v0, rows), :],
                pb[tok:],
                preferred_element_type=jnp.float32,
            )
            acc[pl.ds(a0, rows), :] = acc[pl.ds(a0, rows), :] * shrink + pv

    def turn(t, carry):
        step = t // 2 + 1
        phase = lax.rem(t, 2)
        pair = 2 * step - 1
        for part in range(2):

            @pl.when((phase == part) & (step < last))
            def _():
                for side in range(2):
                    arrived(pair, side, part)

                @pl.when(step < last - 1)
                def _():
                    to_right(step + 1, pair, part, pair + 2).start()
                    to_left(step + 1, pair, part, pair + 2).start()

                @pl.when(step == last - 1)
                def _():
                    if part == 0:
                        to_right(step + 1, pair, 0, 2 * last - 1).start()
                    else:
                        to_left(step + 1, pair, 1, 2 * last - 1, dst_side=0).start()

                for side in range(2):
                    to_partner(pair, side, part, pair + 1, side).start()

        @pl.when(t == 0)
        def _():
            for part in range(2):
                arrived(0, 1, part)

        @pl.when((phase == 0) & (t > 0))
        def _():
            for side in range(2):
                for part in range(2):
                    arrived(t, side, part)

        @pl.when(t == 2 * last - 1)
        def _():
            for part in range(2):
                arrived(2 * last - 1, 0, part)
                to_partner(2 * last - 1, 0, part, 2 * last - 1, 1).start()
            for part in range(2):
                arrived(2 * last - 1, 1, part)

        compute(t)
        return carry

    lax.fori_loop(0, 2 * last, turn, 0)

    for w in w_copies:
        w.wait()
    for h, (a0, rows, v0, scale) in enumerate(heads):
        heard = acc[pl.ds(a0, rows), :] / lbuf[h]
        acc[pl.ds(a0, rows), :] = heard
    heard = jnp.transpose(acc[...]).astype(jnp.bfloat16)
    block = tok // 4
    hbuf[...] = heard.reshape(4, block, heard.shape[1])

    def project(where, owner):
        pbuf[where] = jnp.dot(
            hbuf[owner], wbuf[...], preferred_element_type=jnp.float32
        ).astype(jnp.bfloat16)

    half = block // 2
    lo, hi = pl.ds(0, half), pl.ds(half, half)
    project(0, x_far)
    first_r = _send(pbuf.at[0, lo], xbuf.at[3, lo], xs.at[0], xr.at[0], "tp", x_right)
    first_l = _send(pbuf.at[0, hi], xbuf.at[3, hi], xs.at[1], xr.at[1], "tp", x_left)
    first_r.start()
    first_l.start()
    project(1, x_right)
    near_r = _send(pbuf.at[1], xbuf.at[0], xs.at[2], xr.at[2], "tp", x_right)
    near_r.start()
    project(2, x_left)
    near_l = _send(pbuf.at[2], xbuf.at[1], xs.at[3], xr.at[3], "tp", x_left)
    near_l.start()
    project(3, tp)
    first_r.wait_recv()
    pass_r = _send(xbuf.at[3, lo], xbuf.at[2, lo], xs.at[4], xr.at[4], "tp", x_right)
    pass_r.start()
    first_l.wait_recv()
    pass_l = _send(xbuf.at[3, hi], xbuf.at[2, hi], xs.at[5], xr.at[5], "tp", x_left)
    pass_l.start()

    for pair in range(2 * last):
        for side in range(2):
            rts_ref[pair, side] = kvbuf[pair, side, pl.ds(kv_rows - 16, 16), pl.ds(0, 128)]

    near_r.wait_recv()
    near_l.wait_recv()
    pass_r.wait_recv()
    pass_l.wait_recv()
    total = (
        pbuf[3].astype(jnp.float32)
        + xbuf[0].astype(jnp.float32)
        + xbuf[1].astype(jnp.float32)
        + xbuf[2].astype(jnp.float32)
    )
    attended = (res_ref[...].astype(jnp.float32) + total).astype(jnp.bfloat16)
    att_ref[...] = attended
    wide = attended.astype(jnp.float32)
    nrm_ref[...] = (
        wide
        * lax.rsqrt(jnp.mean(wide * wide, axis=-1, keepdims=True) + norm_eps)
        * gain_ref[...]
    ).astype(jnp.bfloat16)

    for c in (first_r, first_l, near_r, near_l, pass_r, pass_l):
        c.wait_send()
    for part in range(2):
        to_right(1, 0, part, 1).wait_send()
        to_left(1, 0, part, 1, src_side=0).wait_send()
        to_partner(0, 0, part, 0, 1).wait_send()

    def sent(step, carry):
        pair = 2 * step - 1
        for part in range(2):

            @pl.when(step < last - 1)
            def _():
                to_right(step + 1, pair, part, pair + 2).wait_send()
                to_left(step + 1, pair, part, pair + 2).wait_send()

            for side in range(2):
                to_partner(pair, side, part, pair + 1, side).wait_send()
        return carry

    lax.fori_loop(1, last, sent, 0)
    to_right(last, 2 * last - 3, 0, 2 * last - 1).wait_send()
    to_left(last, 2 * last - 3, 1, 2 * last - 1, dst_side=0).wait_send()
    for part in range(2):
        to_partner(2 * last - 1, 0, part, 2 * last - 1, 1).wait_send()


def attend(kv_block, queries_t, w_small, w_large, residual, gain, heads, n_sp):
    pairs = n_sp // 2
    kv_rows, tok = kv_block.shape
    width = residual.shape[1]
    rows = residual.shape[0]
    n_heads = queries_t.shape[0]
    vmem = pl.BlockSpec(memory_space=pltpu.VMEM)
    hbm = pl.BlockSpec(memory_space=pl.ANY)
    depth = w_small.shape[0] + w_large.shape[0]
    return pl.pallas_call(
        functools.partial(attend_kernel, heads),
        out_shape=(
            jax.ShapeDtypeStruct((rows, width), jnp.bfloat16),
            jax.ShapeDtypeStruct((rows, width), jnp.bfloat16),
            jax.ShapeDtypeStruct((pairs, 2, 16, 128), jnp.bfloat16),
        ),
        in_specs=[hbm, vmem, hbm, hbm, vmem, vmem],
        out_specs=(vmem, vmem, vmem),
        scratch_shapes=[
            pltpu.VMEM((pairs, 2, kv_rows, tok), jnp.bfloat16),
            pltpu.VMEM((depth, width), jnp.bfloat16),
            pltpu.VMEM((depth, tok), jnp.float32),
            pltpu.VMEM((n_heads, 1, tok), jnp.float32),
            pltpu.VMEM((n_heads, 1, tok), jnp.float32),
            pltpu.VMEM((4, tok // 4, depth), jnp.bfloat16),
            pltpu.VMEM((4, rows, width), jnp.bfloat16),
            pltpu.VMEM((4, rows, width), jnp.bfloat16),
            pltpu.SemaphoreType.DMA((3,)),
            pltpu.SemaphoreType.DMA((pairs, 2, 2)),
            pltpu.SemaphoreType.DMA((pairs // 2 + 1, 2, 2)),
            pltpu.SemaphoreType.DMA((pairs, 2, 2)),
            pltpu.SemaphoreType.DMA((6,)),
            pltpu.SemaphoreType.DMA((6,)),
        ],
        compiler_params=pltpu.CompilerParams(
            collective_id=0, has_side_effects=True, vmem_limit_bytes=48 * 1024 * 1024
        ),
        name="attend",
    )(kv_block, queries_t, w_small, w_large, residual, gain)


def experts_kernel(
    x_hbm,
    att_ref,
    sel_ref,
    perm_ref,
    pick_ref,
    share_ref,
    wg_hbm,
    wu_hbm,
    wd_hbm,
    out_ref,
    xbuf,
    wg,
    wu,
    wd,
    gbuf,
    pbuf,
    rbuf,
    fbuf,
    obuf,
    ret,
    lsem,
    rsem,
    ssem,
    psem,
    gr,
    gs,
    rr,
    rs,
    tr,
    ts,
):
    n_sp = lax.axis_size("sp")
    n_z = n_sp // 2
    last = n_z // 2
    sp = lax.axis_index("sp")
    tp = lax.axis_index("tp")
    z = sp // 2
    core = lax.rem(sp, 2)
    right = lax.rem(sp + 2, n_sp)
    left = lax.rem(sp + n_sp - 2, n_sp)
    partner = sp + 1 - 2 * core
    x_right = lax.rem(tp + 1, 4)
    x_left = lax.rem(tp + 3, 4)
    rows = xbuf.shape[2]

    own = pltpu.make_async_copy(x_hbm, xbuf.at[0, 0], lsem.at[0])
    own.start()
    w_copies = [
        pltpu.make_async_copy(a, b, lsem.at[1 + i])
        for i, (a, b) in enumerate(((wg_hbm, wg), (wu_hbm, wu), (wd_hbm, wd)))
    ]
    for w in w_copies:
        w.start()

    barrier = pltpu.get_barrier_semaphore()

    def greet(i, carry):
        pl.semaphore_signal(
            barrier,
            inc=1,
            device_id={"sp": lax.rem(sp + i, n_sp)},
            device_id_type=pl.DeviceIdType.MESH,
        )
        return carry

    lax.fori_loop(1, n_sp, greet, 0)
    for dev in (x_right, x_left):
        pl.semaphore_signal(
            barrier, inc=1, device_id={"tp": dev}, device_id_type=pl.DeviceIdType.MESH
        )
    pl.semaphore_wait(barrier, n_sp + 1)

    half = rows // 2
    parts = (pl.ds(0, half), pl.ds(half, half))

    def at(pair, side, part):
        return xbuf.at[pair, side, parts[part]]

    def to_right(step, pair, part, dst_pair):
        return _send(
            at(pair, 0, part),
            at(dst_pair, 0, part),
            ssem.at[step, 0, part],
            rsem.at[dst_pair, 0, part],
            "sp",
            right,
        )

    def to_left(step, pair, part, dst_pair, src_side=1, dst_side=1):
        return _send(
            at(pair, src_side, part),
            at(dst_pair, dst_side, part),
            ssem.at[step, 1, part],
            rsem.at[dst_pair, dst_side, part],
            "sp",
            left,
        )

    def to_partner(pair, side, part, dst_pair, dst_side):
        return _send(
            at(pair, side, part),
            at(dst_pair, dst_side, part),
            psem.at[dst_pair, dst_side, part],
            rsem.at[dst_pair, dst_side, part],
            "sp",
            partner,
        )

    def arrived(pair, side, part):
        to_partner(pair, side, part, pair, side).wait_recv()

    def share_right(c):
        return _send(gbuf.at[c, 0], gbuf.at[c, 1], gs.at[c, 0], gr.at[c, 0], "tp", x_right)

    def share_left(c):
        return _send(gbuf.at[c, 0], gbuf.at[c, 2], gs.at[c, 1], gr.at[c, 1], "tp", x_left)

    def pass_right(c):
        return _send(
            gbuf.at[c, 1, 0], gbuf.at[c, 3, 0], gs.at[c, 2], gr.at[c, 2], "tp", x_right
        )

    def pass_left(c):
        return _send(gbuf.at[c, 2, 1], gbuf.at[c, 3, 1], gs.at[c, 3], gr.at[c, 3], "tp", x_left)

    def far_right(c):
        return _send(pbuf.at[c, 3, 0], rbuf.at[c, 0], rs.at[c, 0], rr.at[c, 0], "tp", x_right)

    def far_left(c):
        return _send(pbuf.at[c, 3, 1], rbuf.at[c, 1], rs.at[c, 1], rr.at[c, 1], "tp", x_left)

    def near_right(c):
        return _send(pbuf.at[c, 2], fbuf.at[c, 0], rs.at[c, 2], rr.at[c, 2], "tp", x_right)

    def near_left(c):
        return _send(pbuf.at[c, 1], fbuf.at[c, 1], rs.at[c, 3], rr.at[c, 3], "tp", x_left)

    own.wait()
    for part in range(2):
        to_right(1, 0, part, 1).start()
        to_left(1, 0, part, 1, src_side=0).start()
        to_partner(0, 0, part, 0, 1).start()

    def run_experts(c):
        for e in range(2):
            x = gbuf[c, :, e].reshape(64, gbuf.shape[4])
            gate = jnp.dot(x, wg[e], preferred_element_type=jnp.float32)
            up = jnp.dot(x, wu[e], preferred_element_type=jnp.float32)
            active = (gate / (1.0 + jnp.exp(-gate)) * up).astype(jnp.bfloat16)
            term = jnp.dot(active, wd[e], preferred_element_type=jnp.float32)
            pbuf[c, :, e] = term.astype(jnp.bfloat16).reshape(4, 16, gbuf.shape[4])

    def gather_turn(c):
        step = c + 1
        pair = 2 * step - 1

        @pl.when(step < last)
        def _():
            for part in range(2):
                for side in range(2):
                    arrived(pair, side, part)

                @pl.when(step < last - 1)
                def _():
                    to_right(step + 1, pair, part, pair + 2).start()
                    to_left(step + 1, pair, part, pair + 2).start()

                @pl.when(step == last - 1)
                def _():
                    if part == 0:
                        to_right(step + 1, pair, 0, 2 * last - 1).start()
                    else:
                        to_left(step + 1, pair, 1, 2 * last - 1, dst_side=0).start()

                for side in range(2):
                    to_partner(pair, side, part, pair + 1, side).start()

        @pl.when(step == last)
        def _():
            for part in range(2):
                arrived(2 * last - 1, 0, part)
                to_partner(2 * last - 1, 0, part, 2 * last - 1, 1).start()

        @pl.when(c == 0)
        def _():
            for part in range(2):
                arrived(0, 1, part)

        @pl.when((c > 0) & (c < last))
        def _():
            for side in range(2):
                for part in range(2):
                    arrived(2 * c, side, part)

        @pl.when(step == last)
        def _():
            for part in range(2):
                arrived(2 * last - 1, 1, part)

        @pl.when(c < last)
        def _():
            tokens = xbuf[pl.ds(2 * c, 2)].reshape(4 * rows, xbuf.shape[3])
            chosen = jnp.dot(sel_ref[c], tokens, preferred_element_type=jnp.float32)
            gbuf[c, 0] = chosen.astype(jnp.bfloat16).reshape(2, 16, xbuf.shape[3])
            share_right(c).start()
            share_left(c).start()

        @pl.when((c >= 1) & (c < last + 1))
        def _():
            share_right(c - 1).wait_recv()
            pass_right(c - 1).start()
            share_left(c - 1).wait_recv()
            pass_left(c - 1).start()

        @pl.when(c == 2)
        def _():
            for w in w_copies:
                w.wait()

        @pl.when((c >= 2) & (c < last + 2))
        def _():
            pass_right(c - 2).wait_recv()
            pass_left(c - 2).wait_recv()
            run_experts(c - 2)

    def home(c, q):
        if q == 0:
            return lax.rem(z - c + n_z, n_z) * 2 + 1 - core, 2 * c, 0
        if q == 1:
            return lax.rem(z + c, n_z) * 2 + 1 - core, 2 * c, 1
        if q == 2:
            return lax.rem(z - c - 1 + n_z, n_z) * 2 + core, 2 * c + 1, 0
        return lax.rem(z + c + 1, n_z) * 2 + core, 2 * c + 1, 1

    def give(c, q):
        dev, pair, side = home(c, q)
        return _send(
            obuf.at[c, q], ret.at[pair, side], ts.at[c, q], tr.at[pair, side], "sp", dev
        )

    def give_last():
        dev = lax.rem(z + last, n_z) * 2 + 1 - core
        return _send(
            obuf.at[last - 1, 3],
            ret.at[2 * last - 1, 1],
            ts.at[last - 1, 3],
            tr.at[2 * last - 1, 1],
            "sp",
            dev,
        )

    width = fbuf.shape[4]

    def return_turn(i):
        @pl.when((i >= 1) & (i < last + 1))
        def _():
            c = i - 1
            far_right(c).wait_recv()
            pbuf[c, 2, 0] = (
                pbuf[c, 2, 0].astype(jnp.float32) + rbuf[c, 0].astype(jnp.float32)
            ).astype(jnp.bfloat16)
            near_right(c).start()
            far_left(c).wait_recv()
            pbuf[c, 1, 1] = (
                pbuf[c, 1, 1].astype(jnp.float32) + rbuf[c, 1].astype(jnp.float32)
            ).astype(jnp.bfloat16)
            near_left(c).start()

        @pl.when((i >= 0) & (i < last))
        def _():
            far_right(i).start()
            far_left(i).start()

        @pl.when(i >= 2)
        def _():
            c = i - 2
            near_right(c).wait_recv()
            near_left(c).wait_recv()
            total = (
                pbuf[c, 0].astype(jnp.float32)
                + fbuf[c, 0].astype(jnp.float32)
                + fbuf[c, 1].astype(jnp.float32)
            )
            total = total.astype(jnp.bfloat16).reshape(32, width)
            split = jnp.concatenate([total[:, : width // 2], total[:, width // 2 :]], axis=0)
            ordered = jnp.dot(perm_ref[...], split, preferred_element_type=jnp.float32)
            obuf[c] = ordered.astype(jnp.bfloat16).reshape(4, 16, width // 2)

            @pl.when(c > 0)
            def _():
                give(c, 0).start()

            @pl.when(c == 0)
            def _():
                ret[0, 0] = obuf[0, 0]

            give(c, 1).start()
            give(c, 2).start()

            @pl.when(c < last - 1)
            def _():
                give(c, 3).start()

            @pl.when(c == last - 1)
            def _():
                give_last().start()

    def turn(t, carry):
        gather_turn(t)
        return_turn(t - return_lag)
        return carry

    lax.fori_loop(0, last + return_lag + 2, turn, 0)

    for part in range(2):
        to_right(1, 0, part, 1).wait_send()
        to_left(1, 0, part, 1, src_side=0).wait_send()
        to_partner(0, 0, part, 0, 1).wait_send()

    def sent(step, carry):
        pair = 2 * step - 1
        for part in range(2):

            @pl.when(step < last - 1)
            def _():
                to_right(step + 1, pair, part, pair + 2).wait_send()
                to_left(step + 1, pair, part, pair + 2).wait_send()

            for side in range(2):
                to_partner(pair, side, part, pair + 1, side).wait_send()
        return carry

    lax.fori_loop(1, last, sent, 0)
    to_right(last, 2 * last - 3, 0, 2 * last - 1).wait_send()
    to_left(last, 2 * last - 3, 1, 2 * last - 1, dst_side=0).wait_send()
    for part in range(2):
        to_partner(2 * last - 1, 0, part, 2 * last - 1, 1).wait_send()

    def left_all(c, carry):
        for copy in (share_right, share_left, pass_right, pass_left):
            copy(c).wait_send()
        for copy in (far_right, far_left, near_right, near_left):
            copy(c).wait_send()
        return carry

    lax.fori_loop(0, last, left_all, 0)

    def came(i, carry):
        c = i

        @pl.when(c > 0)
        def _():
            give(c, 0).wait_recv()

        for q in (1, 2, 3):
            give(c, q).wait_recv()
        return carry

    lax.fori_loop(0, last, came, 0)

    back = ret[...].reshape(ret.shape[0] * 32, width // 2)
    picked = jnp.dot(pick_ref[...], back, preferred_element_type=jnp.float32)
    out = att_ref[...].astype(jnp.float32)
    lo = picked[:rows] * share_ref[:, 0:1] + picked[rows : 2 * rows] * share_ref[:, 1:2]
    hi = (
        picked[2 * rows : 3 * rows] * share_ref[:, 0:1]
        + picked[3 * rows :] * share_ref[:, 1:2]
    )
    out_ref[:, : width // 2] = (out[:, : width // 2] + lo).astype(jnp.bfloat16)
    out_ref[:, width // 2 :] = (out[:, width // 2 :] + hi).astype(jnp.bfloat16)

    def gone(c, carry):
        @pl.when(c > 0)
        def _():
            give(c, 0).wait_send()

        for q in (1, 2, 3):
            give(c, q).wait_send()
        return carry

    lax.fori_loop(0, last, gone, 0)


def run_layer_experts(normed, attended, sel, perm, pick, shares, gate, up, down, n_sp):
    pairs = n_sp // 2
    chunks = pairs // 2
    rows, width = normed.shape
    vmem = pl.BlockSpec(memory_space=pltpu.VMEM)
    hbm = pl.BlockSpec(memory_space=pl.ANY)
    bf16 = jnp.bfloat16
    dma = pltpu.SemaphoreType.DMA
    return pl.pallas_call(
        experts_kernel,
        out_shape=jax.ShapeDtypeStruct((rows, width), bf16),
        in_specs=[hbm, vmem, vmem, vmem, vmem, vmem, hbm, hbm, hbm],
        out_specs=vmem,
        scratch_shapes=[
            pltpu.VMEM((pairs, 2, rows, width), bf16),
            pltpu.VMEM(gate.shape, bf16),
            pltpu.VMEM(up.shape, bf16),
            pltpu.VMEM(down.shape, bf16),
            pltpu.VMEM((chunks, 4, 2, 16, width), bf16),
            pltpu.VMEM((chunks, 4, 2, 16, width), bf16),
            pltpu.VMEM((chunks, 2, 16, width), bf16),
            pltpu.VMEM((chunks, 2, 2, 16, width), bf16),
            pltpu.VMEM((chunks, 4, 16, width // 2), bf16),
            pltpu.VMEM((pairs, 2, 16, width // 2), bf16),
            dma((4,)),
            dma((pairs, 2, 2)),
            dma((chunks + 1, 2, 2)),
            dma((pairs, 2, 2)),
            dma((chunks, 4)),
            dma((chunks, 4)),
            dma((chunks, 4)),
            dma((chunks, 4)),
            dma((pairs, 2)),
            dma((chunks, 4)),
        ],
        compiler_params=pltpu.CompilerParams(
            collective_id=1, has_side_effects=True, vmem_limit_bytes=56 * 1024 * 1024
        ),
        name="experts",
    )(normed, attended, sel, perm, pick, shares, gate, up, down)


def experts_of(normed, attended, names_all, routes, route_scores, gate, up, down):
    n_sp = lax.axis_size("sp")
    n_z = n_sp // 2
    last = n_z // 2
    pairs = n_sp // 2
    chunks = pairs // 2
    rows = routes.shape[0]
    sp = lax.axis_index("sp")
    bf16 = jnp.bfloat16
    names = names_all[:, :, 0, :].reshape(n_sp, 2, rows)
    mine = (2 * sp + jnp.arange(2)).astype(bf16)
    member = jnp.any(names[:, None] == mine[None, :, None, None], axis=2)
    before = (jnp.arange(rows)[:, None] < jnp.arange(rows)[None, :]).astype(bf16)
    rank = jnp.einsum(
        "bet,tu->beu", member.astype(bf16), before, preferred_element_type=jnp.float32
    )
    seats = jnp.arange(4, dtype=jnp.float32)
    seated = member[:, :, None] & (rank[:, :, None] == seats[None, None, :, None])
    seated = seated.reshape(chunks, 4, 2, 4, rows).transpose(0, 2, 1, 3, 4)
    same_block = jnp.arange(4)[:, None, None, None] == jnp.arange(4)[None, None, :, None]
    sel = (seated[:, :, :, :, None] & same_block[None, None]).astype(bf16)
    sel = sel.reshape(chunks, 32, 4 * rows)
    out_row = jnp.arange(64)
    block, piece, slot = out_row // 16, (out_row // 8) % 2, out_row % 8
    in_row = piece * 32 + (slot // 4) * 16 + block * 4 + slot % 4
    perm = (in_row[:, None] == jnp.arange(64)[None, :]).astype(bf16)
    same = routes[:, :, None, None] == routes[None, None, :, :]
    earlier = jnp.arange(rows)[:, None, None, None] > jnp.arange(rows)[None, None, :, None]
    own_rank = jnp.sum((same & earlier).astype(jnp.int32), axis=(2, 3))
    host = routes // 2
    away = (sp // 2 - host // 2 + n_z) % n_z
    other = (host % 2 != sp % 2).astype(jnp.int32)
    step = jnp.minimum(away, n_z - away)
    edge = (away == 0) | (away == last)
    pair = jnp.where(away == 0, 0, jnp.where(away == last, 2 * last - 1, 2 * step - 1 + other))
    side = jnp.where(edge, other, (away < last).astype(jnp.int32))
    base = (pair * 2 + side) * 16 + (routes % 2) * 4 + own_rank
    seats_back = jnp.concatenate([base[:, 0], base[:, 1], base[:, 0] + 8, base[:, 1] + 8])
    pick = (seats_back[:, None] == jnp.arange(pairs * 32)[None, :]).astype(bf16)
    shares = route_scores / jnp.sum(route_scores, axis=1, keepdims=True)
    return run_layer_experts(
        normed, attended, sel, perm, pick, shares, gate, up, down, n_sp
    )


def grid_tables(offset, length, head_size):
    places = offset + jnp.arange(length, dtype=jnp.int32)
    grid_rows = (places // GRID_W).astype(jnp.float32)
    grid_cols = (places % GRID_W).astype(jnp.float32)
    rates = jnp.power(
        theta_base, -2.0 * jnp.arange(head_size // 4, dtype=jnp.float32) / (head_size // 2)
    )
    row_angles = grid_rows[:, None, None] * rates
    col_angles = grid_cols[:, None, None] * rates
    return (jnp.cos(row_angles), jnp.sin(row_angles), jnp.cos(col_angles), jnp.sin(col_angles))


def half_turn(segment, cosine, sine_part):
    half_size = segment.shape[-1] // 2
    leading = segment[..., :half_size]
    trailing = segment[..., half_size:]
    return jnp.concatenate(
        [leading * cosine - trailing * sine_part, trailing * cosine + leading * sine_part], axis=-1
    )


def grid_turn(vectors, tables):
    row_cos, row_sin, col_cos, col_sin = tables
    half_size = vectors.shape[-1] // 2
    return jnp.concatenate(
        [
            half_turn(vectors[..., :half_size], row_cos, row_sin),
            half_turn(vectors[..., half_size:], col_cos, col_sin),
        ],
        axis=-1,
    )


def normed_turn(raw_rows, gain, tables):
    widened = raw_rows.astype(jnp.float32)
    scaled = (
        widened * lax.rsqrt(jnp.mean(widened * widened, axis=-1, keepdims=True) + norm_eps) * gain
    )
    return grid_turn(scaled, tables).astype(jnp.bfloat16)


def on_device(
    queries_small,
    keys_small,
    values_small,
    queries_large,
    keys_large,
    values_large,
    query_gain_small,
    key_gain_small,
    query_gain_large,
    key_gain_large,
    residual_in,
    out_weight_small,
    out_weight_large,
    norm_gain,
    routes,
    route_scores,
    expert_gate,
    expert_up,
    expert_down,
):
    token_rows = queries_small.shape[0]
    offset = lax.axis_index("sp") * token_rows
    tables_small = grid_tables(offset, token_rows, HS_SMALL)
    tables_large = grid_tables(offset, token_rows, HS_LARGE)
    kv_small = keys_small.shape[1] // HS_SMALL
    kv_large = keys_large.shape[1] // HS_LARGE
    asked_small = normed_turn(
        queries_small.reshape(token_rows, -1, HS_SMALL), query_gain_small, tables_small
    )
    asked_large = normed_turn(
        queries_large.reshape(token_rows, -1, HS_LARGE), query_gain_large, tables_large
    )
    turned_small = normed_turn(
        keys_small.reshape(token_rows, kv_small, HS_SMALL), key_gain_small, tables_small
    ).reshape(token_rows, -1)
    turned_large = normed_turn(
        keys_large.reshape(token_rows, kv_large, HS_LARGE), key_gain_large, tables_large
    ).reshape(token_rows, -1)
    wide_small = turned_small.shape[1]
    width = wide_small + turned_large.shape[1]
    key_block = jnp.concatenate([turned_small, turned_large], axis=1)
    value_block = jnp.concatenate([values_small, values_large], axis=1).T
    names = routes.T.reshape(1, -1).astype(jnp.bfloat16)
    names = jnp.pad(names, ((0, 15), (0, token_rows - names.shape[1])))
    kv_block = jnp.concatenate([key_block, value_block, names], axis=0)
    heads, query_parts = [], []
    for asked, count, size, base in (
        (asked_small, kv_small, HS_SMALL, 0),
        (asked_large, kv_large, HS_LARGE, wide_small),
    ):
        by_head = jnp.transpose(asked, (1, 2, 0))
        ratio = asked.shape[1] // count
        for h in range(asked.shape[1]):
            at = base + (h // ratio) * size
            heads.append((base * 2 + h * size, size, at, size ** (-0.5)))
            query_parts.append(jnp.pad(by_head[h], ((at, width - at - size), (0, 0))))
    attended, normed, names_all = attend(
        kv_block,
        jnp.stack(query_parts),
        out_weight_small,
        out_weight_large,
        residual_in,
        norm_gain.reshape(1, -1),
        tuple(heads),
        lax.axis_size("sp"),
    )
    return experts_of(
        normed,
        attended,
        names_all,
        routes,
        route_scores,
        expert_gate,
        expert_up,
        expert_down,
    )


def solution(mesh):
    in_specs = (
        P(("grp", "sp"), "tp"),
        P(("grp", "sp"), "tp"),
        P(("grp", "sp"), "tp"),
        P(("grp", "sp"), "tp"),
        P(("grp", "sp"), "tp"),
        P(("grp", "sp"), "tp"),
        P("grp"),
        P("grp"),
        P("grp"),
        P("grp"),
        P(("grp", "sp", "tp"), None),
        P("tp", None),
        P("tp", None),
        P(),
        P(("grp", "sp", "tp"), None),
        P(("grp", "sp", "tp"), None),
        P("sp", None, "tp"),
        P("sp", None, "tp"),
        P("sp", "tp", None),
    )
    out_specs = P(("grp", "sp", "tp"), None)
    return jax.shard_map(
        on_device, mesh=mesh, in_specs=in_specs, out_specs=out_specs, check_vma=False
    )
```

```python
import functools
import jax
import jax.numpy as jnp
import numpy as np
from jax import lax
from jax.experimental import pallas as pl
from jax.experimental.pallas import tpu as pltpu
from jax.sharding import PartitionSpec as P

HS_SMALL = 64
HS_LARGE = 128
GRID_W = 64
LANES = 128
LOG2E = 1.4426950408889634
theta_base = 10000.0
norm_eps = 1e-06
SEATS = 4
MESH = pl.DeviceIdType.MESH
BF16 = jnp.bfloat16
F32 = jnp.float32


def _send(src, dst, ssem, rsem, axis, dev):
    return pltpu.make_async_remote_copy(
        src_ref=src,
        dst_ref=dst,
        send_sem=ssem,
        recv_sem=rsem,
        device_id={axis: dev},
        device_id_type=MESH,
    )


def _iota(shape, dim):
    return lax.broadcasted_iota(jnp.int32, shape, dim)


class Ring:
    def __init__(self, buf, parts, ssem, rsem, psem, right, left, partner, last):
        self.buf, self.parts, self.last = buf, parts, last
        self.ssem, self.rsem, self.psem = ssem, rsem, psem
        self.right, self.left, self.partner = right, left, partner

    def at(self, pair, side, part):
        return self.buf.at[pair, side, self.parts[part]]

    def to_right(self, step, pair, part, dst_pair):
        return _send(
            self.at(pair, 0, part),
            self.at(dst_pair, 0, part),
            self.ssem.at[step, 0, part],
            self.rsem.at[dst_pair, 0, part],
            "sp",
            self.right,
        )

    def to_left(self, step, pair, part, dst_pair, src_side=1, dst_side=1):
        return _send(
            self.at(pair, src_side, part),
            self.at(dst_pair, dst_side, part),
            self.ssem.at[step, 1, part],
            self.rsem.at[dst_pair, dst_side, part],
            "sp",
            self.left,
        )

    def to_partner(self, pair, side, part, dst_pair, dst_side):
        return _send(
            self.at(pair, side, part),
            self.at(dst_pair, dst_side, part),
            self.psem.at[dst_pair, dst_side, part],
            self.rsem.at[dst_pair, dst_side, part],
            "sp",
            self.partner,
        )

    def arrived(self, pair, side, part):
        self.to_partner(pair, side, part, pair, side).wait_recv()

    def first(self, part):
        return (
            self.to_right(1, 0, part, 1),
            self.to_left(1, 0, part, 1, src_side=0),
            self.to_partner(0, 0, part, 0, 1),
        )

    def begin(self, part):
        for copy in self.first(part):
            copy.start()

    def pass_on(self, step, part):
        pair, last = 2 * step - 1, self.last
        for side in range(2):
            self.arrived(pair, side, part)

        @pl.when(step < last - 1)
        def _():
            self.to_right(step + 1, pair, part, pair + 2).start()
            self.to_left(step + 1, pair, part, pair + 2).start()

        @pl.when(step == last - 1)
        def _():
            if part == 0:
                self.to_right(step + 1, pair, 0, 2 * last - 1).start()
            else:
                self.to_left(step + 1, pair, 1, 2 * last - 1, dst_side=0).start()

        for side in range(2):
            self.to_partner(pair, side, part, pair + 1, side).start()

    def opposite(self):
        pair = 2 * self.last - 1
        for part in range(2):
            self.arrived(pair, 0, part)
            self.to_partner(pair, 0, part, pair, 1).start()

    def opposite_partner(self):
        for part in range(2):
            self.arrived(2 * self.last - 1, 1, part)

    def finish(self):
        last = self.last
        for part in range(2):
            for copy in self.first(part):
                copy.wait_send()

        def sent(step, carry):
            pair = 2 * step - 1
            for part in range(2):

                @pl.when(step < last - 1)
                def _():
                    self.to_right(step + 1, pair, part, pair + 2).wait_send()
                    self.to_left(step + 1, pair, part, pair + 2).wait_send()

                for side in range(2):
                    self.to_partner(pair, side, part, pair + 1, side).wait_send()
            return carry

        lax.fori_loop(1, last, sent, 0)
        self.to_right(last, 2 * last - 3, 0, 2 * last - 1).wait_send()
        self.to_left(last, 2 * last - 3, 1, 2 * last - 1, dst_side=0).wait_send()
        for part in range(2):
            self.to_partner(2 * last - 1, 0, part, 2 * last - 1, 1).wait_send()


def layer_kernel(
    heads,
    qs_ref,
    ks_ref,
    vs_ref,
    ql_ref,
    kl_ref,
    vl_ref,
    gqs_ref,
    gks_ref,
    gql_ref,
    gkl_ref,
    col_hbm,
    row_hbm,
    ws_hbm,
    wl_hbm,
    res_ref,
    gain_ref,
    names_ref,
    score_ref,
    wg_hbm,
    wu_hbm,
    wd_hbm,
    out_ref,
    kvbuf,
    qt,
    coltab,
    rowtab,
    tabs,
    wbuf,
    acc,
    mbuf,
    lbuf,
    hbuf,
    cbuf,
    dbuf,
    abuf,
    xbuf,
    wg,
    wu,
    wd,
    gbuf,
    pbuf,
    rbuf,
    fbuf,
    obuf,
    ret,
    below,
    perm,
    pick,
    lsem,
    rsem,
    ssem,
    psem,
    xr,
    xs,
    rsem2,
    ssem2,
    psem2,
    gr,
    gs,
    rr,
    rs,
    tr,
    ts,
):
    n_sp = lax.axis_size("sp")
    n_z = n_sp // 2
    last = n_z // 2
    tok = kvbuf.shape[3]
    kv_rows = kvbuf.shape[2]
    rows, width = res_ref.shape
    sp = lax.axis_index("sp")
    tp = lax.axis_index("tp")
    z = sp // 2
    core = lax.rem(sp, 2)
    right = lax.rem(sp + 2, n_sp)
    left = lax.rem(sp + n_sp - 2, n_sp)
    partner = sp + 1 - 2 * core
    x_right = lax.rem(tp + 1, 4)
    x_left = lax.rem(tp + 3, 4)
    x_far = lax.rem(tp + 2, 4)
    grid_rows = tok // GRID_W

    loads = [
        pltpu.make_async_copy(a, b, lsem.at[i])
        for i, (a, b) in enumerate(
            (
                (col_hbm, coltab),
                (row_hbm.at[pl.ds(sp * grid_rows, grid_rows)], rowtab),
                (ws_hbm, wbuf.at[pl.ds(0, ws_hbm.shape[0])]),
                (wl_hbm, wbuf.at[pl.ds(ws_hbm.shape[0], wl_hbm.shape[0])]),
                (wg_hbm, wg),
                (wu_hbm, wu),
                (wd_hbm, wd),
            )
        )
    ]
    loads[0].start()
    loads[1].start()

    barrier = pltpu.get_barrier_semaphore()

    def greet(i, carry):
        pl.semaphore_signal(
            barrier, inc=1, device_id={"sp": lax.rem(sp + i, n_sp)}, device_id_type=MESH
        )
        return carry

    lax.fori_loop(1, n_sp, greet, 0)
    for dev in (x_right, x_left):
        pl.semaphore_signal(barrier, inc=1, device_id={"tp": dev}, device_id_type=MESH)

    ring = Ring(
        kvbuf,
        (pl.ds(0, tok), pl.ds(tok, kv_rows - tok)),
        ssem,
        rsem,
        psem,
        right,
        left,
        partner,
        last,
    )
    tokens = Ring(
        xbuf,
        (pl.ds(0, rows // 2), pl.ds(rows // 2, rows // 2)),
        ssem2,
        rsem2,
        psem2,
        right,
        left,
        partner,
        last,
    )

    lane = _iota((tok, LANES), 1)

    def turned(raw, gain, table, size):
        x = raw.astype(F32)
        square = x * x
        if size < LANES:
            lower = lane < size
            mean = jnp.where(
                lower,
                jnp.sum(jnp.where(lower, square, 0.0), axis=1, keepdims=True),
                jnp.sum(jnp.where(lower, 0.0, square), axis=1, keepdims=True),
            ) * (1.0 / size)
            gain = jnp.concatenate([gain, gain], axis=1)
        else:
            mean = jnp.sum(square, axis=1, keepdims=True) * (1.0 / size)
        x = x * lax.rsqrt(mean + norm_eps) * gain
        quarter = size // 4
        swapped = jnp.where(
            lane % (2 * quarter) < quarter,
            pltpu.roll(x, LANES - quarter, 1),
            pltpu.roll(x, quarter, 1),
        )
        return x * tabs[table] + swapped * tabs[table + 1]

    kvbuf[0, 0, pl.ds(tok, LANES), :] = jnp.transpose(vs_ref[...].astype(F32)).astype(BF16)
    kvbuf[0, 0, pl.ds(tok + LANES, LANES), :] = jnp.transpose(vl_ref[...].astype(F32)).astype(BF16)
    names = names_ref[...].astype(F32)
    repeat = (_iota((16, 2), 0) % 2 == _iota((16, 2), 1)).astype(BF16)
    named = jnp.dot(repeat, names.astype(BF16), preferred_element_type=F32).astype(BF16)
    spread = (_iota((rows, tok), 1) % rows == _iota((rows, tok), 0)).astype(BF16)
    named = jnp.dot(named, spread, preferred_element_type=F32)
    own_lane = _iota((16, tok), 1) // rows == _iota((16, tok), 0) // 2
    kvbuf[0, 0, pl.ds(2 * tok, 16), :] = jnp.where(own_lane, named, 0.0).astype(BF16)

    loads[0].wait()
    loads[1].wait()
    for i in range(4):
        for g in range(grid_rows):
            tabs[i, pl.ds(g * GRID_W, GRID_W), :] = coltab[i] + rowtab[g, pl.ds(i, 1), :]
    kvbuf[0, 0, pl.ds(0, tok), pl.ds(0, LANES)] = turned(
        ks_ref[...], gks_ref[...], 0, HS_SMALL
    ).astype(BF16)
    kvbuf[0, 0, pl.ds(0, tok), pl.ds(LANES, LANES)] = turned(
        kl_ref[...], gkl_ref[...], 2, HS_LARGE
    ).astype(BF16)

    pl.semaphore_wait(barrier, n_sp + 1)
    for part in range(2):
        ring.begin(part)
    for load in loads[2:]:
        load.start()

    qt[...] = jnp.zeros_like(qt)
    h = 0
    for ref, gain_of, table, size, base in (
        (qs_ref, gqs_ref, 0, HS_SMALL, 0),
        (ql_ref, gql_ref, 2, HS_LARGE, LANES),
    ):
        for i in range(ref.shape[1] // LANES):
            flipped = jnp.transpose(
                turned(ref[:, pl.ds(i * LANES, LANES)], gain_of[...], table, size)
            ).astype(BF16)
            for j in range(LANES // size):
                at = base + (h - base // LANES * 4) // 2 * size
                qt[h, pl.ds(at, size), :] = flipped[j * size : (j + 1) * size]
                h += 1

    acc[...] = jnp.zeros_like(acc)
    lbuf[...] = jnp.zeros_like(lbuf)
    mbuf[...] = jnp.full(mbuf.shape, -1e30, F32)

    below[...] = (
        (_iota((tok, tok), 0) < _iota((tok, tok), 1))
        & (_iota((tok, tok), 0) // rows == _iota((tok, tok), 1) // rows)
    ).astype(BF16)
    out_row = _iota((64, 64), 0)
    in_row = (
        (out_row // 8) % 2 * 32 + (out_row % 8) // SEATS * 16 + out_row // 16 * SEATS
    ) + out_row % SEATS
    perm[...] = (in_row == _iota((64, 64), 1)).astype(BF16)
    eye = (_iota((rows, rows), 0) == _iota((rows, rows), 1)).astype(BF16)
    columns = lax.dot_general(
        eye, names.astype(BF16), (((1,), (1,)), ((), ())), preferred_element_type=F32
    )
    earlier = _iota((rows, rows), 1) < _iota((rows, rows), 0)
    for k in range(2):
        column = columns[:, k : k + 1]
        same = ((column == names[0:1, :]) | (column == names[1:2, :])) & earlier
        rank = jnp.sum(same.astype(F32), axis=1, keepdims=True).astype(jnp.int32)
        expert = column.astype(jnp.int32)
        host = expert // 2
        away = z - host // 2
        away = jnp.where(away < 0, away + n_z, away)
        other = (host % 2 != core).astype(jnp.int32)
        step = jnp.minimum(away, n_z - away)
        edge = (away == 0) | (away == last)
        pair = jnp.where(
            away == 0, 0, jnp.where(away == last, 2 * last - 1, 2 * step - 1 + other)
        )
        side = jnp.where(edge, other, (away < last).astype(jnp.int32))
        base = (pair * 2 + side) * 16 + expert % 2 * SEATS + rank
        seat = _iota((rows, pick.shape[1]), 1)
        pick[pl.ds(k * rows, rows), :] = (seat == base).astype(BF16)
        pick[pl.ds((2 + k) * rows, rows), :] = (seat == base + 8).astype(BF16)

    def attend(pair):
        keys = kvbuf[pair, :, pl.ds(0, tok), :].reshape(2 * tok, tok)
        for h, (a0, size, v0, scale) in enumerate(heads):
            s = jnp.dot(keys, qt[h], preferred_element_type=F32)
            m_old = mbuf[h]
            m_new = jnp.maximum(m_old, jnp.max(s, axis=0, keepdims=True))
            p = jnp.exp2((s - m_new) * (scale * LOG2E))
            shrink = jnp.exp2((m_old - m_new) * (scale * LOG2E))
            mbuf[h] = m_new
            lbuf[h] = lbuf[h] * shrink + jnp.sum(p, axis=0, keepdims=True)
            pb = p.astype(BF16)
            pv = jnp.dot(
                kvbuf[pair, 0, pl.ds(tok + v0, size), :],
                pb[:tok],
                preferred_element_type=F32,
            ) + jnp.dot(
                kvbuf[pair, 1, pl.ds(tok + v0, size), :],
                pb[tok:],
                preferred_element_type=F32,
            )
            acc[pl.ds(a0, size), :] = acc[pl.ds(a0, size), :] * shrink + pv

    def attend_turn(t, carry):
        step = t // 2 + 1
        phase = lax.rem(t, 2)
        for part in range(2):

            @pl.when((phase == part) & (step < last))
            def _():
                ring.pass_on(step, part)

        @pl.when(t == 0)
        def _():
            for part in range(2):
                ring.arrived(0, 1, part)

        @pl.when((phase == 0) & (t > 0))
        def _():
            for side in range(2):
                for part in range(2):
                    ring.arrived(t, side, part)

        @pl.when(t == 2 * last - 1)
        def _():
            ring.opposite()
            ring.opposite_partner()

        attend(t)
        return carry

    lax.fori_loop(0, 2 * last, attend_turn, 0)

    loads[2].wait()
    loads[3].wait()
    for h, (a0, size, v0, scale) in enumerate(heads):
        acc[pl.ds(a0, size), :] = acc[pl.ds(a0, size), :] / lbuf[h]
    heard = jnp.transpose(acc[...]).astype(BF16)
    hbuf[...] = heard.reshape(4, rows, heard.shape[1])

    def project(where, owner):
        cbuf[where] = jnp.dot(hbuf[owner], wbuf[...], preferred_element_type=F32).astype(BF16)

    lo, hi = pl.ds(0, rows // 2), pl.ds(rows // 2, rows // 2)
    project(0, x_far)
    first_r = _send(cbuf.at[0, lo], dbuf.at[3, lo], xs.at[0], xr.at[0], "tp", x_right)
    first_l = _send(cbuf.at[0, hi], dbuf.at[3, hi], xs.at[1], xr.at[1], "tp", x_left)
    first_r.start()
    first_l.start()
    project(1, x_right)
    near_r = _send(cbuf.at[1], dbuf.at[0], xs.at[2], xr.at[2], "tp", x_right)
    near_r.start()
    project(2, x_left)
    near_l = _send(cbuf.at[2], dbuf.at[1], xs.at[3], xr.at[3], "tp", x_left)
    near_l.start()
    project(3, tp)
    first_r.wait_recv()
    pass_r = _send(dbuf.at[3, lo], dbuf.at[2, lo], xs.at[4], xr.at[4], "tp", x_right)
    pass_r.start()
    first_l.wait_recv()
    pass_l = _send(dbuf.at[3, hi], dbuf.at[2, hi], xs.at[5], xr.at[5], "tp", x_left)
    pass_l.start()
    ring.finish()
    near_r.wait_recv()
    near_l.wait_recv()
    pass_r.wait_recv()
    pass_l.wait_recv()
    for part, half in enumerate((lo, hi)):
        total = (
            cbuf[3, half].astype(F32)
            + dbuf[0, half].astype(F32)
            + dbuf[1, half].astype(F32)
            + dbuf[2, half].astype(F32)
        )
        attended = (res_ref[half].astype(F32) + total).astype(BF16)
        abuf[half] = attended
        wide = attended.astype(F32)
        xbuf[0, 0, half] = (
            wide
            * lax.rsqrt(jnp.mean(wide * wide, axis=-1, keepdims=True) + norm_eps)
            * gain_ref[...]
        ).astype(BF16)
        tokens.begin(part)
    for c in (first_r, first_l, near_r, near_l, pass_r, pass_l):
        c.wait_send()

    def share_right(c):
        return _send(gbuf.at[c, 0], gbuf.at[c, 1], gs.at[c, 0], gr.at[c, 0], "tp", x_right)

    def share_left(c):
        return _send(gbuf.at[c, 0], gbuf.at[c, 2], gs.at[c, 1], gr.at[c, 1], "tp", x_left)

    def pass_right(c):
        return _send(
            gbuf.at[c, 1, 0], gbuf.at[c, 3, 0], gs.at[c, 2], gr.at[c, 2], "tp", x_right
        )

    def pass_left(c):
        return _send(gbuf.at[c, 2, 1], gbuf.at[c, 3, 1], gs.at[c, 3], gr.at[c, 3], "tp", x_left)

    def far_right(c):
        return _send(pbuf.at[c, 3, 0], rbuf.at[c, 0], rs.at[c, 0], rr.at[c, 0], "tp", x_right)

    def far_left(c):
        return _send(pbuf.at[c, 3, 1], rbuf.at[c, 1], rs.at[c, 1], rr.at[c, 1], "tp", x_left)

    def near_right(c):
        return _send(pbuf.at[c, 2], fbuf.at[c, 0], rs.at[c, 2], rr.at[c, 2], "tp", x_right)

    def near_left(c):
        return _send(pbuf.at[c, 1], fbuf.at[c, 1], rs.at[c, 3], rr.at[c, 3], "tp", x_left)

    def seats_of(c):
        row = _iota((16, tok), 0)
        kept = jnp.zeros((16, tok), F32)
        for q in range(4):
            block = kvbuf[2 * c + q // 2, q % 2, pl.ds(2 * tok, 16), :].astype(F32)
            kept = jnp.where(row // 2 == q, block, kept)
        name0 = jnp.sum(jnp.where(row % 2 == 0, kept, 0.0), axis=0, keepdims=True)
        name1 = jnp.sum(jnp.where(row % 2 == 1, kept, 0.0), axis=0, keepdims=True)
        wide_row = _iota((32, tok), 0)
        mine = (2 * sp + wide_row // 16).astype(F32)
        member = (name0 == mine) | (name1 == mine)
        rank = jnp.dot(member.astype(F32).astype(BF16), below[...], preferred_element_type=F32)
        seated = (
            member
            & (rank == (wide_row % SEATS).astype(F32))
            & (_iota((32, tok), 1) // rows == wide_row % 16 // SEATS)
        )
        return seated.astype(F32).astype(BF16)

    def run_experts(c):
        for e in range(2):
            x = gbuf[c, :, e].reshape(64, width)
            gate = jnp.dot(x, wg[e], preferred_element_type=F32)
            up = jnp.dot(x, wu[e], preferred_element_type=F32)
            active = (gate / (1.0 + jnp.exp(-gate)) * up).astype(BF16)
            term = jnp.dot(active, wd[e], preferred_element_type=F32)
            pbuf[c, :, e] = term.astype(BF16).reshape(4, 16, width)

    def gather_turn(c):
        step = c + 1

        @pl.when(step < last)
        def _():
            for part in range(2):
                tokens.pass_on(step, part)

        @pl.when(step == last)
        def _():
            tokens.opposite()

        @pl.when(c == 0)
        def _():
            for part in range(2):
                tokens.arrived(0, 1, part)

        @pl.when((c > 0) & (c < last))
        def _():
            for side in range(2):
                for part in range(2):
                    tokens.arrived(2 * c, side, part)

        @pl.when(step == last)
        def _():
            tokens.opposite_partner()

        @pl.when(c < last)
        def _():
            block = xbuf[pl.ds(2 * c, 2)].reshape(4 * rows, width)
            chosen = jnp.dot(seats_of(c), block, preferred_element_type=F32)
            gbuf[c, 0] = chosen.astype(BF16).reshape(2, 16, width)
            share_right(c).start()
            share_left(c).start()

        @pl.when((c >= 1) & (c < last + 1))
        def _():
            share_right(c - 1).wait_recv()
            pass_right(c - 1).start()
            share_left(c - 1).wait_recv()
            pass_left(c - 1).start()

        @pl.when(c == 2)
        def _():
            for load in loads[4:]:
                load.wait()

        @pl.when((c >= 2) & (c < last + 2))
        def _():
            pass_right(c - 2).wait_recv()
            pass_left(c - 2).wait_recv()
            run_experts(c - 2)

    def home(c, q):
        if q == 0:
            return lax.rem(z - c + n_z, n_z) * 2 + 1 - core, 2 * c, 0
        if q == 1:
            return lax.rem(z + c, n_z) * 2 + 1 - core, 2 * c, 1
        if q == 2:
            return lax.rem(z - c - 1 + n_z, n_z) * 2 + core, 2 * c + 1, 0
        return lax.rem(z + c + 1, n_z) * 2 + core, 2 * c + 1, 1

    def give(c, q):
        dev, pair, side = home(c, q)
        return _send(
            obuf.at[c, q], ret.at[pair, side], ts.at[c, q], tr.at[pair, side], "sp", dev
        )

    def give_last():
        dev = lax.rem(z + last, n_z) * 2 + 1 - core
        return _send(
            obuf.at[last - 1, 3],
            ret.at[2 * last - 1, 1],
            ts.at[last - 1, 3],
            tr.at[2 * last - 1, 1],
            "sp",
            dev,
        )

    def order(i):
        half = last // 2
        late = i // half
        return (1 - late) * (i + half) + late * (last - 1 - i)

    def return_turn(i):
        @pl.when((i >= 1) & (i < last + 1))
        def _():
            c = order(i - 1)
            far_right(c).wait_recv()
            pbuf[c, 2, 0] = (pbuf[c, 2, 0].astype(F32) + rbuf[c, 0].astype(F32)).astype(BF16)
            near_right(c).start()
            far_left(c).wait_recv()
            pbuf[c, 1, 1] = (pbuf[c, 1, 1].astype(F32) + rbuf[c, 1].astype(F32)).astype(BF16)
            near_left(c).start()

        @pl.when((i >= 0) & (i < last))
        def _():
            c = order(i)
            far_right(c).start()
            far_left(c).start()

        @pl.when(i >= 2)
        def _():
            c = order(i - 2)
            near_right(c).wait_recv()
            near_left(c).wait_recv()
            total = pbuf[c, 0].astype(F32) + fbuf[c, 0].astype(F32) + fbuf[c, 1].astype(F32)
            total = total.astype(BF16).reshape(32, width)
            split = jnp.concatenate([total[:, : width // 2], total[:, width // 2 :]], axis=0)
            ordered = jnp.dot(perm[...], split, preferred_element_type=F32)
            obuf[c] = ordered.astype(BF16).reshape(4, 16, width // 2)

            @pl.when(c > 0)
            def _():
                give(c, 0).start()

            @pl.when(c == 0)
            def _():
                ret[0, 0] = obuf[0, 0]

            give(c, 1).start()
            give(c, 2).start()

            @pl.when(c < last - 1)
            def _():
                give(c, 3).start()

            @pl.when(c == last - 1)
            def _():
                give_last().start()

    def turn(t, carry):
        gather_turn(t)
        return_turn(t - (last - 1))
        return carry

    lax.fori_loop(0, 2 * last + 1, turn, 0)

    tokens.finish()

    def left_all(c, carry):
        for copy in (share_right, share_left, pass_right, pass_left):
            copy(c).wait_send()
        for copy in (far_right, far_left, near_right, near_left):
            copy(c).wait_send()
        return carry

    lax.fori_loop(0, last, left_all, 0)

    def came(c, carry):
        @pl.when(c > 0)
        def _():
            give(c, 0).wait_recv()

        for q in (1, 2, 3):
            give(c, q).wait_recv()
        return carry

    lax.fori_loop(0, last, came, 0)

    back = ret[...].reshape(ret.shape[0] * 32, width // 2)
    picked = jnp.dot(pick[...], back, preferred_element_type=F32)
    scores = score_ref[...]
    scores = scores / (scores[:, 0:1] + scores[:, 1:2])
    one, two = scores[:, 0:1], scores[:, 1:2]
    out = abuf[...].astype(F32)
    lower = picked[:rows] * one + picked[rows : 2 * rows] * two
    upper = picked[2 * rows : 3 * rows] * one + picked[3 * rows :] * two
    out_ref[:, : width // 2] = (out[:, : width // 2] + lower).astype(BF16)
    out_ref[:, width // 2 :] = (out[:, width // 2 :] + upper).astype(BF16)

    def gone(c, carry):
        @pl.when(c > 0)
        def _():
            give(c, 0).wait_send()

        for q in (1, 2, 3):
            give(c, q).wait_send()
        return carry

    lax.fori_loop(0, last, gone, 0)


def turn_tables(places, size, by_row):
    lane = np.arange(LANES) % size
    quarter = size // 4
    rates = np.power(
        np.float32(theta_base), (-2.0 * np.arange(quarter) / (size // 2)).astype(np.float32)
    ).astype(np.float32)
    angles = (places[:, None].astype(np.float32) * rates[lane % quarter]).astype(np.float32)
    here = (lane < size // 2) if by_row else (lane >= size // 2)
    sign = np.where(lane % (2 * quarter) < quarter, -1.0, 1.0)
    cosine = np.where(here, np.cos(angles), 0.0)
    sine = np.where(here, np.sin(angles) * sign, 0.0)
    return cosine.astype(np.float32), sine.astype(np.float32)


def on_device(
    queries_small,
    keys_small,
    values_small,
    queries_large,
    keys_large,
    values_large,
    query_gain_small,
    key_gain_small,
    query_gain_large,
    key_gain_large,
    residual_in,
    out_weight_small,
    out_weight_large,
    norm_gain,
    routes,
    route_scores,
    expert_gate,
    expert_up,
    expert_down,
):
    tok = queries_small.shape[0]
    rows, width = residual_in.shape
    n_sp = lax.axis_size("sp")
    pairs = n_sp // 2
    chunks = pairs // 2
    depth = out_weight_small.shape[0] + out_weight_large.shape[0]
    kv_rows = 2 * tok + 16
    grid_rows = tok // GRID_W
    row_places = np.arange(n_sp * grid_rows)
    col_places = np.arange(GRID_W)
    row_tables, col_tables = [], []
    for size in (HS_SMALL, HS_LARGE):
        row_tables.extend(turn_tables(row_places, size, True))
        col_tables.extend(turn_tables(col_places, size, False))
    heads = []
    wide_small = keys_small.shape[1]
    for count, kv_count, size, a0, v0 in (
        (queries_small.shape[1] // HS_SMALL, wide_small // HS_SMALL, HS_SMALL, 0, 0),
        (
            queries_large.shape[1] // HS_LARGE,
            keys_large.shape[1] // HS_LARGE,
            HS_LARGE,
            queries_small.shape[1],
            wide_small,
        ),
    ):
        for h in range(count):
            kv = h // (count // kv_count)
            heads.append((a0 + h * size, size, v0 + kv * size, size ** (-0.5)))
    vmem = pl.BlockSpec(memory_space=pltpu.VMEM)
    hbm = pl.BlockSpec(memory_space=pl.ANY)
    dma = pltpu.SemaphoreType.DMA
    V = pltpu.VMEM
    return pl.pallas_call(
        functools.partial(layer_kernel, tuple(heads)),
        out_shape=jax.ShapeDtypeStruct((rows, width), BF16),
        in_specs=[vmem] * 10 + [hbm] * 4 + [vmem] * 4 + [hbm] * 3,
        out_specs=vmem,
        scratch_shapes=[
            V((pairs, 2, kv_rows, tok), BF16),
            V((len(heads), tok, tok), BF16),
            V((4, GRID_W, LANES), F32),
            V((grid_rows, 4, LANES), F32),
            V((4, tok, LANES), F32),
            V((depth, width), BF16),
            V((depth, tok), F32),
            V((len(heads), 1, tok), F32),
            V((len(heads), 1, tok), F32),
            V((4, rows, depth), BF16),
            V((4, rows, width), BF16),
            V((4, rows, width), BF16),
            V((rows, width), BF16),
            V((pairs, 2, rows, width), BF16),
            V(expert_gate.shape, BF16),
            V(expert_up.shape, BF16),
            V(expert_down.shape, BF16),
            V((chunks, 4, 2, 16, width), BF16),
            V((chunks, 4, 2, 16, width), BF16),
            V((chunks, 2, 16, width), BF16),
            V((chunks, 2, 2, 16, width), BF16),
            V((chunks, 4, 16, width // 2), BF16),
            V((pairs, 2, 16, width // 2), BF16),
            V((tok, tok), BF16),
            V((64, 64), BF16),
            V((4 * rows, pairs * 32), BF16),
            dma((7,)),
            dma((pairs, 2, 2)),
            dma((chunks + 1, 2, 2)),
            dma((pairs, 2, 2)),
            dma((6,)),
            dma((6,)),
            dma((pairs, 2, 2)),
            dma((chunks + 1, 2, 2)),
            dma((pairs, 2, 2)),
            dma((chunks, 4)),
            dma((chunks, 4)),
            dma((chunks, 4)),
            dma((chunks, 4)),
            dma((pairs, 2)),
            dma((chunks, 4)),
        ],
        compiler_params=pltpu.CompilerParams(
            collective_id=0, has_side_effects=True, vmem_limit_bytes=58 * 1024 * 1024
        ),
        name="layer",
    )(
        queries_small,
        keys_small,
        values_small,
        queries_large,
        keys_large,
        values_large,
        query_gain_small.reshape(1, -1),
        key_gain_small.reshape(1, -1),
        query_gain_large.reshape(1, -1),
        key_gain_large.reshape(1, -1),
        jnp.asarray(np.stack(col_tables)),
        jnp.asarray(np.stack(row_tables, axis=1)),
        out_weight_small,
        out_weight_large,
        residual_in,
        norm_gain.reshape(1, -1),
        routes.T,
        route_scores,
        expert_gate,
        expert_up,
        expert_down,
    )


def solution(mesh):
    in_specs = (
        P(("grp", "sp"), "tp"),
        P(("grp", "sp"), "tp"),
        P(("grp", "sp"), "tp"),
        P(("grp", "sp"), "tp"),
        P(("grp", "sp"), "tp"),
        P(("grp", "sp"), "tp"),
        P("grp"),
        P("grp"),
        P("grp"),
        P("grp"),
        P(("grp", "sp", "tp"), None),
        P("tp", None),
        P("tp", None),
        P(),
        P(("grp", "sp", "tp"), None),
        P(("grp", "sp", "tp"), None),
        P("sp", None, "tp"),
        P("sp", None, "tp"),
        P("sp", "tp", None),
    )
    out_specs = P(("grp", "sp", "tp"), None)
    return jax.shard_map(
        on_device, mesh=mesh, in_specs=in_specs, out_specs=out_specs, check_vma=False
    )
```

```python
import functools
import jax
import jax.numpy as jnp
import numpy as np
from jax import lax
from jax.experimental import pallas as pl
from jax.experimental.pallas import tpu as pltpu
from jax.sharding import PartitionSpec as P

HS_SMALL = 64
HS_LARGE = 128
GRID_W = 64
LANES = 128
LOG2E = 1.4426950408889634
theta_base = 10000.0
norm_eps = 1e-06
SEATS = 4
MESH = pl.DeviceIdType.MESH
BF16 = jnp.bfloat16
F32 = jnp.float32


def _send(src, dst, ssem, rsem, axis, dev):
    return pltpu.make_async_remote_copy(
        src_ref=src,
        dst_ref=dst,
        send_sem=ssem,
        recv_sem=rsem,
        device_id={axis: dev},
        device_id_type=MESH,
    )


def _iota(shape, dim):
    return lax.broadcasted_iota(jnp.int32, shape, dim)


class Ring:
    def __init__(self, buf, parts, rsem, psem, fsem, ssem, right, left, partner, last):
        self.buf, self.parts, self.last = buf, parts, last
        self.rsem, self.psem, self.fsem, self.ssem = rsem, psem, fsem, ssem
        self.right, self.left, self.partner = right, left, partner

    def at(self, pair, side, part):
        return self.buf.at[pair, side, self.parts[part]]

    def copy(self, src, dst, rsem, dev):
        return _send(src, dst, self.ssem.at[0], rsem, "sp", dev)

    def begin(self, part):
        own = self.at(0, 0, part)
        self.copy(own, self.at(1, 0, part), self.rsem.at[1, part], self.right).start()
        self.copy(own, self.at(1, 1, part), self.rsem.at[1, part], self.left).start()
        self.copy(own, self.at(0, 1, part), self.psem.at[0], self.partner).start()

    def got(self, ref, sem):
        self.copy(ref, ref, sem, self.partner).wait_recv()

    def pass_on(self, step, part):
        pair, last = 2 * step - 1, self.last
        self.got(self.buf.at[pair, pl.ds(0, 2), self.parts[part]], self.rsem.at[step, part])

        @pl.when(step < last - 1)
        def _():
            sem = self.rsem.at[step + 1, part]
            self.copy(self.at(pair, 0, part), self.at(pair + 2, 0, part), sem, self.right).start()
            self.copy(self.at(pair, 1, part), self.at(pair + 2, 1, part), sem, self.left).start()

        @pl.when(step == last - 1)
        def _():
            dev = self.right if part == 0 else self.left
            self.copy(
                self.at(pair, part, part), self.at(2 * last - 1, 0, part), self.fsem.at[0], dev
            ).start()

        for side in range(2):
            self.copy(
                self.at(pair, side, part),
                self.at(pair + 1, side, part),
                self.psem.at[step],
                self.partner,
            ).start()

    def first_partner(self):
        self.got(self.buf.at[0, 1], self.psem.at[0])

    def from_partner(self, step):
        self.got(self.buf.at[2 * step], self.psem.at[step])

    def to_opposite(self):
        pair = 2 * self.last - 1
        return _send(
            self.buf.at[pair, 0],
            self.buf.at[pair, 1],
            self.ssem.at[1],
            self.fsem.at[1],
            "sp",
            self.partner,
        )

    def opposite(self):
        self.got(self.buf.at[2 * self.last - 1, 0], self.fsem.at[0])
        self.to_opposite().start()

    def opposite_partner(self):
        self.to_opposite().wait_recv()

    def finish(self):
        every = self.buf.at[pl.ds(0, 2 * self.last - 1)]
        self.copy(every, every, self.fsem.at[0], self.partner).wait_send()
        self.to_opposite().wait_send()


def layer_kernel(
    heads,
    qs_ref,
    ks_ref,
    vs_ref,
    ql_ref,
    kl_ref,
    vl_ref,
    gqs_ref,
    gks_ref,
    gql_ref,
    gkl_ref,
    col_hbm,
    row_hbm,
    ws_hbm,
    wl_hbm,
    res_ref,
    gain_ref,
    names_ref,
    score_ref,
    wg_hbm,
    wu_hbm,
    wd_hbm,
    out_ref,
    kvbuf,
    qt,
    coltab,
    rowtab,
    tabs,
    wbuf,
    acc,
    mbuf,
    lbuf,
    hbuf,
    cbuf,
    dbuf,
    abuf,
    xbuf,
    wg,
    wu,
    wd,
    gbuf,
    pbuf,
    rbuf,
    fbuf,
    obuf,
    ret,
    below,
    perm,
    pick,
    lsem,
    rsem,
    psem,
    fsem,
    ssem,
    xr,
    xs,
    rsem2,
    psem2,
    fsem2,
    ssem2,
    gr,
    gs,
    rr,
    rs,
    tr,
    ts,
):
    n_sp = lax.axis_size("sp")
    n_z = n_sp // 2
    last = n_z // 2
    tok = kvbuf.shape[3]
    kv_rows = kvbuf.shape[2]
    rows, width = res_ref.shape
    sp = lax.axis_index("sp")
    tp = lax.axis_index("tp")
    z = sp // 2
    core = lax.rem(sp, 2)
    right = lax.rem(sp + 2, n_sp)
    left = lax.rem(sp + n_sp - 2, n_sp)
    partner = sp + 1 - 2 * core
    x_right = lax.rem(tp + 1, 4)
    x_left = lax.rem(tp + 3, 4)
    x_far = lax.rem(tp + 2, 4)
    grid_rows = tok // GRID_W

    loads = [
        pltpu.make_async_copy(a, b, lsem.at[i])
        for i, (a, b) in enumerate(
            (
                (col_hbm, coltab),
                (row_hbm.at[pl.ds(sp * grid_rows, grid_rows)], rowtab),
                (ws_hbm, wbuf.at[pl.ds(0, ws_hbm.shape[0])]),
                (wl_hbm, wbuf.at[pl.ds(ws_hbm.shape[0], wl_hbm.shape[0])]),
                (wg_hbm, wg),
                (wu_hbm, wu),
                (wd_hbm, wd),
            )
        )
    ]
    loads[0].start()
    loads[1].start()

    barrier = pltpu.get_barrier_semaphore()

    def greet(i, carry):
        pl.semaphore_signal(
            barrier, inc=1, device_id={"sp": lax.rem(sp + i, n_sp)}, device_id_type=MESH
        )
        return carry

    lax.fori_loop(1, n_sp, greet, 0)
    for dev in (x_right, x_left):
        pl.semaphore_signal(barrier, inc=1, device_id={"tp": dev}, device_id_type=MESH)

    ring = Ring(
        kvbuf,
        (pl.ds(0, tok), pl.ds(tok, kv_rows - tok)),
        rsem,
        psem,
        fsem,
        ssem,
        right,
        left,
        partner,
        last,
    )
    tokens = Ring(
        xbuf,
        (pl.ds(0, rows // 2), pl.ds(rows // 2, rows // 2)),
        rsem2,
        psem2,
        fsem2,
        ssem2,
        right,
        left,
        partner,
        last,
    )

    lane = _iota((tok, LANES), 1)

    def turned(raw, gain, table, size):
        x = raw.astype(F32)
        square = x * x
        if size < LANES:
            lower = lane < size
            mean = jnp.where(
                lower,
                jnp.sum(jnp.where(lower, square, 0.0), axis=1, keepdims=True),
                jnp.sum(jnp.where(lower, 0.0, square), axis=1, keepdims=True),
            ) * (1.0 / size)
            gain = jnp.concatenate([gain, gain], axis=1)
        else:
            mean = jnp.sum(square, axis=1, keepdims=True) * (1.0 / size)
        x = x * lax.rsqrt(mean + norm_eps) * gain
        quarter = size // 4
        swapped = jnp.where(
            lane % (2 * quarter) < quarter,
            pltpu.roll(x, LANES - quarter, 1),
            pltpu.roll(x, quarter, 1),
        )
        return x * tabs[table] + swapped * tabs[table + 1]

    kvbuf[0, 0, pl.ds(tok, LANES), :] = jnp.transpose(vs_ref[...].astype(F32)).astype(BF16)
    kvbuf[0, 0, pl.ds(tok + LANES, LANES), :] = jnp.transpose(vl_ref[...].astype(F32)).astype(BF16)
    names = names_ref[...].astype(F32)
    repeat = (_iota((16, 2), 0) % 2 == _iota((16, 2), 1)).astype(BF16)
    named = jnp.dot(repeat, names.astype(BF16), preferred_element_type=F32).astype(BF16)
    spread = (_iota((rows, tok), 1) % rows == _iota((rows, tok), 0)).astype(BF16)
    named = jnp.dot(named, spread, preferred_element_type=F32)
    own_lane = _iota((16, tok), 1) // rows == _iota((16, tok), 0) // 2
    kvbuf[0, 0, pl.ds(2 * tok, 16), :] = jnp.where(own_lane, named, 0.0).astype(BF16)

    loads[0].wait()
    loads[1].wait()
    for i in range(4):
        for g in range(grid_rows):
            tabs[i, pl.ds(g * GRID_W, GRID_W), :] = coltab[i] + rowtab[g, pl.ds(i, 1), :]
    kvbuf[0, 0, pl.ds(0, tok), pl.ds(0, LANES)] = turned(
        ks_ref[...], gks_ref[...], 0, HS_SMALL
    ).astype(BF16)
    kvbuf[0, 0, pl.ds(0, tok), pl.ds(LANES, LANES)] = turned(
        kl_ref[...], gkl_ref[...], 2, HS_LARGE
    ).astype(BF16)

    pl.semaphore_wait(barrier, n_sp + 1)
    for part in range(2):
        ring.begin(part)
    for load in loads[2:]:
        load.start()

    qt[...] = jnp.zeros_like(qt)
    h = 0
    for ref, gain_of, table, size, base in (
        (qs_ref, gqs_ref, 0, HS_SMALL, 0),
        (ql_ref, gql_ref, 2, HS_LARGE, LANES),
    ):
        for i in range(ref.shape[1] // LANES):
            flipped = jnp.transpose(
                turned(ref[:, pl.ds(i * LANES, LANES)], gain_of[...], table, size)
            ).astype(BF16)
            for j in range(LANES // size):
                at = base + (h - base // LANES * 4) // 2 * size
                qt[h, pl.ds(at, size), :] = flipped[j * size : (j + 1) * size]
                h += 1

    acc[...] = jnp.zeros_like(acc)
    lbuf[...] = jnp.zeros_like(lbuf)
    mbuf[...] = jnp.full(mbuf.shape, -1e30, F32)

    below[...] = (
        (_iota((tok, tok), 0) < _iota((tok, tok), 1))
        & (_iota((tok, tok), 0) // rows == _iota((tok, tok), 1) // rows)
    ).astype(BF16)
    out_row = _iota((64, 64), 0)
    in_row = (
        (out_row // 8) % 2 * 32 + (out_row % 8) // SEATS * 16 + out_row // 16 * SEATS
    ) + out_row % SEATS
    perm[...] = (in_row == _iota((64, 64), 1)).astype(BF16)
    eye = (_iota((rows, rows), 0) == _iota((rows, rows), 1)).astype(BF16)
    columns = lax.dot_general(
        eye, names.astype(BF16), (((1,), (1,)), ((), ())), preferred_element_type=F32
    )
    earlier = _iota((rows, rows), 1) < _iota((rows, rows), 0)
    for k in range(2):
        column = columns[:, k : k + 1]
        same = ((column == names[0:1, :]) | (column == names[1:2, :])) & earlier
        rank = jnp.sum(same.astype(F32), axis=1, keepdims=True).astype(jnp.int32)
        expert = column.astype(jnp.int32)
        host = expert // 2
        away = z - host // 2
        away = jnp.where(away < 0, away + n_z, away)
        other = (host % 2 != core).astype(jnp.int32)
        step = jnp.minimum(away, n_z - away)
        edge = (away == 0) | (away == last)
        pair = jnp.where(
            away == 0, 0, jnp.where(away == last, 2 * last - 1, 2 * step - 1 + other)
        )
        side = jnp.where(edge, other, (away < last).astype(jnp.int32))
        base = (pair * 2 + side) * 16 + expert % 2 * SEATS + rank
        seat = _iota((rows, pick.shape[1]), 1)
        pick[pl.ds(k * rows, rows), :] = (seat == base).astype(BF16)
        pick[pl.ds((2 + k) * rows, rows), :] = (seat == base + 8).astype(BF16)

    def attend(pair):
        keys = kvbuf[pair, :, pl.ds(0, tok), :].reshape(2 * tok, tok)
        ahead = jnp.dot(keys, qt[0], preferred_element_type=F32)
        for h, (a0, size, v0, scale) in enumerate(heads):
            s = ahead
            if h + 1 < len(heads):
                ahead = jnp.dot(keys, qt[h + 1], preferred_element_type=F32)
            m_old = mbuf[h]
            m_new = jnp.maximum(m_old, jnp.max(s, axis=0, keepdims=True))
            p = jnp.exp2((s - m_new) * (scale * LOG2E))
            shrink = jnp.exp2((m_old - m_new) * (scale * LOG2E))
            mbuf[h] = m_new
            lbuf[h] = lbuf[h] * shrink + jnp.sum(p, axis=0, keepdims=True)
            pb = p.astype(BF16)
            pv = jnp.dot(
                kvbuf[pair, 0, pl.ds(tok + v0, size), :],
                pb[:tok],
                preferred_element_type=F32,
            ) + jnp.dot(
                kvbuf[pair, 1, pl.ds(tok + v0, size), :],
                pb[tok:],
                preferred_element_type=F32,
            )
            acc[pl.ds(a0, size), :] = acc[pl.ds(a0, size), :] * shrink + pv

    def attend_turn(t, carry):
        step = t // 2 + 1
        phase = lax.rem(t, 2)
        for part in range(2):

            @pl.when((phase == part) & (step < last))
            def _():
                ring.pass_on(step, part)

        @pl.when(t == 0)
        def _():
            ring.first_partner()

        @pl.when((phase == 0) & (t > 0))
        def _():
            ring.from_partner(t // 2)

        @pl.when(t == 2 * last - 1)
        def _():
            ring.opposite()
            ring.opposite_partner()

        attend(t)
        return carry

    lax.fori_loop(0, 2 * last, attend_turn, 0)

    loads[2].wait()
    loads[3].wait()
    for h, (a0, size, v0, scale) in enumerate(heads):
        acc[pl.ds(a0, size), :] = acc[pl.ds(a0, size), :] / lbuf[h]
    heard = jnp.transpose(acc[...]).astype(BF16)
    hbuf[...] = heard.reshape(4, rows, heard.shape[1])

    def project(where, owner):
        cbuf[where] = jnp.dot(hbuf[owner], wbuf[...], preferred_element_type=F32).astype(BF16)

    quarter = rows // 4
    halves = (pl.ds(0, 2 * quarter), pl.ds(2 * quarter, 2 * quarter))

    def first(part, way):
        piece = pl.ds((2 * part + way) * quarter, quarter)
        return _send(
            cbuf.at[0, piece],
            dbuf.at[3, piece],
            xs.at[0],
            xr.at[part, way],
            "tp",
            (x_right, x_left)[way],
        )

    def near(part, way):
        return _send(
            cbuf.at[1 + way, halves[part]],
            dbuf.at[way, halves[part]],
            xs.at[0],
            xr.at[part, 2],
            "tp",
            (x_right, x_left)[way],
        )

    def relay(part, way):
        piece = pl.ds((2 * part + way) * quarter, quarter)
        return _send(
            dbuf.at[3, piece],
            dbuf.at[2, piece],
            xs.at[0],
            xr.at[part, 3],
            "tp",
            (x_right, x_left)[way],
        )

    def came_in(ref, sem):
        _send(ref, ref, xs.at[0], sem, "tp", x_right).wait_recv()

    project(0, x_far)
    for way in range(2):
        first(0, way).start()
    project(1, x_right)
    near(0, 0).start()
    project(2, x_left)
    near(0, 1).start()
    for way in range(2):
        first(1, way).start()
    project(3, tp)
    for way in range(2):
        first(0, way).wait_recv()
        relay(0, way).start()
    for way in range(2):
        near(1, way).start()
    for way in range(2):
        first(1, way).wait_recv()
        relay(1, way).start()
    ring.finish()
    for part, half in enumerate(halves):
        came_in(dbuf.at[pl.ds(0, 2), half], xr.at[part, 2])
        came_in(dbuf.at[2, half], xr.at[part, 3])
        total = (
            cbuf[3, half].astype(F32)
            + dbuf[0, half].astype(F32)
            + dbuf[1, half].astype(F32)
            + dbuf[2, half].astype(F32)
        )
        attended = (res_ref[half].astype(F32) + total).astype(BF16)
        abuf[half] = attended
        wide = attended.astype(F32)
        xbuf[0, 0, half] = (
            wide
            * lax.rsqrt(jnp.mean(wide * wide, axis=-1, keepdims=True) + norm_eps)
            * gain_ref[...]
        ).astype(BF16)
        tokens.begin(part)
    _send(cbuf, cbuf, xs.at[0], xr.at[0, 0], "tp", x_right).wait_send()

    def share_right(c):
        return _send(gbuf.at[c, 0], gbuf.at[c, 1], gs.at[0], gr.at[c, 0], "tp", x_right)

    def share_left(c):
        return _send(gbuf.at[c, 0], gbuf.at[c, 2], gs.at[0], gr.at[c, 0], "tp", x_left)

    def pass_right(c):
        return _send(
            gbuf.at[c, 1, 0], gbuf.at[c, 3, 0], gs.at[0], gr.at[c, 1], "tp", x_right
        )

    def pass_left(c):
        return _send(gbuf.at[c, 2, 1], gbuf.at[c, 3, 1], gs.at[0], gr.at[c, 1], "tp", x_left)

    def far_right(c):
        return _send(pbuf.at[c, 3, 0], rbuf.at[c, 0], rs.at[0], rr.at[c, 0], "tp", x_right)

    def far_left(c):
        return _send(pbuf.at[c, 3, 1], rbuf.at[c, 1], rs.at[0], rr.at[c, 0], "tp", x_left)

    def near_right(c):
        return _send(pbuf.at[c, 2], fbuf.at[c, 0], rs.at[0], rr.at[c, 1], "tp", x_right)

    def near_left(c):
        return _send(pbuf.at[c, 1], fbuf.at[c, 1], rs.at[0], rr.at[c, 1], "tp", x_left)

    def both(ref, sem):
        _send(ref, ref, gs.at[0], sem, "tp", x_right).wait_recv()

    def seats_of(c):
        row = _iota((16, tok), 0)
        kept = jnp.zeros((16, tok), F32)
        for q in range(4):
            block = kvbuf[2 * c + q // 2, q % 2, pl.ds(2 * tok, 16), :].astype(F32)
            kept = jnp.where(row // 2 == q, block, kept)
        name0 = jnp.sum(jnp.where(row % 2 == 0, kept, 0.0), axis=0, keepdims=True)
        name1 = jnp.sum(jnp.where(row % 2 == 1, kept, 0.0), axis=0, keepdims=True)
        wide_row = _iota((32, tok), 0)
        mine = (2 * sp + wide_row // 16).astype(F32)
        member = (name0 == mine) | (name1 == mine)
        rank = jnp.dot(member.astype(F32).astype(BF16), below[...], preferred_element_type=F32)
        seated = (
            member
            & (rank == (wide_row % SEATS).astype(F32))
            & (_iota((32, tok), 1) // rows == wide_row % 16 // SEATS)
        )
        return seated.astype(F32).astype(BF16)

    def run_experts(c):
        for e in range(2):
            x = gbuf[c, :, e].reshape(64, width)
            gate = jnp.dot(x, wg[e], preferred_element_type=F32)
            up = jnp.dot(x, wu[e], preferred_element_type=F32)
            active = (gate / (1.0 + jnp.exp(-gate)) * up).astype(BF16)
            term = jnp.dot(active, wd[e], preferred_element_type=F32)
            pbuf[c, :, e] = term.astype(BF16).reshape(4, 16, width)

    def gather_turn(c):
        step = c + 1

        @pl.when(step < last)
        def _():
            for part in range(2):
                tokens.pass_on(step, part)

        @pl.when(step == last)
        def _():
            tokens.opposite()

        @pl.when(c == 0)
        def _():
            tokens.first_partner()

        @pl.when((c > 0) & (c < last))
        def _():
            tokens.from_partner(c)

        @pl.when(step == last)
        def _():
            tokens.opposite_partner()

        @pl.when(c < last)
        def _():
            block = xbuf[pl.ds(2 * c, 2)].reshape(4 * rows, width)
            chosen = jnp.dot(seats_of(c), block, preferred_element_type=F32)
            gbuf[c, 0] = chosen.astype(BF16).reshape(2, 16, width)
            share_right(c).start()
            share_left(c).start()

        @pl.when((c >= 1) & (c < last + 1))
        def _():
            both(gbuf.at[c - 1, pl.ds(1, 2)], gr.at[c - 1, 0])
            pass_right(c - 1).start()
            pass_left(c - 1).start()

        @pl.when(c == 2)
        def _():
            for load in loads[4:]:
                load.wait()

        @pl.when((c >= 2) & (c < last + 2))
        def _():
            both(gbuf.at[c - 2, 3], gr.at[c - 2, 1])
            run_experts(c - 2)

    def home(c, q):
        if q == 0:
            return lax.rem(z - c + n_z, n_z) * 2 + 1 - core, 2 * c, 0
        if q == 1:
            return lax.rem(z + c, n_z) * 2 + 1 - core, 2 * c, 1
        if q == 2:
            return lax.rem(z - c - 1 + n_z, n_z) * 2 + core, 2 * c + 1, 0
        return lax.rem(z + c + 1, n_z) * 2 + core, 2 * c + 1, 1

    def give(c, q):
        dev, pair, side = home(c, q)
        return _send(
            obuf.at[c, q], ret.at[pair, side], ts.at[min(q, 1)], tr.at[1], "sp", dev
        )

    def give_last():
        dev = lax.rem(z + last, n_z) * 2 + 1 - core
        return _send(
            obuf.at[last - 1, 3],
            ret.at[2 * last - 1, 1],
            ts.at[1],
            tr.at[1],
            "sp",
            dev,
        )

    start = last // 2 - 1

    def order(i):
        high = last - start
        late = i // high
        return (1 - late) * (i + start) + late * (last - 1 - i)

    def give_partner():
        return _send(obuf.at[0, 1], ret.at[0, 1], ts.at[1], tr.at[0], "sp", partner)

    def return_turn(i):
        @pl.when((i >= 1) & (i < last + 1))
        def _():
            c = order(i - 1)
            both(rbuf.at[c], rr.at[c, 0])
            pbuf[c, 2, 0] = (pbuf[c, 2, 0].astype(F32) + rbuf[c, 0].astype(F32)).astype(BF16)
            near_right(c).start()
            pbuf[c, 1, 1] = (pbuf[c, 1, 1].astype(F32) + rbuf[c, 1].astype(F32)).astype(BF16)
            near_left(c).start()

        @pl.when((i >= 0) & (i < last))
        def _():
            c = order(i)
            far_right(c).start()
            far_left(c).start()

        @pl.when(i >= 2)
        def _():
            c = order(i - 2)
            both(fbuf.at[c], rr.at[c, 1])
            total = pbuf[c, 0].astype(F32) + fbuf[c, 0].astype(F32) + fbuf[c, 1].astype(F32)
            total = total.astype(BF16).reshape(32, width)
            split = jnp.concatenate([total[:, : width // 2], total[:, width // 2 :]], axis=0)
            ordered = jnp.dot(perm[...], split, preferred_element_type=F32)
            obuf[c] = ordered.astype(BF16).reshape(4, 16, width // 2)

            @pl.when(c > 0)
            def _():
                give(c, 0).start()
                give(c, 1).start()

            @pl.when(c == 0)
            def _():
                ret[0, 0] = obuf[0, 0]
                give_partner().start()

            give(c, 2).start()

            @pl.when(c < last - 1)
            def _():
                give(c, 3).start()

            @pl.when(c == last - 1)
            def _():
                give_last().start()

    def turn(t, carry):
        gather_turn(t)
        return_turn(t - (start + 2))
        return carry

    lax.fori_loop(0, last + start + 4, turn, 0)

    tokens.finish()

    sent = gbuf.at[pl.ds(0, 3 * (last // 4))]
    _send(sent, sent, gs.at[0], gr.at[0, 0], "tp", x_right).wait_send()
    sent = pbuf.at[pl.ds(0, 3 * (last // 4))]
    _send(sent, sent, rs.at[0], rr.at[0, 0], "tp", x_right).wait_send()
    home_all = ret.at[pl.ds(1, 2 * last - 1)]
    give_partner().wait_recv()
    _send(home_all, home_all, ts.at[0], tr.at[1], "sp", partner).wait_recv()

    back = ret[...].reshape(ret.shape[0] * 32, width // 2)
    picked = jnp.dot(pick[...], back, preferred_element_type=F32)
    scores = score_ref[...]
    scores = scores / (scores[:, 0:1] + scores[:, 1:2])
    one, two = scores[:, 0:1], scores[:, 1:2]
    out = abuf[...].astype(F32)
    lower = picked[:rows] * one + picked[rows : 2 * rows] * two
    upper = picked[2 * rows : 3 * rows] * one + picked[3 * rows :] * two
    out_ref[:, : width // 2] = (out[:, : width // 2] + lower).astype(BF16)
    out_ref[:, width // 2 :] = (out[:, width // 2 :] + upper).astype(BF16)

    sent = obuf.at[pl.ds(1, last - 1), 0]
    _send(sent, sent, ts.at[0], tr.at[1], "sp", partner).wait_send()
    sent = obuf.at[pl.ds(0, 3 * (last // 4))]
    _send(sent, sent, ts.at[1], tr.at[1], "sp", partner).wait_send()


def turn_tables(places, size, by_row):
    lane = np.arange(LANES) % size
    quarter = size // 4
    rates = np.power(
        np.float32(theta_base), (-2.0 * np.arange(quarter) / (size // 2)).astype(np.float32)
    ).astype(np.float32)
    angles = (places[:, None].astype(np.float32) * rates[lane % quarter]).astype(np.float32)
    here = (lane < size // 2) if by_row else (lane >= size // 2)
    sign = np.where(lane % (2 * quarter) < quarter, -1.0, 1.0)
    cosine = np.where(here, np.cos(angles), 0.0)
    sine = np.where(here, np.sin(angles) * sign, 0.0)
    return cosine.astype(np.float32), sine.astype(np.float32)


def on_device(
    queries_small,
    keys_small,
    values_small,
    queries_large,
    keys_large,
    values_large,
    query_gain_small,
    key_gain_small,
    query_gain_large,
    key_gain_large,
    residual_in,
    out_weight_small,
    out_weight_large,
    norm_gain,
    routes,
    route_scores,
    expert_gate,
    expert_up,
    expert_down,
):
    tok = queries_small.shape[0]
    rows, width = residual_in.shape
    n_sp = lax.axis_size("sp")
    pairs = n_sp // 2
    chunks = pairs // 2
    depth = out_weight_small.shape[0] + out_weight_large.shape[0]
    kv_rows = 2 * tok + 16
    grid_rows = tok // GRID_W
    row_places = np.arange(n_sp * grid_rows)
    col_places = np.arange(GRID_W)
    row_tables, col_tables = [], []
    for size in (HS_SMALL, HS_LARGE):
        row_tables.extend(turn_tables(row_places, size, True))
        col_tables.extend(turn_tables(col_places, size, False))
    heads = []
    wide_small = keys_small.shape[1]
    for count, kv_count, size, a0, v0 in (
        (queries_small.shape[1] // HS_SMALL, wide_small // HS_SMALL, HS_SMALL, 0, 0),
        (
            queries_large.shape[1] // HS_LARGE,
            keys_large.shape[1] // HS_LARGE,
            HS_LARGE,
            queries_small.shape[1],
            wide_small,
        ),
    ):
        for h in range(count):
            kv = h // (count // kv_count)
            heads.append((a0 + h * size, size, v0 + kv * size, size ** (-0.5)))
    vmem = pl.BlockSpec(memory_space=pltpu.VMEM)
    hbm = pl.BlockSpec(memory_space=pl.ANY)
    dma = pltpu.SemaphoreType.DMA
    V = pltpu.VMEM
    return pl.pallas_call(
        functools.partial(layer_kernel, tuple(heads)),
        out_shape=jax.ShapeDtypeStruct((rows, width), BF16),
        in_specs=[vmem] * 10 + [hbm] * 4 + [vmem] * 4 + [hbm] * 3,
        out_specs=vmem,
        scratch_shapes=[
            V((pairs, 2, kv_rows, tok), BF16),
            V((len(heads), tok, tok), BF16),
            V((4, GRID_W, LANES), F32),
            V((grid_rows, 4, LANES), F32),
            V((4, tok, LANES), F32),
            V((depth, width), BF16),
            V((depth, tok), F32),
            V((len(heads), 1, tok), F32),
            V((len(heads), 1, tok), F32),
            V((4, rows, depth), BF16),
            V((4, rows, width), BF16),
            V((4, rows, width), BF16),
            V((rows, width), BF16),
            V((pairs, 2, rows, width), BF16),
            V(expert_gate.shape, BF16),
            V(expert_up.shape, BF16),
            V(expert_down.shape, BF16),
            V((chunks, 4, 2, 16, width), BF16),
            V((chunks, 4, 2, 16, width), BF16),
            V((chunks, 2, 16, width), BF16),
            V((chunks, 2, 2, 16, width), BF16),
            V((chunks, 4, 16, width // 2), BF16),
            V((pairs, 2, 16, width // 2), BF16),
            V((tok, tok), BF16),
            V((64, 64), BF16),
            V((4 * rows, pairs * 32), BF16),
            dma((7,)),
            dma((chunks, 2)),
            dma((chunks,)),
            dma((2,)),
            dma((2,)),
            dma((2, 4)),
            dma((1,)),
            dma((chunks, 2)),
            dma((chunks,)),
            dma((2,)),
            dma((2,)),
            dma((chunks, 2)),
            dma((1,)),
            dma((chunks, 2)),
            dma((1,)),
            dma((2,)),
            dma((2,)),
        ],
        compiler_params=pltpu.CompilerParams(
            collective_id=0, has_side_effects=True, vmem_limit_bytes=58 * 1024 * 1024
        ),
        name="layer",
    )(
        queries_small,
        keys_small,
        values_small,
        queries_large,
        keys_large,
        values_large,
        query_gain_small.reshape(1, -1),
        key_gain_small.reshape(1, -1),
        query_gain_large.reshape(1, -1),
        key_gain_large.reshape(1, -1),
        jnp.asarray(np.stack(col_tables)),
        jnp.asarray(np.stack(row_tables, axis=1)),
        out_weight_small,
        out_weight_large,
        residual_in,
        norm_gain.reshape(1, -1),
        routes.T,
        route_scores,
        expert_gate,
        expert_up,
        expert_down,
    )


def solution(mesh):
    in_specs = (
        P(("grp", "sp"), "tp"),
        P(("grp", "sp"), "tp"),
        P(("grp", "sp"), "tp"),
        P(("grp", "sp"), "tp"),
        P(("grp", "sp"), "tp"),
        P(("grp", "sp"), "tp"),
        P("grp"),
        P("grp"),
        P("grp"),
        P("grp"),
        P(("grp", "sp", "tp"), None),
        P("tp", None),
        P("tp", None),
        P(),
        P(("grp", "sp", "tp"), None),
        P(("grp", "sp", "tp"), None),
        P("sp", None, "tp"),
        P("sp", None, "tp"),
        P("sp", "tp", None),
    )
    out_specs = P(("grp", "sp", "tp"), None)
    return jax.shard_map(
        on_device, mesh=mesh, in_specs=in_specs, out_specs=out_specs, check_vma=False
    )
```

```python
import functools
import jax
import jax.numpy as jnp
import numpy as np
from jax import lax
from jax.experimental import pallas as pl
from jax.experimental.pallas import tpu as pltpu
from jax.sharding import PartitionSpec as P

HS_SMALL = 64
HS_LARGE = 128
GRID_W = 64
LANES = 128
LOG2E = 1.4426950408889634
theta_base = 10000.0
norm_eps = 1e-06
SEATS = 4
MESH = pl.DeviceIdType.MESH
BF16 = jnp.bfloat16
F32 = jnp.float32


def _send(src, dst, ssem, rsem, axis, dev):
    return pltpu.make_async_remote_copy(
        src_ref=src,
        dst_ref=dst,
        send_sem=ssem,
        recv_sem=rsem,
        device_id={axis: dev},
        device_id_type=MESH,
    )


def _iota(shape, dim):
    return lax.broadcasted_iota(jnp.int32, shape, dim)


class Ring:
    def __init__(self, buf, parts, rsem, psem, fsem, ssem, right, left, partner, last):
        self.buf, self.parts, self.last = buf, parts, last
        self.rsem, self.psem, self.fsem, self.ssem = rsem, psem, fsem, ssem
        self.right, self.left, self.partner = right, left, partner

    def at(self, pair, side, part):
        return self.buf.at[pair, side, self.parts[part]]

    def copy(self, src, dst, rsem, dev):
        return _send(src, dst, self.ssem.at[0], rsem, "sp", dev)

    def begin(self, part):
        own = self.at(0, 0, part)
        self.copy(own, self.at(1, 0, part), self.rsem.at[1, part], self.right).start()
        self.copy(own, self.at(1, 1, part), self.rsem.at[1, part], self.left).start()
        self.copy(own, self.at(0, 1, part), self.psem.at[0], self.partner).start()

    def got(self, ref, sem):
        self.copy(ref, ref, sem, self.partner).wait_recv()

    def pass_on(self, step, part):
        pair, last = 2 * step - 1, self.last
        self.got(self.buf.at[pair, pl.ds(0, 2), self.parts[part]], self.rsem.at[step, part])

        @pl.when(step < last - 1)
        def _():
            sem = self.rsem.at[step + 1, part]
            self.copy(self.at(pair, 0, part), self.at(pair + 2, 0, part), sem, self.right).start()
            self.copy(self.at(pair, 1, part), self.at(pair + 2, 1, part), sem, self.left).start()

        @pl.when(step == last - 1)
        def _():
            dev = self.right if part == 0 else self.left
            self.copy(
                self.at(pair, part, part), self.at(2 * last - 1, 0, part), self.fsem.at[0], dev
            ).start()

        for side in range(2):
            self.copy(
                self.at(pair, side, part),
                self.at(pair + 1, side, part),
                self.psem.at[step],
                self.partner,
            ).start()

    def first_partner(self):
        self.got(self.buf.at[0, 1], self.psem.at[0])

    def from_partner(self, step):
        self.got(self.buf.at[2 * step], self.psem.at[step])

    def to_opposite(self):
        pair = 2 * self.last - 1
        return _send(
            self.buf.at[pair, 0],
            self.buf.at[pair, 1],
            self.ssem.at[1],
            self.fsem.at[1],
            "sp",
            self.partner,
        )

    def opposite(self):
        self.got(self.buf.at[2 * self.last - 1, 0], self.fsem.at[0])
        self.to_opposite().start()

    def opposite_partner(self):
        self.to_opposite().wait_recv()

    def finish(self):
        every = self.buf.at[pl.ds(0, 2 * self.last - 1)]
        self.copy(every, every, self.fsem.at[0], self.partner).wait_send()
        self.to_opposite().wait_send()


def layer_kernel(
    heads,
    qs_ref,
    ks_ref,
    vs_ref,
    ql_ref,
    kl_ref,
    vl_ref,
    gqs_ref,
    gks_ref,
    gql_ref,
    gkl_ref,
    col_hbm,
    row_hbm,
    ws_hbm,
    wl_hbm,
    res_ref,
    gain_ref,
    names_ref,
    score_ref,
    wg_hbm,
    wu_hbm,
    wd_hbm,
    out_ref,
    kvbuf,
    qt,
    coltab,
    rowtab,
    tabs,
    wbuf,
    acc,
    mbuf,
    lbuf,
    hbuf,
    cbuf,
    dbuf,
    abuf,
    xbuf,
    wg,
    wu,
    wd,
    gbuf,
    pbuf,
    rbuf,
    fbuf,
    obuf,
    ret,
    below,
    perm,
    pick,
    lsem,
    rsem,
    psem,
    fsem,
    ssem,
    xr,
    xs,
    rsem2,
    psem2,
    fsem2,
    ssem2,
    gr,
    gs,
    rr,
    rs,
    tr,
    ts,
):
    n_sp = lax.axis_size("sp")
    n_z = n_sp // 2
    last = n_z // 2
    tok = kvbuf.shape[3]
    kv_rows = kvbuf.shape[2]
    rows, width = res_ref.shape
    sp = lax.axis_index("sp")
    tp = lax.axis_index("tp")
    z = sp // 2
    core = lax.rem(sp, 2)
    right = lax.rem(sp + 2, n_sp)
    left = lax.rem(sp + n_sp - 2, n_sp)
    partner = sp + 1 - 2 * core
    x_right = lax.rem(tp + 1, 4)
    x_left = lax.rem(tp + 3, 4)
    x_far = lax.rem(tp + 2, 4)
    grid_rows = tok // GRID_W

    loads = [
        pltpu.make_async_copy(a, b, lsem.at[i])
        for i, (a, b) in enumerate(
            (
                (col_hbm, coltab),
                (row_hbm.at[pl.ds(sp * grid_rows, grid_rows)], rowtab),
                (ws_hbm, wbuf.at[pl.ds(0, ws_hbm.shape[0])]),
                (wl_hbm, wbuf.at[pl.ds(ws_hbm.shape[0], wl_hbm.shape[0])]),
                (wg_hbm, wg),
                (wu_hbm, wu),
                (wd_hbm, wd),
            )
        )
    ]
    loads[0].start()
    loads[1].start()

    barrier = pltpu.get_barrier_semaphore()

    def greet(i, carry):
        pl.semaphore_signal(
            barrier, inc=1, device_id={"sp": lax.rem(sp + i, n_sp)}, device_id_type=MESH
        )
        return carry

    lax.fori_loop(1, n_sp, greet, 0)
    for dev in (x_right, x_left):
        pl.semaphore_signal(barrier, inc=1, device_id={"tp": dev}, device_id_type=MESH)

    ring = Ring(
        kvbuf,
        (pl.ds(0, tok), pl.ds(tok, kv_rows - tok)),
        rsem,
        psem,
        fsem,
        ssem,
        right,
        left,
        partner,
        last,
    )
    tokens = Ring(
        xbuf,
        (pl.ds(0, rows // 2), pl.ds(rows // 2, rows // 2)),
        rsem2,
        psem2,
        fsem2,
        ssem2,
        right,
        left,
        partner,
        last,
    )

    lane = _iota((tok, LANES), 1)

    def turned(raw, gain, table, size):
        x = raw.astype(F32)
        square = x * x
        if size < LANES:
            lower = lane < size
            mean = jnp.where(
                lower,
                jnp.sum(jnp.where(lower, square, 0.0), axis=1, keepdims=True),
                jnp.sum(jnp.where(lower, 0.0, square), axis=1, keepdims=True),
            ) * (1.0 / size)
            gain = jnp.concatenate([gain, gain], axis=1)
        else:
            mean = jnp.sum(square, axis=1, keepdims=True) * (1.0 / size)
        x = x * lax.rsqrt(mean + norm_eps) * gain
        quarter = size // 4
        swapped = jnp.where(
            lane % (2 * quarter) < quarter,
            pltpu.roll(x, LANES - quarter, 1),
            pltpu.roll(x, quarter, 1),
        )
        return x * tabs[table] + swapped * tabs[table + 1]

    kvbuf[0, 0, pl.ds(tok, LANES), :] = jnp.transpose(vs_ref[...].astype(F32)).astype(BF16)
    kvbuf[0, 0, pl.ds(tok + LANES, LANES), :] = jnp.transpose(vl_ref[...].astype(F32)).astype(BF16)
    names = names_ref[...].astype(F32)
    repeat = (_iota((16, 2), 0) % 2 == _iota((16, 2), 1)).astype(BF16)
    named = jnp.dot(repeat, names.astype(BF16), preferred_element_type=F32).astype(BF16)
    spread = (_iota((rows, tok), 1) % rows == _iota((rows, tok), 0)).astype(BF16)
    named = jnp.dot(named, spread, preferred_element_type=F32)
    own_lane = _iota((16, tok), 1) // rows == _iota((16, tok), 0) // 2
    kvbuf[0, 0, pl.ds(2 * tok, 16), :] = jnp.where(own_lane, named, 0.0).astype(BF16)

    loads[0].wait()
    loads[1].wait()
    for i in range(4):
        for g in range(grid_rows):
            tabs[i, pl.ds(g * GRID_W, GRID_W), :] = coltab[i] + rowtab[g, pl.ds(i, 1), :]
    kvbuf[0, 0, pl.ds(0, tok), pl.ds(0, LANES)] = turned(
        ks_ref[...], gks_ref[...], 0, HS_SMALL
    ).astype(BF16)
    kvbuf[0, 0, pl.ds(0, tok), pl.ds(LANES, LANES)] = turned(
        kl_ref[...], gkl_ref[...], 2, HS_LARGE
    ).astype(BF16)

    pl.semaphore_wait(barrier, n_sp + 1)
    for part in range(2):
        ring.begin(part)
    for load in loads[2:]:
        load.start()

    qt[...] = jnp.zeros_like(qt)
    h = 0
    for ref, gain_of, table, size, base in (
        (qs_ref, gqs_ref, 0, HS_SMALL, 0),
        (ql_ref, gql_ref, 2, HS_LARGE, LANES),
    ):
        for i in range(ref.shape[1] // LANES):
            flipped = jnp.transpose(
                turned(ref[:, pl.ds(i * LANES, LANES)], gain_of[...], table, size)
            ).astype(BF16)
            for j in range(LANES // size):
                at = base + (h - base // LANES * 4) // 2 * size
                qt[h, pl.ds(at, size), :] = flipped[j * size : (j + 1) * size]
                h += 1

    acc[...] = jnp.zeros_like(acc)
    lbuf[...] = jnp.zeros_like(lbuf)
    mbuf[...] = jnp.full(mbuf.shape, -1e30, F32)

    below[...] = (
        (_iota((tok, tok), 0) < _iota((tok, tok), 1))
        & (_iota((tok, tok), 0) // rows == _iota((tok, tok), 1) // rows)
    ).astype(BF16)
    out_row = _iota((64, 64), 0)
    in_row = (
        (out_row // 8) % 2 * 32 + (out_row % 8) // SEATS * 16 + out_row // 16 * SEATS
    ) + out_row % SEATS
    perm[...] = (in_row == _iota((64, 64), 1)).astype(BF16)
    eye = (_iota((rows, rows), 0) == _iota((rows, rows), 1)).astype(BF16)
    columns = lax.dot_general(
        eye, names.astype(BF16), (((1,), (1,)), ((), ())), preferred_element_type=F32
    )
    earlier = _iota((rows, rows), 1) < _iota((rows, rows), 0)
    for k in range(2):
        column = columns[:, k : k + 1]
        same = ((column == names[0:1, :]) | (column == names[1:2, :])) & earlier
        rank = jnp.sum(same.astype(F32), axis=1, keepdims=True).astype(jnp.int32)
        expert = column.astype(jnp.int32)
        host = expert // 2
        away = z - host // 2
        away = jnp.where(away < 0, away + n_z, away)
        other = (host % 2 != core).astype(jnp.int32)
        step = jnp.minimum(away, n_z - away)
        edge = (away == 0) | (away == last)
        pair = jnp.where(
            away == 0, 0, jnp.where(away == last, 2 * last - 1, 2 * step - 1 + other)
        )
        side = jnp.where(edge, other, (away < last).astype(jnp.int32))
        base = (pair * 2 + side) * 16 + expert % 2 * SEATS + rank
        seat = _iota((rows, pick.shape[1]), 1)
        pick[pl.ds(k * rows, rows), :] = (seat == base).astype(BF16)
        pick[pl.ds((2 + k) * rows, rows), :] = (seat == base + 8).astype(BF16)

    def attend(pair):
        keys = kvbuf[pair, :, pl.ds(0, tok), :].reshape(2 * tok, tok)
        ahead = jnp.dot(keys, qt[0], preferred_element_type=F32)
        for h, (a0, size, v0, scale) in enumerate(heads):
            s = ahead
            if h + 1 < len(heads):
                ahead = jnp.dot(keys, qt[h + 1], preferred_element_type=F32)
            m_old = mbuf[h]
            m_new = jnp.maximum(m_old, jnp.max(s, axis=0, keepdims=True))
            p = jnp.exp2((s - m_new) * (scale * LOG2E))
            shrink = jnp.exp2((m_old - m_new) * (scale * LOG2E))
            mbuf[h] = m_new
            lbuf[h] = lbuf[h] * shrink + jnp.sum(p, axis=0, keepdims=True)
            pb = p.astype(BF16)
            pv = jnp.dot(
                kvbuf[pair, 0, pl.ds(tok + v0, size), :],
                pb[:tok],
                preferred_element_type=F32,
            ) + jnp.dot(
                kvbuf[pair, 1, pl.ds(tok + v0, size), :],
                pb[tok:],
                preferred_element_type=F32,
            )
            acc[pl.ds(a0, size), :] = acc[pl.ds(a0, size), :] * shrink + pv

    def attend_turn(t, carry):
        step = t // 2 + 1
        phase = lax.rem(t, 2)
        for part in range(2):

            @pl.when((phase == part) & (step < last))
            def _():
                ring.pass_on(step, part)

        @pl.when(t == 0)
        def _():
            ring.first_partner()

        @pl.when((phase == 0) & (t > 0))
        def _():
            ring.from_partner(t // 2)

        @pl.when(t == 2 * last - 1)
        def _():
            ring.opposite()
            ring.opposite_partner()

        attend(t)
        return carry

    lax.fori_loop(0, 2 * last, attend_turn, 0)

    loads[2].wait()
    loads[3].wait()
    for h, (a0, size, v0, scale) in enumerate(heads):
        acc[pl.ds(a0, size), :] = acc[pl.ds(a0, size), :] / lbuf[h]
    heard = jnp.transpose(acc[...]).astype(BF16)
    hbuf[...] = heard.reshape(4, rows, heard.shape[1])

    def project(where, owner):
        cbuf[where] = jnp.dot(hbuf[owner], wbuf[...], preferred_element_type=F32).astype(BF16)

    quarter = rows // 4
    halves = (pl.ds(0, 2 * quarter), pl.ds(2 * quarter, 2 * quarter))

    def first(part, way):
        piece = pl.ds((2 * part + way) * quarter, quarter)
        return _send(
            cbuf.at[0, piece],
            dbuf.at[3, piece],
            xs.at[0],
            xr.at[part, way],
            "tp",
            (x_right, x_left)[way],
        )

    def near(part, way):
        return _send(
            cbuf.at[1 + way, halves[part]],
            dbuf.at[way, halves[part]],
            xs.at[0],
            xr.at[part, 2],
            "tp",
            (x_right, x_left)[way],
        )

    def relay(part, way):
        piece = pl.ds((2 * part + way) * quarter, quarter)
        return _send(
            dbuf.at[3, piece],
            dbuf.at[2, piece],
            xs.at[0],
            xr.at[part, 3],
            "tp",
            (x_right, x_left)[way],
        )

    def came_in(ref, sem):
        _send(ref, ref, xs.at[0], sem, "tp", x_right).wait_recv()

    project(0, x_far)
    for way in range(2):
        first(0, way).start()
    project(1, x_right)
    near(0, 0).start()
    project(2, x_left)
    near(0, 1).start()
    for way in range(2):
        first(1, way).start()
    project(3, tp)
    for way in range(2):
        first(0, way).wait_recv()
        relay(0, way).start()
    for way in range(2):
        near(1, way).start()
    for way in range(2):
        first(1, way).wait_recv()
        relay(1, way).start()
    ring.finish()
    for part, half in enumerate(halves):
        came_in(dbuf.at[pl.ds(0, 2), half], xr.at[part, 2])
        came_in(dbuf.at[2, half], xr.at[part, 3])
        total = (
            cbuf[3, half].astype(F32)
            + dbuf[0, half].astype(F32)
            + dbuf[1, half].astype(F32)
            + dbuf[2, half].astype(F32)
        )
        attended = (res_ref[half].astype(F32) + total).astype(BF16)
        abuf[half] = attended
        wide = attended.astype(F32)
        xbuf[0, 0, half] = (
            wide
            * lax.rsqrt(jnp.mean(wide * wide, axis=-1, keepdims=True) + norm_eps)
            * gain_ref[...]
        ).astype(BF16)
        tokens.begin(part)
    _send(cbuf, cbuf, xs.at[0], xr.at[0, 0], "tp", x_right).wait_send()

    def share_right(c):
        return _send(gbuf.at[c, 0], gbuf.at[c, 1], gs.at[0], gr.at[c, 0], "tp", x_right)

    def share_left(c):
        return _send(gbuf.at[c, 0], gbuf.at[c, 2], gs.at[0], gr.at[c, 0], "tp", x_left)

    def pass_right(c):
        return _send(
            gbuf.at[c, 1, 0], gbuf.at[c, 3, 0], gs.at[0], gr.at[c, 1], "tp", x_right
        )

    def pass_left(c):
        return _send(gbuf.at[c, 2, 1], gbuf.at[c, 3, 1], gs.at[0], gr.at[c, 1], "tp", x_left)

    def far_right(c):
        return _send(pbuf.at[c, 3, 0], rbuf.at[c, 0], rs.at[0], rr.at[c, 0], "tp", x_right)

    def far_left(c):
        return _send(pbuf.at[c, 3, 1], rbuf.at[c, 1], rs.at[0], rr.at[c, 0], "tp", x_left)

    def near_right(c):
        return _send(pbuf.at[c, 2], fbuf.at[c, 0], rs.at[0], rr.at[c, 1], "tp", x_right)

    def near_left(c):
        return _send(pbuf.at[c, 1], fbuf.at[c, 1], rs.at[0], rr.at[c, 1], "tp", x_left)

    def both(ref, sem):
        _send(ref, ref, gs.at[0], sem, "tp", x_right).wait_recv()

    def seats_of(c):
        row = _iota((16, tok), 0)
        kept = jnp.zeros((16, tok), F32)
        for q in range(4):
            block = kvbuf[2 * c + q // 2, q % 2, pl.ds(2 * tok, 16), :].astype(F32)
            kept = jnp.where(row // 2 == q, block, kept)
        name0 = jnp.sum(jnp.where(row % 2 == 0, kept, 0.0), axis=0, keepdims=True)
        name1 = jnp.sum(jnp.where(row % 2 == 1, kept, 0.0), axis=0, keepdims=True)
        wide_row = _iota((32, tok), 0)
        mine = (2 * sp + wide_row // 16).astype(F32)
        member = (name0 == mine) | (name1 == mine)
        rank = jnp.dot(member.astype(F32).astype(BF16), below[...], preferred_element_type=F32)
        seated = (
            member
            & (rank == (wide_row % SEATS).astype(F32))
            & (_iota((32, tok), 1) // rows == wide_row % 16 // SEATS)
        )
        return seated.astype(F32).astype(BF16)

    def run_experts(c):
        for e in range(2):
            x = gbuf[c, :, e].reshape(64, width)
            gate = jnp.dot(x, wg[e], preferred_element_type=F32)
            up = jnp.dot(x, wu[e], preferred_element_type=F32)
            active = (gate / (1.0 + jnp.exp(-gate)) * up).astype(BF16)
            term = jnp.dot(active, wd[e], preferred_element_type=F32)
            pbuf[c, :, e] = term.astype(BF16).reshape(4, 16, width)

    def gather_turn(c):
        step = c + 1

        @pl.when(step < last)
        def _():
            for part in range(2):
                tokens.pass_on(step, part)

        @pl.when(step == last)
        def _():
            tokens.opposite()

        @pl.when(c == 0)
        def _():
            tokens.first_partner()

        @pl.when((c > 0) & (c < last))
        def _():
            tokens.from_partner(c)

        @pl.when(step == last)
        def _():
            tokens.opposite_partner()

        @pl.when(c < last)
        def _():
            block = xbuf[pl.ds(2 * c, 2)].reshape(4 * rows, width)
            chosen = jnp.dot(seats_of(c), block, preferred_element_type=F32)
            gbuf[c, 0] = chosen.astype(BF16).reshape(2, 16, width)
            share_right(c).start()
            share_left(c).start()

        @pl.when((c >= 1) & (c < last + 1))
        def _():
            both(gbuf.at[c - 1, pl.ds(1, 2)], gr.at[c - 1, 0])
            pass_right(c - 1).start()
            pass_left(c - 1).start()

        @pl.when(c == 2)
        def _():
            for load in loads[4:]:
                load.wait()

        @pl.when((c >= 2) & (c < last + 2))
        def _():
            both(gbuf.at[c - 2, 3], gr.at[c - 2, 1])
            run_experts(c - 2)

    def home(c, q):
        if q == 0:
            return lax.rem(z - c + n_z, n_z) * 2 + 1 - core, 2 * c, 0
        if q == 1:
            return lax.rem(z + c, n_z) * 2 + 1 - core, 2 * c, 1
        if q == 2:
            return lax.rem(z - c - 1 + n_z, n_z) * 2 + core, 2 * c + 1, 0
        return lax.rem(z + c + 1, n_z) * 2 + core, 2 * c + 1, 1

    def give(c, q):
        dev, pair, side = home(c, q)
        return _send(
            obuf.at[c, q], ret.at[pair, side], ts.at[min(q, 1)], tr.at[1], "sp", dev
        )

    def give_last():
        dev = lax.rem(z + last, n_z) * 2 + 1 - core
        return _send(
            obuf.at[last - 1, 3],
            ret.at[2 * last - 1, 1],
            ts.at[1],
            tr.at[1],
            "sp",
            dev,
        )

    start = last // 2 - 1

    def order(i):
        high = last - start
        late = i // high
        return (1 - late) * (i + start) + late * (last - 1 - i)

    def give_partner():
        return _send(obuf.at[0, 1], ret.at[0, 1], ts.at[1], tr.at[0], "sp", partner)

    def return_turn(i):
        @pl.when((i >= 0) & (i < last))
        def _():
            c = order(i)
            far_right(c).start()
            far_left(c).start()

        @pl.when((i >= 1) & (i < last + 1))
        def _():
            c = order(i - 1)
            both(rbuf.at[c], rr.at[c, 0])
            pbuf[c, 2, 0] = (pbuf[c, 2, 0].astype(F32) + rbuf[c, 0].astype(F32)).astype(BF16)
            near_right(c).start()
            pbuf[c, 1, 1] = (pbuf[c, 1, 1].astype(F32) + rbuf[c, 1].astype(F32)).astype(BF16)
            near_left(c).start()

        @pl.when(i >= 2)
        def _():
            c = order(i - 2)
            both(fbuf.at[c], rr.at[c, 1])
            total = pbuf[c, 0].astype(F32) + fbuf[c, 0].astype(F32) + fbuf[c, 1].astype(F32)
            total = total.astype(BF16).reshape(32, width)
            split = jnp.concatenate([total[:, : width // 2], total[:, width // 2 :]], axis=0)
            ordered = jnp.dot(perm[...], split, preferred_element_type=F32)
            obuf[c] = ordered.astype(BF16).reshape(4, 16, width // 2)

            @pl.when(c > 0)
            def _():
                give(c, 0).start()
                give(c, 1).start()

            @pl.when(c == 0)
            def _():
                ret[0, 0] = obuf[0, 0]
                give_partner().start()

            give(c, 2).start()

            @pl.when(c < last - 1)
            def _():
                give(c, 3).start()

            @pl.when(c == last - 1)
            def _():
                give_last().start()

    def turn(t, carry):
        gather_turn(t)
        return_turn(t - (start + 2))
        return carry

    lax.fori_loop(0, last + start + 4, turn, 0)

    tokens.finish()

    sent = gbuf.at[pl.ds(0, 3 * (last // 4))]
    _send(sent, sent, gs.at[0], gr.at[0, 0], "tp", x_right).wait_send()
    sent = pbuf.at[pl.ds(0, 3 * (last // 4))]
    _send(sent, sent, rs.at[0], rr.at[0, 0], "tp", x_right).wait_send()
    home_all = ret.at[pl.ds(1, 2 * last - 1)]
    give_partner().wait_recv()
    _send(home_all, home_all, ts.at[0], tr.at[1], "sp", partner).wait_recv()

    back = ret[...].reshape(ret.shape[0] * 32, width // 2)
    picked = jnp.dot(pick[...], back, preferred_element_type=F32)
    scores = score_ref[...]
    scores = scores / (scores[0:1, :] + scores[1:2, :])
    on_row = _iota((rows, rows), 0) == _iota((rows, rows), 1)
    one = jnp.sum(jnp.where(on_row, scores[0:1, :], 0.0), axis=1, keepdims=True)
    two = jnp.sum(jnp.where(on_row, scores[1:2, :], 0.0), axis=1, keepdims=True)
    out = abuf[...].astype(F32)
    lower = picked[:rows] * one + picked[rows : 2 * rows] * two
    upper = picked[2 * rows : 3 * rows] * one + picked[3 * rows :] * two
    out_ref[:, : width // 2] = (out[:, : width // 2] + lower).astype(BF16)
    out_ref[:, width // 2 :] = (out[:, width // 2 :] + upper).astype(BF16)

    sent = obuf.at[pl.ds(1, last - 1), 0]
    _send(sent, sent, ts.at[0], tr.at[1], "sp", partner).wait_send()
    sent = obuf.at[pl.ds(0, 3 * (last // 4))]
    _send(sent, sent, ts.at[1], tr.at[1], "sp", partner).wait_send()


def turn_tables(places, size, by_row):
    lane = np.arange(LANES) % size
    quarter = size // 4
    rates = np.power(
        np.float32(theta_base), (-2.0 * np.arange(quarter) / (size // 2)).astype(np.float32)
    ).astype(np.float32)
    angles = (places[:, None].astype(np.float32) * rates[lane % quarter]).astype(np.float32)
    here = (lane < size // 2) if by_row else (lane >= size // 2)
    sign = np.where(lane % (2 * quarter) < quarter, -1.0, 1.0)
    cosine = np.where(here, np.cos(angles), 0.0)
    sine = np.where(here, np.sin(angles) * sign, 0.0)
    return cosine.astype(np.float32), sine.astype(np.float32)


def on_device(
    queries_small,
    keys_small,
    values_small,
    queries_large,
    keys_large,
    values_large,
    query_gain_small,
    key_gain_small,
    query_gain_large,
    key_gain_large,
    residual_in,
    out_weight_small,
    out_weight_large,
    norm_gain,
    routes,
    route_scores,
    expert_gate,
    expert_up,
    expert_down,
):
    tok = queries_small.shape[0]
    rows, width = residual_in.shape
    n_sp = lax.axis_size("sp")
    pairs = n_sp // 2
    chunks = pairs // 2
    depth = out_weight_small.shape[0] + out_weight_large.shape[0]
    kv_rows = 2 * tok + 16
    grid_rows = tok // GRID_W
    row_places = np.arange(n_sp * grid_rows)
    col_places = np.arange(GRID_W)
    row_tables, col_tables = [], []
    for size in (HS_SMALL, HS_LARGE):
        row_tables.extend(turn_tables(row_places, size, True))
        col_tables.extend(turn_tables(col_places, size, False))
    heads = []
    wide_small = keys_small.shape[1]
    for count, kv_count, size, a0, v0 in (
        (queries_small.shape[1] // HS_SMALL, wide_small // HS_SMALL, HS_SMALL, 0, 0),
        (
            queries_large.shape[1] // HS_LARGE,
            keys_large.shape[1] // HS_LARGE,
            HS_LARGE,
            queries_small.shape[1],
            wide_small,
        ),
    ):
        for h in range(count):
            kv = h // (count // kv_count)
            heads.append((a0 + h * size, size, v0 + kv * size, size ** (-0.5)))
    vmem = pl.BlockSpec(memory_space=pltpu.VMEM)
    hbm = pl.BlockSpec(memory_space=pl.ANY)
    dma = pltpu.SemaphoreType.DMA
    V = pltpu.VMEM
    return pl.pallas_call(
        functools.partial(layer_kernel, tuple(heads)),
        out_shape=jax.ShapeDtypeStruct((rows, width), BF16),
        in_specs=[vmem] * 10 + [hbm] * 4 + [vmem] * 4 + [hbm] * 3,
        out_specs=vmem,
        scratch_shapes=[
            V((pairs, 2, kv_rows, tok), BF16),
            V((len(heads), tok, tok), BF16),
            V((4, GRID_W, LANES), F32),
            V((grid_rows, 4, LANES), F32),
            V((4, tok, LANES), F32),
            V((depth, width), BF16),
            V((depth, tok), F32),
            V((len(heads), 1, tok), F32),
            V((len(heads), 1, tok), F32),
            V((4, rows, depth), BF16),
            V((4, rows, width), BF16),
            V((4, rows, width), BF16),
            V((rows, width), BF16),
            V((pairs, 2, rows, width), BF16),
            V(expert_gate.shape, BF16),
            V(expert_up.shape, BF16),
            V(expert_down.shape, BF16),
            V((chunks, 4, 2, 16, width), BF16),
            V((chunks, 4, 2, 16, width), BF16),
            V((chunks, 2, 16, width), BF16),
            V((chunks, 2, 2, 16, width), BF16),
            V((chunks, 4, 16, width // 2), BF16),
            V((pairs, 2, 16, width // 2), BF16),
            V((tok, tok), BF16),
            V((64, 64), BF16),
            V((4 * rows, pairs * 32), BF16),
            dma((7,)),
            dma((chunks, 2)),
            dma((chunks,)),
            dma((2,)),
            dma((2,)),
            dma((2, 4)),
            dma((1,)),
            dma((chunks, 2)),
            dma((chunks,)),
            dma((2,)),
            dma((2,)),
            dma((chunks, 2)),
            dma((1,)),
            dma((chunks, 2)),
            dma((1,)),
            dma((2,)),
            dma((2,)),
        ],
        compiler_params=pltpu.CompilerParams(
            collective_id=0, has_side_effects=True, vmem_limit_bytes=58 * 1024 * 1024
        ),
        name="layer",
    )(
        queries_small,
        keys_small,
        values_small,
        queries_large,
        keys_large,
        values_large,
        query_gain_small.reshape(1, -1),
        key_gain_small.reshape(1, -1),
        query_gain_large.reshape(1, -1),
        key_gain_large.reshape(1, -1),
        jnp.asarray(np.stack(col_tables)),
        jnp.asarray(np.stack(row_tables, axis=1)),
        out_weight_small,
        out_weight_large,
        residual_in,
        norm_gain.reshape(1, -1),
        routes.T,
        route_scores.T,
        expert_gate,
        expert_up,
        expert_down,
    )


def solution(mesh):
    in_specs = (
        P(("grp", "sp"), "tp"),
        P(("grp", "sp"), "tp"),
        P(("grp", "sp"), "tp"),
        P(("grp", "sp"), "tp"),
        P(("grp", "sp"), "tp"),
        P(("grp", "sp"), "tp"),
        P("grp"),
        P("grp"),
        P("grp"),
        P("grp"),
        P(("grp", "sp", "tp"), None),
        P("tp", None),
        P("tp", None),
        P(),
        P(("grp", "sp", "tp"), None),
        P(("grp", "sp", "tp"), None),
        P("sp", None, "tp"),
        P("sp", None, "tp"),
        P("sp", "tp", None),
    )
    out_specs = P(("grp", "sp", "tp"), None)
    return jax.shard_map(
        on_device, mesh=mesh, in_specs=in_specs, out_specs=out_specs, check_vma=False
    )
```
